256 devices in a mesh: sp: 32 (over z, y), tp: 8 (over x, core).
Axes of the slice: x: 4, y: 4, z: 8, core: 2. Of those that a mesh axis runs over, the one named last changes fastest.
Arguments:
- head_value_rows: bfloat16 [24576, 2048], P('sp', 'tp'), may hold values from -6 to 6
- entry_map_rows: bfloat16 [24576, 1024], P('sp', 'tp'), may hold values from -6 to 6
- readout_map_rows: bfloat16 [24576, 1024], P('sp', 'tp'), may hold values from -6 to 6
- output_gate_rows: bfloat16 [24576, 2048], P('sp', 'tp'), may hold values from -6 to 6
- step_before_softplus: bfloat16 [24576, 32], P('sp', 'tp'), may hold values from -8 to 8
- sudden_log_decay: float32 [24576, 32], P('sp', 'tp'), may hold values from -1 to 0
- document_index: int32 [24576], replicated, may hold values from 0 to 7, never falling along the last dimension, each value on 1 to 6144 neighbouring positions
- head_rate_logarithm: float32 [2, 32], P(None, 'tp'), may hold values from -30 to 0
- head_step_bias: float32 [2, 32], P(None, 'tp'), may hold values from -3 to 3
- value_conv_taps: bfloat16 [5, 2048], P(None, 'tp'), may hold values from -2.5 to 2.5
- entry_conv_taps: bfloat16 [5, 1024], P(None, 'tp'), may hold values from -2.5 to 2.5
- readout_conv_taps: bfloat16 [5, 1024], P(None, 'tp'), may hold values from -2.5 to 2.5
- group_norm_gain: float32 [2048], P('tp'), may hold values from 0.1 to 1.9
- mixer_output_weight: bfloat16 [2048, 2048], P('tp'), may hold values from -0.125 to 0.125
- stream: bfloat16 [24576, 2048], P('sp', 'tp'), may hold values from -200 to 200
- mixer_norm_gain: float32 [2048], P('tp'), may hold values from 0.1 to 1.9
- channel_norm_gain: float32 [2048], P('tp'), may hold values from 0.1 to 1.9
- up_projection_weight: bfloat16 [2048, 8192], P('sp', 'tp'), may hold values from -0.125 to 0.125
- down_projection_weight: bfloat16 [2048, 8192], P('sp', 'tp'), may hold values from -0.0625 to 0.0625
Outputs:
- mixed: bfloat16 [24576, 2048], P('sp', 'tp')
The draws below stay inside these ranges and needn't reach their ends.
All inputs are finite; a program needn't handle non-finite values.
Results may differ from the reference program's by a relative error of at most 0.018.
Values may be sent and summed in bfloat16 or wider, within the bound.
A program may use at most 64 MiB of HBM per device.

```python
import math
import jax
import jax.numpy as jnp
import numpy as np
from jax import lax

D = 2048
HEADS = 32
HEAD_DIM = 64
GROUPS = 8
STATE = 128
FF = 8192
CONV_WIDTH = 5
BLOCK = 128
TOK_DEV = 768
INNER = 2048
TOKENS = 24576
N_SP = 32
N_TP = 8


def draw_step_before_softplus(key, part):
    jitter_key, shift_key = jax.random.split(key)
    jitter = jnp.clip(jax.random.normal(jitter_key, (TOKENS, HEADS), jnp.float32), -4.0, 4.0)
    shifts = jax.random.uniform(shift_key, (TOKENS // TOK_DEV, 1, HEADS), jnp.float32, -1.0, 1.5)
    shifts = jnp.broadcast_to(shifts, (TOKENS // TOK_DEV, TOK_DEV, HEADS)).reshape(TOKENS, HEADS)
    return (jitter + shifts).astype(jnp.bfloat16)


def draw_head_rate_logarithm(key, part):
    pick_key, slow_key, fast_key = jax.random.split(key, 3)
    quick = jax.random.randint(pick_key, (2, HEADS), 0, 2) == 1
    slow_rate = jax.random.uniform(slow_key, (2, HEADS), jnp.float32, math.log(0.1), math.log(0.5))
    slow_rate = slow_rate - jnp.log(jnp.float32(TOKENS))
    fast_rate = jax.random.uniform(fast_key, (2, HEADS), jnp.float32, math.log(0.01), math.log(1.0 / 30.0))
    return jnp.where(quick, fast_rate, slow_rate)


def draw_sudden_log_decay(key, part):
    where_key, depth_key = jax.random.split(key)
    struck = jax.random.randint(where_key, (TOKENS, 1), 0, TOKENS) < 4
    depth = jax.random.uniform(depth_key, (TOKENS, HEADS), jnp.float32, math.log(0.5), math.log(0.8))
    return jnp.where(struck, depth, 0.0)


def draw_stream(key, part):
    base_key, row_key = jax.random.split(key, 2)
    col_scale = 3.0 ** (jnp.arange(D, dtype=jnp.float32) / D - 0.5)
    values = jnp.clip(jax.random.normal(base_key, (TOKENS, D), jnp.float32), -6.0, 6.0)
    row_scale = jnp.exp(jax.random.uniform(row_key, (TOKENS, 1), jnp.float32, math.log(0.5), math.log(2.0)))
    return (values * row_scale * col_scale).astype(jnp.bfloat16)


def levels(stream_key, shape, cuts, low, largest):
    loudness = 1.0
    for axis_at, blocks in cuts:
        heights = jax.random.uniform(jax.random.fold_in(jax.random.fold_in(stream_key, 6), axis_at), (blocks,), jnp.float32, low / len(cuts), largest / len(cuts))
        loudness = loudness * jnp.repeat(jnp.exp(heights), shape[axis_at] // blocks).reshape((-1,) + (1,) * (len(shape) - 1 - axis_at))
    return loudness


def split_up(amount, total, bound, skew):
    weights = [(1 << 20) // math.isqrt(grade ** skew) + 1 for grade in range(2, amount + 1)]
    spare, holding = total - bound - (amount - 1), [1] * (amount - 1)
    while spare > 0:
        movable = [i for i in range(amount - 1) if holding[i] < bound]
        pool, remaining = sum([weights[i] for i in movable]), spare
        for i in movable:
            more = min(bound - holding[i], max(1, remaining * weights[i] // pool), spare)
            holding[i] = holding[i] + more
            spare = spare - more
    return np.array([bound] + holding)


def ragged_sizes(key, amount, total, reach, skew):
    if amount == 2:
        one = jax.random.randint(key, (), max(1, total - reach), min(reach, total - 1) + 1)
        return jnp.stack([one, total - one])
    sizes = jnp.asarray(split_up(amount, total, reach, skew), jnp.int32)
    twos = (amount - 1) // 2
    donor, receiver = sizes[1:1 + 2 * twos:2], sizes[2:2 + 2 * twos:2]
    margin = jnp.minimum(donor - 1, reach - receiver)
    shifted = jax.random.randint(jax.random.fold_in(key, 1), (twos,), 0, 1 << 20) % (margin + 1)
    sizes = sizes.at[1:1 + 2 * twos:2].set(donor - shifted).at[2:2 + 2 * twos:2].set(receiver + shifted)
    return sizes[jax.random.permutation(jax.random.fold_in(key, 2), amount)]


def noise(own_key, extent, deviation, most, cuts=(), kind=jnp.bfloat16):
    loudness = levels(own_key, extent, cuts, -0.22, 0.18) if cuts else 1.0
    values = jax.random.normal(own_key, extent, jnp.float32) * deviation * loudness
    return jnp.minimum(jnp.maximum(values, -most), most).astype(kind)


def setup_inputs(seed: int = 0) -> dict:
    arg_keys = jax.random.split(jax.random.key(seed), 20)
    return {
        "head_value_rows": noise(arg_keys[0], (TOKENS, INNER), 1.0, 6.0, ((0, 32), (1, 8))),
        "entry_map_rows": noise(arg_keys[1], (TOKENS, GROUPS * STATE), 1.0, 6.0, ((0, 32), (1, 8))),
        "readout_map_rows": noise(arg_keys[2], (TOKENS, GROUPS * STATE), 1.0, 6.0, ((0, 32), (1, 8))),
        "output_gate_rows": noise(arg_keys[3], (TOKENS, INNER), 1.0, 6.0, ((0, 32), (1, 8))),
        "step_before_softplus": draw_step_before_softplus(jax.random.fold_in(arg_keys[19], 71), 0),
        "sudden_log_decay": draw_sudden_log_decay(jax.random.fold_in(arg_keys[19], 71), 0),
        "document_index": jnp.searchsorted(jnp.cumsum(ragged_sizes(arg_keys[6], N_SP // 4, TOKENS, 8 * TOK_DEV, 1)), jnp.arange(TOKENS), side="right").astype(jnp.int32),
        "head_rate_logarithm": draw_head_rate_logarithm(jax.random.fold_in(arg_keys[19], 71), 0),
        "head_step_bias": noise(arg_keys[8], (2, HEADS), 0.5, 3.0, ((1, 8),), jnp.float32),
        "value_conv_taps": noise(arg_keys[9], (CONV_WIDTH, INNER), CONV_WIDTH ** -0.5, 2.5, ((1, 8),)),
        "entry_conv_taps": noise(arg_keys[10], (CONV_WIDTH, GROUPS * STATE), CONV_WIDTH ** -0.5, 2.5, ((1, 8),)),
        "readout_conv_taps": noise(arg_keys[11], (CONV_WIDTH, GROUPS * STATE), CONV_WIDTH ** -0.5, 2.5, ((1, 8),)),
        "group_norm_gain": jnp.clip(1.0 + 0.18 * jax.random.normal(arg_keys[12], (INNER,), jnp.float32), 0.1, 1.9),
        "mixer_output_weight": noise(arg_keys[13], (INNER, D), INNER ** -0.5, 0.125, ((0, 8),)),
        "stream": draw_stream(jax.random.fold_in(arg_keys[19], 71), 0),
        "mixer_norm_gain": jnp.clip(1.0 + 0.18 * jax.random.normal(arg_keys[15], (D,), jnp.float32), 0.1, 1.9),
        "channel_norm_gain": jnp.clip(1.0 + 0.18 * jax.random.normal(arg_keys[16], (D,), jnp.float32), 0.1, 1.9),
        "up_projection_weight": noise(arg_keys[17], (D, FF), D ** -0.5, 0.125, ((0, 32), (1, 8))),
        "down_projection_weight": noise(arg_keys[18], (D, FF), FF ** -0.5, 0.0625, ((0, 32), (1, 8))),
    }


exact_prec = lax.Precision.HIGHEST
norm_eps = 1e-05
resid_scale = 1.4142135623730951

def block_step(running, blocks):
    states, last_doc = running
    scaled, entries, readout, decay_logarithm, block_ids = blocks
    block_len = block_ids.shape[0]
    cum_decay = jnp.cumsum(decay_logarithm, axis=0)
    indices = lax.iota(jnp.int32, block_len)
    linked = (indices[:, None] >= indices[None, :]) & (block_ids[:, None] == block_ids[None, :])
    link_mask = linked[:, :, None, None]
    spread = cum_decay[:, None] - cum_decay[None, :]
    weights = jnp.where(link_mask, jnp.exp(jnp.where(link_mask, spread, 0.0)), 0.0)
    scores = jnp.einsum('tgn,sgn->tsg', readout, entries, precision=exact_prec)
    within = jnp.einsum('tsg,tsgr,sgrp->tgrp', scores, weights, scaled, precision=exact_prec)
    arrival = jnp.where((block_ids == last_doc)[:, None, None], jnp.exp(cum_decay), 0.0)
    carried = jnp.einsum('tgn,grpn->tgrp', readout, states, precision=exact_prec) * arrival[..., None]
    end_doc = block_ids[-1]
    to_end = jnp.where((block_ids == end_doc)[:, None, None], jnp.exp(cum_decay[-1] - cum_decay), 0.0)
    passing = jnp.where(end_doc == last_doc, jnp.exp(cum_decay[-1]), 0.0)
    fresh = jnp.einsum('sgn,sgr,sgrp->grpn', entries, to_end, scaled, precision=exact_prec)
    return ((states * passing[..., None, None] + fresh, end_doc), within + carried)

def sweep_blocks(scaled, entries, readout, decay_logarithm, document_index, states, last_doc, block_len):
    row_count = document_index.shape[0]
    block_count = row_count // block_len

    def in_blocks(array):
        return array.reshape((block_count, block_len) + array.shape[1:])
    inputs = tuple((in_blocks(array) for array in (scaled, entries, readout, decay_logarithm, document_index)))
    (states, last_doc), output = lax.scan(block_step, (states, last_doc), inputs)
    return (output.reshape((row_count,) + output.shape[2:]), states)

def short_conv(inputs, weights, document_index):
    taps = weights.shape[0]
    half_width = taps // 2
    row_count = inputs.shape[0]
    padded = jnp.pad(inputs, ((half_width, half_width), (0, 0)))
    doc_pad = jnp.pad(document_index, half_width, constant_values=-1)
    summed = jnp.zeros(inputs.shape, jnp.float32)
    for offset in range(taps):
        same_doc = (doc_pad[offset:offset + row_count] == document_index)[:, None]
        summed = summed + weights[offset] * jnp.where(same_doc, padded[offset:offset + row_count], 0.0)
    return jax.nn.silu(summed)

def layer_norm(residual, gain):
    row_mean = lax.optimization_barrier(jnp.mean(residual, axis=1))
    row_var = lax.optimization_barrier(jnp.mean(residual * residual, axis=1)) - row_mean * row_mean
    return ((residual - row_mean[:, None]) * lax.rsqrt(row_var + norm_eps)[:, None] * gain).astype(jnp.bfloat16)

def block_sums(left, right):
    parts = jnp.einsum('tjc,jcd->jtd', left, right)
    rounded = parts.astype(jnp.bfloat16)
    rounded = lax.optimization_barrier(rounded)
    return lax.optimization_barrier(jnp.sum(rounded.astype(jnp.float32), axis=0))

def reference(head_value_rows, entry_map_rows, readout_map_rows, output_gate_rows, step_before_softplus, sudden_log_decay, document_index, head_rate_logarithm, head_step_bias, value_conv_taps, entry_conv_taps, readout_conv_taps, group_norm_gain, mixer_output_weight, stream, mixer_norm_gain, channel_norm_gain, up_projection_weight, down_projection_weight):
    per_group = HEADS // GROUPS
    values = short_conv(head_value_rows.astype(jnp.float32), value_conv_taps.astype(jnp.float32), document_index)
    values = values.reshape(TOKENS, GROUPS, per_group, HEAD_DIM)
    entries = short_conv(entry_map_rows.astype(jnp.float32), entry_conv_taps.astype(jnp.float32), document_index)
    entries = entries.reshape(TOKENS, GROUPS, STATE)
    readout = short_conv(readout_map_rows.astype(jnp.float32), readout_conv_taps.astype(jnp.float32), document_index)
    readout = readout.reshape(TOKENS, GROUPS, STATE)
    summed = jnp.zeros((TOKENS, GROUPS, per_group, HEAD_DIM), jnp.float32)
    for sweep_direction in range(2):
        head_step_length = jax.nn.softplus(step_before_softplus.astype(jnp.float32) + head_step_bias[sweep_direction])
        decay_logarithm = -jnp.exp(head_rate_logarithm[sweep_direction]) * head_step_length + sudden_log_decay
        decay_logarithm = decay_logarithm.reshape(TOKENS, GROUPS, per_group)
        scaled = values * head_step_length.reshape(TOKENS, GROUPS, per_group)[..., None]
        arrays = (scaled, entries, readout, decay_logarithm, document_index)
        if sweep_direction == 1:
            arrays = tuple((jnp.flip(array, 0) for array in arrays))
        start_state = jnp.zeros((GROUPS, per_group, HEAD_DIM, STATE), jnp.float32)
        output, _ = sweep_blocks(*arrays, start_state, jnp.int32(-1), BLOCK)
        if sweep_direction == 1:
            output = jnp.flip(output, 0)
        summed = summed + output
    gated = summed.reshape(TOKENS, GROUPS, per_group * HEAD_DIM)
    gated = gated * jax.nn.silu(output_gate_rows.astype(jnp.float32)).reshape(TOKENS, GROUPS, per_group * HEAD_DIM)
    gated = gated * lax.rsqrt(lax.optimization_barrier(jnp.mean(gated * gated, axis=2, keepdims=True)) + norm_eps)
    normed = (gated.reshape(TOKENS, INNER) * group_norm_gain).astype(jnp.bfloat16)
    out_blocks = mixer_output_weight.astype(jnp.float32).reshape(N_TP, INNER // N_TP, D)
    down_blocks = down_projection_weight.astype(jnp.float32).reshape(D, N_TP, FF // N_TP)

    def dense_rows(pieces):
        normed_rows, stream_rows = pieces
        mixer_sum = block_sums(normed_rows.astype(jnp.float32).reshape(-1, N_TP, INNER // N_TP), out_blocks)
        first_sum = resid_scale * stream_rows.astype(jnp.float32) + mixer_sum
        normed_one = layer_norm(first_sum, mixer_norm_gain)
        hidden = jnp.dot(normed_one, up_projection_weight, preferred_element_type=jnp.float32)
        squared = jnp.square(jax.nn.relu(hidden)).astype(jnp.bfloat16)
        parts = jnp.einsum('tjf,djf->jtd', squared.astype(jnp.float32).reshape(-1, N_TP, FF // N_TP), down_blocks)
        rounded = lax.optimization_barrier(parts.astype(jnp.bfloat16))
        down_sum = lax.optimization_barrier(jnp.sum(rounded.astype(jnp.float32), axis=0))
        second_sum = resid_scale * normed_one.astype(jnp.float32) + down_sum
        return layer_norm(second_sum, channel_norm_gain)
    result = lax.map(dense_rows, (normed.reshape(N_SP, TOK_DEV, INNER), stream.reshape(N_SP, TOK_DEV, D)))
    return result.reshape(TOKENS, D)
```

```python
import functools

import jax
import jax.numpy as jnp
from jax import lax
from jax.experimental import pallas as pl
from jax.experimental.pallas import tpu as pltpu
from jax.sharding import PartitionSpec as P

D = 2048
HEAD_DIM = 64
STATE = 128
REACH = 8
MESH = pl.DeviceIdType.MESH
norm_eps = 1e-05
resid_scale = 1.4142135623730951
F32 = jnp.float32
BF16 = jnp.bfloat16


def lanes_of(cols, rows, base):
    n = rows.size
    low = lax.broadcasted_iota(jnp.int32, (n, 128), 1) < HEAD_DIM
    halves = []
    for k in (0, 2):
        a = jnp.broadcast_to(cols[rows, base + k : base + k + 1], (n, 128))
        b = jnp.broadcast_to(cols[rows, base + k + 1 : base + k + 2], (n, 128))
        halves.append(jnp.where(low, a, b))
    return jnp.concatenate(halves, axis=1)


def head_lanes(column):
    return jnp.concatenate([jnp.broadcast_to(c, (1, HEAD_DIM)) for c in column], axis=1)


C0, D1, W0, W1, A0, A1, DT0, CM, DOC = 0, 4, 8, 12, 16, 20, 24, 28, 33


def mixer_kernel(
    hv, em, rm, gate, per_token, source_mask, taps, gain, out,
    prev_v, prev_e, prev_r, next_v, next_e, next_r,
    wide, rowq, cols, val, ent, ent32, rdo, weight, local,
    msg0, msg1, got0, got1,
    halo_send, halo_recv, state_send, state_recv,
):
    sp, tp = lax.axis_index("sp"), lax.axis_index("tp")
    n_sp = lax.axis_size("sp")
    rows = hv.shape[0]
    tiles = rows // 128

    def at(d):
        return (lax.rem(sp + d + n_sp, n_sp), tp)

    barrier = pltpu.get_barrier_semaphore()
    for d in range(1, REACH + 1):
        for s in (d, -d):
            pl.semaphore_signal(barrier, inc=1, device_id=at(s), device_id_type=MESH)
    pl.semaphore_wait(barrier, 2 * REACH)

    halos = []
    for k, (src, low, high) in enumerate(((hv, prev_v, next_v), (em, prev_e, next_e), (rm, prev_r, next_r))):
        for m, (first, dst, step) in enumerate(((rows - 16, low, 1), (0, high, -1))):
            halos.append(pltpu.make_async_remote_copy(
                src_ref=src.at[pl.ds(first, 16)], dst_ref=dst,
                send_sem=halo_send.at[2 * k + m], recv_sem=halo_recv.at[2 * k + m],
                device_id=at(step), device_id_type=MESH))
    for copy in halos:
        copy.start()

    dt = per_token[0:8, :]
    log_decay = per_token[8:16, :]
    lane = lax.broadcasted_iota(jnp.int32, (8, rows), 1)
    total = log_decay
    shift = 1
    while shift < rows:
        total = total + jnp.where(lane >= shift, pltpu.roll(total, shift, 1), 0.0)
        shift *= 2
    c0 = total[0:4]
    d1 = total[4:8] - log_decay[4:8]
    all0, all1 = total[0:4, rows - 1 : rows], total[4:8, rows - 1 : rows]
    docs = per_token[16:24, :]
    own = docs[2:3]
    same_end = jnp.where(own == own[:, rows - 1 : rows], 1.0, 0.0)
    same_start = jnp.where(own == own[:, 0:1], 1.0, 0.0)
    from_prev = jnp.where(own == docs[5:6], 1.0, 0.0)
    from_next = jnp.where(own == docs[6:7], 1.0, 0.0)
    rowq[...] = jnp.zeros_like(rowq)
    rowq[C0 : C0 + 4, :] = c0
    rowq[D1 : D1 + 4, :] = d1
    rowq[W0 : W0 + 4, :] = jnp.exp(all0 - c0) * dt[0:4] * same_end
    rowq[W1 : W1 + 4, :] = jnp.exp(d1) * dt[4:8] * same_start
    rowq[A0 : A0 + 4, :] = jnp.exp(c0) * from_prev
    rowq[A1 : A1 + 4, :] = jnp.exp(all1 - d1) * from_next
    rowq[DT0 : DT0 + 4, :] = dt[0:4]
    rowq[CM : CM + 5, :] = jnp.where(docs[0:5] == own, 1.0, 0.0)
    rowq[DOC : DOC + 1, :] = own
    for t in range(tiles):
        cols[pl.ds(128 * t, 128), :] = jnp.transpose(rowq[:, 128 * t : 128 * t + 128])

    wide[8 : 8 + rows, 0:256] = hv[...].astype(F32)
    wide[8 : 8 + rows, 256:384] = em[...].astype(F32)
    wide[8 : 8 + rows, 384:512] = rm[...].astype(F32)
    for copy in halos:
        copy.wait()
    wide[0:8, 0:256] = prev_v[8:16, :].astype(F32)
    wide[0:8, 256:384] = prev_e[8:16, :].astype(F32)
    wide[0:8, 384:512] = prev_r[8:16, :].astype(F32)
    wide[8 + rows : 16 + rows, 0:256] = next_v[0:8, :].astype(F32)
    wide[8 + rows : 16 + rows, 256:384] = next_e[0:8, :].astype(F32)
    wide[8 + rows : 16 + rows, 384:512] = next_r[0:8, :].astype(F32)

    for t in range(tiles):
        lo = 128 * t
        masks = [jnp.broadcast_to(cols[lo : lo + 128, CM + o : CM + o + 1], (128, 128)) for o in range(5)]
        for g in range(4):
            acc = jnp.zeros((128, 128), F32)
            for o in range(5):
                part = wide[lo + 6 + o : lo + 134 + o, 128 * g : 128 * g + 128]
                if o != 2:
                    part = part * masks[o]
                acc = acc + taps[o : o + 1, 128 * g : 128 * g + 128] * part
            act = acc * jax.nn.sigmoid(acc)
            if g < 2:
                val[lo : lo + 128, 128 * g : 128 * g + 128] = act.astype(BF16)
            elif g == 2:
                ent32[lo : lo + 128, :] = act
                ent[lo : lo + 128, :] = act.astype(BF16)
            else:
                rdo[lo : lo + 128, :] = act.astype(BF16)

    state0 = jnp.zeros((STATE, 256), F32)
    state1 = jnp.zeros((STATE, 256), F32)
    for t in range(tiles):
        r = pl.ds(128 * t, 128)
        ent_t = jnp.transpose(ent32[r, :]).astype(BF16)
        v = val[r, :].astype(F32)
        state0 += jnp.dot(ent_t, (v * lanes_of(cols, r, W0)).astype(BF16), preferred_element_type=F32)
        state1 += jnp.dot(ent_t, (v * lanes_of(cols, r, W1)).astype(BF16), preferred_element_type=F32)
    for msg, state, whole in ((msg0, state0, all0), (msg1, state1, all1)):
        msg[0:STATE, :] = state.astype(BF16)
        passing = head_lanes([jnp.exp(whole[h : h + 1, :]) for h in range(4)])
        coarse = passing.astype(BF16)
        fine = (passing - coarse.astype(F32)).astype(BF16)
        row = lax.broadcasted_iota(jnp.int32, (16, 256), 0)
        both = jnp.where(row == 0, coarse.astype(F32), jnp.where(row == 1, fine.astype(F32), 0.0))
        msg[STATE : STATE + 16, :] = both.astype(BF16)

    for t in range(tiles):
        r = pl.ds(128 * t, 128)
        own_score = jnp.sum(rdo[r, :].astype(F32) * ent[r, :].astype(F32), axis=1, keepdims=True)
        local[r, :] = own_score * lanes_of(cols, r, DT0) * val[r, :].astype(F32)

    sends = []
    for d in range(1, REACH + 1):
        for m, (msg, got, step) in enumerate(((msg0, got0, d), (msg1, got1, -d))):
            k = 2 * (d - 1) + m
            sends.append(pltpu.make_async_remote_copy(
                src_ref=msg, dst_ref=got.at[d - 1],
                send_sem=state_send.at[k], recv_sem=state_recv.at[k],
                device_id=at(step), device_id_type=MESH))
    for copy in sends:
        copy.start()

    low_lane = lax.broadcasted_iota(jnp.int32, (128, 128), 1) < HEAD_DIM

    def tile_step(i, _):
        r = pl.ds(pl.multiple_of(i * 128, 128), 128)
        here = rdo[r, :]
        doc_t = jnp.broadcast_to(cols[r, DOC : DOC + 1], (128, 128))
        t_index = lax.broadcasted_iota(jnp.int32, (128, 128), 0) + i * 128
        for pair in range(2):
            outs = []
            for h in (2 * pair, 2 * pair + 1):
                ct = jnp.broadcast_to(cols[r, C0 + h : C0 + h + 1], (128, 128))
                dd = jnp.broadcast_to(cols[r, D1 + h : D1 + h + 1], (128, 128))
                for j in range(tiles):
                    s = pl.ds(128 * j, 128)
                    if h == 0:
                        score = lax.dot_general(here, ent[s, :], (((1,), (1,)), ((), ())), preferred_element_type=F32)
                        score = jnp.where(doc_t == per_token[18:19, 128 * j : 128 * j + 128], score, 0.0)
                        weight[1, :, 128 * j : 128 * j + 128] = score
                    score = weight[1, :, 128 * j : 128 * j + 128]
                    s_index = lax.broadcasted_iota(jnp.int32, (128, 128), 1) + 128 * j
                    spread = jnp.minimum(ct - rowq[C0 + h : C0 + h + 1, 128 * j : 128 * j + 128],
                                         rowq[D1 + h : D1 + h + 1, 128 * j : 128 * j + 128] - dd)
                    step = jnp.where(s_index < t_index, per_token[h : h + 1, 128 * j : 128 * j + 128],
                                     per_token[4 + h : 5 + h, 128 * j : 128 * j + 128])
                    weight[0, :, 128 * j : 128 * j + 128] = score * jnp.exp(spread) * step
                outs.append(jnp.dot(weight[0].astype(BF16), val[:, 128 * pair : 128 * pair + 128],
                                    preferred_element_type=F32))
            local[r, 128 * pair : 128 * pair + 128] += jnp.where(low_lane, outs[0], outs[1])
        return 0

    lax.fori_loop(0, tiles, tile_step, 0)

    for copy in sends:
        copy.wait()
    carried = []
    for m, got in enumerate((got0, got1)):
        through = jnp.ones((1, 256), F32)
        state = jnp.zeros((STATE, 256), F32)
        for d in range(1, REACH + 1):
            state = state + got[d - 1, 0:STATE, :].astype(F32) * (through * source_mask[REACH * m + d - 1])
            tail = got[d - 1, STATE : STATE + 16, :].astype(F32)
            through = through * (tail[0:1] + tail[1:2])
        carried.append(state.astype(BF16))

    for t in range(tiles):
        r = pl.ds(128 * t, 128)
        here = rdo[r, :]
        y = local[r, :]
        y += jnp.dot(here, carried[0], preferred_element_type=F32) * lanes_of(cols, r, A0)
        y += jnp.dot(here, carried[1], preferred_element_type=F32) * lanes_of(cols, r, A1)
        z = gate[r, :].astype(F32)
        y = y * (z * jax.nn.sigmoid(z))
        y = y * lax.rsqrt(jnp.mean(y * y, axis=1, keepdims=True) + norm_eps)
        out[r, :] = (y * gain[...]).astype(BF16)


def mixer(hv, em, rm, gate, step, sudden, document_index, rate, bias, tv, te, tr, gain):
    rows = hv.shape[0]
    n_sp = lax.axis_size("sp")
    sp = lax.axis_index("sp")
    raw, sud = step.astype(F32).T, sudden.T
    dts, lds = [], []
    for k in range(2):
        dt = jax.nn.softplus(raw + bias[k][:, None])
        dts.append(dt)
        lds.append(-jnp.exp(rate[k])[:, None] * dt + sud)
    pad = jnp.pad(document_index, 3, constant_values=-1).astype(F32)
    window = lax.dynamic_slice_in_dim(pad, sp * rows, rows + 6)
    shifted = [window[1 + o : 1 + o + rows][None] for o in range(5)]
    before = jnp.broadcast_to(window[2:3], (1, rows))
    after = jnp.broadcast_to(window[rows + 3 : rows + 4], (1, rows))
    per_token = jnp.concatenate(dts + lds + shifted + [before, after, jnp.zeros((1, rows), F32)], axis=0)
    grid = document_index.reshape(n_sp, rows)
    last = lax.dynamic_slice_in_dim(jnp.pad(grid[:, rows - 1], REACH, constant_values=-1), sp, REACH)[::-1]
    first = lax.dynamic_slice_in_dim(jnp.pad(grid[:, 0], REACH, constant_values=-1), sp + REACH + 1, REACH)
    mask = jnp.concatenate([(last == last[0]) & (last >= 0), (first == first[0]) & (first >= 0)]).astype(F32)
    taps = jnp.pad(jnp.concatenate([tv, te, tr], axis=1).astype(F32), ((0, 3), (0, 0)))
    vmem = pl.BlockSpec(memory_space=pltpu.VMEM)
    return pl.pallas_call(
        mixer_kernel,
        out_shape=jax.ShapeDtypeStruct((rows, 256), BF16),
        in_specs=[vmem] * 5 + [pl.BlockSpec(memory_space=pltpu.SMEM)] + [vmem] * 2,
        out_specs=vmem,
        scratch_shapes=[
            pltpu.VMEM((16, 256), BF16), pltpu.VMEM((16, 128), BF16), pltpu.VMEM((16, 128), BF16),
            pltpu.VMEM((16, 256), BF16), pltpu.VMEM((16, 128), BF16), pltpu.VMEM((16, 128), BF16),
            pltpu.VMEM((rows + 16, 512), F32),
            pltpu.VMEM((128, rows), F32),
            pltpu.VMEM((rows, 128), F32),
            pltpu.VMEM((rows, 256), BF16), pltpu.VMEM((rows, 128), BF16), pltpu.VMEM((rows, 128), F32),
            pltpu.VMEM((rows, 128), BF16),
            pltpu.VMEM((2, 128, rows), F32),
            pltpu.VMEM((rows, 256), F32),
            pltpu.VMEM((STATE + 16, 256), BF16), pltpu.VMEM((STATE + 16, 256), BF16),
            pltpu.VMEM((REACH, STATE + 16, 256), BF16), pltpu.VMEM((REACH, STATE + 16, 256), BF16),
            pltpu.SemaphoreType.DMA((6,)), pltpu.SemaphoreType.DMA((6,)),
            pltpu.SemaphoreType.DMA((2 * REACH,)), pltpu.SemaphoreType.DMA((2 * REACH,)),
        ],
        compiler_params=pltpu.CompilerParams(
            collective_id=0, has_side_effects=True, vmem_limit_bytes=40 * 1024 * 1024),
        cost_estimate=pl.CostEstimate(flops=2_000_000_000, bytes_accessed=3_000_000, transcendentals=0),
        name="mixer",
    )(hv, em, rm, gate, per_token, mask, taps, gain[None, :])


def cut_along(array, dim, count):
    dims = array.shape
    blocks = array.reshape(*dims[:dim], count, dims[dim] // count, *dims[dim + 1 :])
    return jnp.moveaxis(blocks, dim, 0)


def sent_and_summed(array, axis, dim):
    blocks = cut_along(array, dim, lax.axis_size(axis))
    arrived = lax.all_to_all(blocks, axis, split_axis=0, concat_axis=0, tiled=True)
    return arrived.astype(jnp.float32).sum(axis=0)


def norm_rows(residual, gain, width):
    sums = lax.psum((jnp.sum(residual, axis=1), jnp.sum(residual * residual, axis=1)), "tp")
    row_mean = sums[0] / width
    row_var = sums[1] / width - row_mean * row_mean
    return ((residual - row_mean[:, None]) * lax.rsqrt(row_var + norm_eps)[:, None] * gain).astype(
        jnp.bfloat16
    )


def per_device(hv, em, rm, gate, step, sudden, document_index, rate, bias, tv, te, tr, gain,
               mixer_output_weight, stream, mixer_norm_gain, channel_norm_gain, up, down):
    normed = mixer(hv, em, rm, gate, step, sudden, document_index, rate, bias, tv, te, tr, gain)
    partial_value = jnp.dot(normed, mixer_output_weight, preferred_element_type=jnp.float32)
    mixer_sum = sent_and_summed(partial_value.astype(jnp.bfloat16), "tp", 1)
    first_sum = resid_scale * stream.astype(jnp.float32) + mixer_sum
    normed_one = norm_rows(first_sum, mixer_norm_gain, D)
    up_full, down_full = (
        lax.all_gather(up, "sp", axis=0, tiled=True),
        lax.all_gather(down, "sp", axis=0, tiled=True),
    )
    hidden = jnp.dot(
        lax.all_gather(normed_one, "tp", axis=1, tiled=True),
        up_full,
        preferred_element_type=jnp.float32,
    )
    squared = jnp.square(jax.nn.relu(hidden)).astype(jnp.bfloat16)
    down_part = lax.dot_general(
        squared, down_full, (((1,), (1,)), ((), ())), preferred_element_type=jnp.float32
    )
    down_sum = lax.psum_scatter(
        down_part.astype(jnp.bfloat16), "tp", scatter_dimension=1, tiled=True
    ).astype(jnp.float32)
    second_sum = resid_scale * normed_one.astype(jnp.float32) + down_sum
    return norm_rows(second_sum, channel_norm_gain, D)


SPECS = (
    P("sp", "tp"), P("sp", "tp"), P("sp", "tp"), P("sp", "tp"), P("sp", "tp"), P("sp", "tp"), P(),
    P(None, "tp"), P(None, "tp"), P(None, "tp"), P(None, "tp"), P(None, "tp"), P("tp"),
    P("tp", None), P("sp", "tp"), P("tp"), P("tp"), P("sp", "tp"), P("sp", "tp"),
)


def solution(mesh):
    return jax.shard_map(per_device, mesh=mesh, in_specs=SPECS, out_specs=P("sp", "tp"), check_vma=False)
```

```python
import functools

import jax
import jax.numpy as jnp
from jax import lax
from jax.experimental import pallas as pl
from jax.experimental.pallas import tpu as pltpu
from jax.sharding import PartitionSpec as P

D = 2048
HEAD_DIM = 64
STATE = 128
REACH = 8
MESH = pl.DeviceIdType.MESH
norm_eps = 1e-05
resid_scale = 1.4142135623730951
F32 = jnp.float32
BF16 = jnp.bfloat16


def lanes_of(cols, rows, base):
    n = rows.size
    low = lax.broadcasted_iota(jnp.int32, (n, 128), 1) < HEAD_DIM
    halves = []
    for k in (0, 2):
        a = jnp.broadcast_to(cols[rows, base + k : base + k + 1], (n, 128))
        b = jnp.broadcast_to(cols[rows, base + k + 1 : base + k + 2], (n, 128))
        halves.append(jnp.where(low, a, b))
    return jnp.concatenate(halves, axis=1)


def head_lanes(column):
    return jnp.concatenate([jnp.broadcast_to(c, (1, HEAD_DIM)) for c in column], axis=1)


C0, D1, W0, W1, A0, A1, DT0, CM, DOC = 0, 4, 8, 12, 16, 20, 24, 28, 33


def copy_to(src, dst, send, recv, device):
    return pltpu.make_async_remote_copy(src_ref=src, dst_ref=dst, send_sem=send, recv_sem=recv,
                                        device_id=device, device_id_type=MESH)


class WeightRing:
    def __init__(self, up_in, down_in, up, down, sems, sp, tp):
        (self.uy_s, self.uy_r, self.uh_s, self.uh_r, self.uz_s, self.uz_r,
         self.dz_s, self.dz_r, self.dy_s, self.dy_r, self.dh_s, self.dh_r) = sems
        self.up_in, self.down_in, self.up, self.down, self.tp = up_in, down_in, up, down, tp
        self.y, self.z = lax.rem(sp, 4), sp // 4
        self.sent = []

    def dev(self, dz, dy):
        return (lax.rem(self.z + dz + 8, 8) * 4 + lax.rem(self.y + dy + 4, 4), self.tp)

    def rows(self, dz, dy, low=0, count=64):
        shard = lax.rem(self.z + dz + 8, 8) * 4 + lax.rem(self.y + dy + 4, 4)
        return pl.ds(pl.multiple_of(shard * 64 + low, 32), count)

    def send(self, src, dst, send, recv, device):
        copy = copy_to(src, dst, send, recv, device)
        copy.start()
        self.sent.append(copy)

    def arrived(self, dst, send, recv):
        copy_to(dst, dst, send, recv, self.dev(1, 0)).wait_recv()

    def up_z(self, s, p, receive):
        for m, sign in enumerate((1, -1)):
            low, count = (32 * m, 32) if s == 3 else (0, 64)
            if receive:
                r = self.rows(-sign * (s + 1), p, low, count)
                self.arrived(self.up.at[r], self.uz_s.at[m, s, p], self.uz_r.at[m, s, p])
            else:
                r = self.rows(-sign * s, p, low, count)
                src = self.up_in if s == 0 and p == 0 else self.up.at[r]
                self.send(src, self.up.at[r], self.uz_s.at[m, s, p], self.uz_r.at[m, s, p], self.dev(sign, 0))

    def down_z(self, s, receive):
        for m, sign in enumerate((1, -1)):
            low, count = (32 * m, 32) if s == 3 else (0, 64)
            if receive:
                r = self.rows(-sign * (s + 1), 0, low, count)
                self.arrived(self.down.at[r], self.dz_s.at[m, s], self.dz_r.at[m, s])
            else:
                r = self.rows(-sign * s, 0, low, count)
                src = self.down_in if s == 0 else self.down.at[r]
                self.send(src, self.down.at[r], self.dz_s.at[m, s], self.dz_r.at[m, s], self.dev(sign, 0))

    def planes(self, s):
        return [(0, 0)] if s == 0 else [(7, 4)] if s == 4 else [(2 * s - 1, -s), (2 * s, s)]

    def down_y(self, s):
        for k, dz in self.planes(s):
            for m, sign in enumerate((1, -1)):
                r = self.rows(dz, 0)
                src = self.down_in if s == 0 else self.down.at[r]
                self.send(src, self.down.at[r], self.dy_s.at[k, m], self.dy_r.at[k, m], self.dev(0, sign))

    def down_half(self, s, receive):
        for k, dz in self.planes(s):
            for m, sign in enumerate((1, -1)):
                if receive:
                    r = self.rows(dz, -2 * sign, 32 * m, 32)
                    self.arrived(self.down.at[r], self.dh_s.at[k, m], self.dh_r.at[k, m])
                else:
                    self.arrived(self.down.at[self.rows(dz, -sign)], self.dy_s.at[k, m], self.dy_r.at[k, m])
                    r = self.rows(dz, -sign, 32 * m, 32)
                    self.send(self.down.at[r], self.down.at[r], self.dh_s.at[k, m], self.dh_r.at[k, m],
                              self.dev(0, sign))

    def step(self, n):
        s, part = divmod(n, 3)
        if part == 0:
            if s == 0:
                for m, sign in enumerate((1, -1)):
                    self.send(self.up_in, self.up.at[self.rows(0, 0)], self.uy_s.at[m], self.uy_r.at[m],
                              self.dev(0, sign))
            else:
                self.up_z(s - 1, 0, True)
                self.down_z(s - 1, True)
            if s < 4:
                self.up_z(s, 0, False)
                self.down_z(s, False)
            self.down_y(s)
        elif part == 1:
            if s == 0:
                for m, sign in enumerate((1, -1)):
                    self.arrived(self.up.at[self.rows(0, -sign)], self.uy_s.at[m], self.uy_r.at[m])
                    r = self.rows(0, -sign, 32 * m, 32)
                    self.send(self.up.at[r], self.up.at[r], self.uh_s.at[m], self.uh_r.at[m], self.dev(0, sign))
            else:
                self.up_z(s - 1, 1, True)
                self.up_z(s - 1, 3, True)
            if s < 4:
                self.up_z(s, 1, False)
                self.up_z(s, 3, False)
            self.down_half(s, False)
        else:
            if s == 0:
                for m, sign in enumerate((1, -1)):
                    self.arrived(self.up.at[self.rows(0, -2 * sign, 32 * m, 32)], self.uh_s.at[m], self.uh_r.at[m])
            else:
                self.up_z(s - 1, 2, True)
            if s < 4:
                self.up_z(s, 2, False)

    def finish(self):
        for s in range(5):
            self.down_half(s, True)


class TpGather:
    def __init__(self, own, buf, size, send, recv, sp, tp):
        self.own, self.buf, self.size, self.s, self.r, self.sp = own, buf, size, send, recv, sp
        self.x, self.c = tp // 2, lax.rem(tp, 2)
        self.sent = []

    def slot(self, dx, other):
        return lax.rem(self.x + dx + 4, 4) * 2 + (1 - self.c if other else self.c)

    def rows(self, dx, other, half=None):
        low, count = (0, self.size) if half is None else (half * (self.size // 2), self.size // 2)
        return self.buf.at[pl.ds(pl.multiple_of(self.slot(dx, other) * self.size + low, 16), count)]

    def send(self, src, dst, k, dx, other):
        copy = copy_to(src, dst, self.s.at[k], self.r.at[k], (self.sp, self.slot(dx, other)))
        copy.start()
        self.sent.append(copy)

    def arrived(self, dst, k):
        copy_to(dst, dst, self.s.at[k], self.r.at[k], (self.sp, self.slot(0, True))).wait_recv()

    def begin(self):
        mine = self.rows(0, False)
        self.send(self.own, mine, 0, 1, False)
        self.send(self.own, mine, 1, -1, False)
        self.send(self.own, mine, 2, 0, True)

    def relay(self):
        left, right = self.rows(-1, False), self.rows(1, False)
        self.arrived(left, 0)
        self.send(self.rows(-1, False, 0), self.rows(-1, False, 0), 3, 1, False)
        self.send(left, left, 5, 0, True)
        self.arrived(right, 1)
        self.send(self.rows(1, False, 1), self.rows(1, False, 1), 4, -1, False)
        self.send(right, right, 6, 0, True)

    def far(self):
        self.arrived(self.rows(2, False, 0), 3)
        self.arrived(self.rows(2, False, 1), 4)
        self.send(self.rows(2, False), self.rows(2, False), 7, 0, True)

    def sibling(self, k):
        self.arrived(self.rows({2: 0, 5: -1, 6: 1, 7: 2}[k], True), k)


def layer_kernel(
    hv, em, rm, gate, per_token, source_mask, taps, gain, up_in, down_in, wout_in, stream, gains_in, last_gain, out,
    prev_v, prev_e, prev_r, next_v, next_e, next_r,
    wide, rowq, cols, val, ent, ent32, rdo, weight, local,
    msg0, msg1, got0, got1,
    up, down, wout, norm_out, norm_in, stream_in, gains, first, tok, squares,
    sib_out, sib_in, own_part, outgoing, parts, stat_out, stat_in,
    halo_send, halo_recv, state_send, state_recv,
    uy_s, uy_r, uh_s, uh_r, uz_s, uz_r, dz_s, dz_r, dy_s, dy_r, dh_s, dh_r,
    wo_s, wo_r, tk_s, tk_r, ex_s, ex_r, sb_s, sb_r, rs_s, rs_r, st_s, st_r,
):
    sp, tp = lax.axis_index("sp"), lax.axis_index("tp")
    n_sp = lax.axis_size("sp")
    n_tp = lax.axis_size("tp")
    rows = hv.shape[0]
    tiles = rows // 128
    share = rows // n_tp

    def at(d):
        return (lax.rem(sp + d + n_sp, n_sp), tp)

    def peer(d):
        return lax.rem(tp + d + n_tp, n_tp)

    barrier = pltpu.get_barrier_semaphore()
    for d in range(1, REACH + 1):
        for s in (d, -d):
            pl.semaphore_signal(barrier, inc=1, device_id=at(s), device_id_type=MESH)
    for d in range(1, n_tp):
        pl.semaphore_signal(barrier, inc=1, device_id=(sp, peer(d)), device_id_type=MESH)
    pl.semaphore_wait(barrier, 2 * REACH + n_tp - 1)

    halos = []
    for k, (src, low, high) in enumerate(((hv, prev_v, next_v), (em, prev_e, next_e), (rm, prev_r, next_r))):
        for m, (start, dst, step) in enumerate(((rows - 16, low, 1), (0, high, -1))):
            halos.append(copy_to(src.at[pl.ds(start, 16)], dst, halo_send.at[2 * k + m], halo_recv.at[2 * k + m],
                                 at(step)))
    for copy in halos:
        copy.start()
    ring = WeightRing(up_in, down_in, up, down,
                      (uy_s, uy_r, uh_s, uh_r, uz_s, uz_r, dz_s, dz_r, dy_s, dy_r, dh_s, dh_r), sp, tp)
    ring.step(0)
    wo = TpGather(wout_in, wout, 256, wo_s, wo_r, sp, tp)
    wo.begin()

    def my_lanes(ref, q):
        return ref.at[:, pl.ds(pl.multiple_of(q * 256, 256), 256)]

    def exchange(k, src_of, dst):
        sent = []
        for d in range(1, n_tp):
            q = peer(d)
            copy = copy_to(src_of(q), my_lanes(dst, tp), ex_s.at[k, d - 1], ex_r.at[k, d - 1], (sp, q))
            copy.start()
            sent.append(copy)
        return sent

    def exchanged(k, dst):
        for d in range(1, n_tp):
            r = my_lanes(dst, peer(-d))
            copy_to(r, r, ex_s.at[k, d - 1], ex_r.at[k, d - 1], (sp, peer(d))).wait_recv()

    def token_rows(ref):
        return lambda q: ref.at[pl.ds(pl.multiple_of(q * share, 16), share)]

    sends = exchange(0, token_rows(stream), stream_in)
    sends += exchange(1, lambda q: gains_in, gains)
    mine = pl.ds(pl.multiple_of(tp * share, 16), share)
    my_cols = pl.ds(pl.multiple_of(tp * 256, 256), 256)
    own_rows = pl.ds(pl.multiple_of(sp * 64, 64), 64)
    stream_in[:, my_cols] = stream[mine, :]
    gains[:, my_cols] = gains_in[...]
    up[own_rows, :] = up_in[...]
    down[own_rows, :] = down_in[...]
    wout[pl.ds(pl.multiple_of(tp * 256, 256), 256), :] = wout_in[...]

    dt = per_token[0:8, :]
    log_decay = per_token[8:16, :]
    lane = lax.broadcasted_iota(jnp.int32, (8, rows), 1)
    total = log_decay
    shift = 1
    while shift < rows:
        total = total + jnp.where(lane >= shift, pltpu.roll(total, shift, 1), 0.0)
        shift *= 2
    c0 = total[0:4]
    d1 = total[4:8] - log_decay[4:8]
    all0, all1 = total[0:4, rows - 1 : rows], total[4:8, rows - 1 : rows]
    docs = per_token[16:24, :]
    own = docs[2:3]
    same_end = jnp.where(own == own[:, rows - 1 : rows], 1.0, 0.0)
    same_start = jnp.where(own == own[:, 0:1], 1.0, 0.0)
    from_prev = jnp.where(own == docs[5:6], 1.0, 0.0)
    from_next = jnp.where(own == docs[6:7], 1.0, 0.0)
    rowq[...] = jnp.zeros_like(rowq)
    rowq[C0 : C0 + 4, :] = c0
    rowq[D1 : D1 + 4, :] = d1
    rowq[W0 : W0 + 4, :] = jnp.exp(all0 - c0) * dt[0:4] * same_end
    rowq[W1 : W1 + 4, :] = jnp.exp(d1) * dt[4:8] * same_start
    rowq[A0 : A0 + 4, :] = jnp.exp(c0) * from_prev
    rowq[A1 : A1 + 4, :] = jnp.exp(all1 - d1) * from_next
    rowq[DT0 : DT0 + 4, :] = dt[0:4]
    rowq[CM : CM + 5, :] = jnp.where(docs[0:5] == own, 1.0, 0.0)
    rowq[DOC : DOC + 1, :] = own
    for t in range(tiles):
        cols[pl.ds(128 * t, 128), :] = jnp.transpose(rowq[:, 128 * t : 128 * t + 128])

    wide[8 : 8 + rows, 0:256] = hv[...].astype(F32)
    wide[8 : 8 + rows, 256:384] = em[...].astype(F32)
    wide[8 : 8 + rows, 384:512] = rm[...].astype(F32)
    for copy in halos:
        copy.wait()
    wide[0:8, 0:256] = prev_v[8:16, :].astype(F32)
    wide[0:8, 256:384] = prev_e[8:16, :].astype(F32)
    wide[0:8, 384:512] = prev_r[8:16, :].astype(F32)
    wide[8 + rows : 16 + rows, 0:256] = next_v[0:8, :].astype(F32)
    wide[8 + rows : 16 + rows, 256:384] = next_e[0:8, :].astype(F32)
    wide[8 + rows : 16 + rows, 384:512] = next_r[0:8, :].astype(F32)

    for t in range(tiles):
        lo = 128 * t
        masks = [jnp.broadcast_to(cols[lo : lo + 128, CM + o : CM + o + 1], (128, 128)) for o in range(5)]
        for g in range(4):
            acc = jnp.zeros((128, 128), F32)
            for o in range(5):
                part = wide[lo + 6 + o : lo + 134 + o, 128 * g : 128 * g + 128]
                if o != 2:
                    part = part * masks[o]
                acc = acc + taps[o : o + 1, 128 * g : 128 * g + 128] * part
            act = acc * jax.nn.sigmoid(acc)
            if g < 2:
                val[lo : lo + 128, 128 * g : 128 * g + 128] = act.astype(BF16)
            elif g == 2:
                ent32[lo : lo + 128, :] = act
                ent[lo : lo + 128, :] = act.astype(BF16)
            else:
                rdo[lo : lo + 128, :] = act.astype(BF16)

    ring.step(1)
    ring.step(2)
    state0 = jnp.zeros((STATE, 256), F32)
    state1 = jnp.zeros((STATE, 256), F32)
    for t in range(tiles):
        r = pl.ds(128 * t, 128)
        ent_t = jnp.transpose(ent32[r, :]).astype(BF16)
        v = val[r, :].astype(F32)
        state0 += jnp.dot(ent_t, (v * lanes_of(cols, r, W0)).astype(BF16), preferred_element_type=F32)
        state1 += jnp.dot(ent_t, (v * lanes_of(cols, r, W1)).astype(BF16), preferred_element_type=F32)
    for msg, state, whole in ((msg0, state0, all0), (msg1, state1, all1)):
        msg[0:STATE, :] = state.astype(BF16)
        passing = head_lanes([jnp.exp(whole[h : h + 1, :]) for h in range(4)])
        coarse = passing.astype(BF16)
        fine = (passing - coarse.astype(F32)).astype(BF16)
        row = lax.broadcasted_iota(jnp.int32, (16, 256), 0)
        both = jnp.where(row == 0, coarse.astype(F32), jnp.where(row == 1, fine.astype(F32), 0.0))
        msg[STATE : STATE + 16, :] = both.astype(BF16)

    for t in range(tiles):
        r = pl.ds(128 * t, 128)
        own_score = jnp.sum(rdo[r, :].astype(F32) * ent[r, :].astype(F32), axis=1, keepdims=True)
        local[r, :] = own_score * lanes_of(cols, r, DT0) * val[r, :].astype(F32)

    state_sends = []
    for d in range(1, REACH + 1):
        for m, (msg, got, step) in enumerate(((msg0, got0, d), (msg1, got1, -d))):
            k = 2 * (d - 1) + m
            state_sends.append(pltpu.make_async_remote_copy(
                src_ref=msg, dst_ref=got.at[d - 1],
                send_sem=state_send.at[k], recv_sem=state_recv.at[k],
                device_id=at(step), device_id_type=MESH))
    for copy in state_sends:
        copy.start()
    ring.step(3)

    low_lane = lax.broadcasted_iota(jnp.int32, (128, 128), 1) < HEAD_DIM

    def tile_step(i, _):
        r = pl.ds(pl.multiple_of(i * 128, 128), 128)
        here = rdo[r, :]
        doc_t = jnp.broadcast_to(cols[r, DOC : DOC + 1], (128, 128))
        t_index = lax.broadcasted_iota(jnp.int32, (128, 128), 0) + i * 128
        for pair in range(2):
            outs = []
            for h in (2 * pair, 2 * pair + 1):
                ct = jnp.broadcast_to(cols[r, C0 + h : C0 + h + 1], (128, 128))
                dd = jnp.broadcast_to(cols[r, D1 + h : D1 + h + 1], (128, 128))
                for j in range(tiles):
                    s = pl.ds(128 * j, 128)
                    if h == 0:
                        score = lax.dot_general(here, ent[s, :], (((1,), (1,)), ((), ())), preferred_element_type=F32)
                        score = jnp.where(doc_t == per_token[18:19, 128 * j : 128 * j + 128], score, 0.0)
                        weight[1, :, 128 * j : 128 * j + 128] = score
                    score = weight[1, :, 128 * j : 128 * j + 128]
                    s_index = lax.broadcasted_iota(jnp.int32, (128, 128), 1) + 128 * j
                    spread = jnp.minimum(ct - rowq[C0 + h : C0 + h + 1, 128 * j : 128 * j + 128],
                                         rowq[D1 + h : D1 + h + 1, 128 * j : 128 * j + 128] - dd)
                    step = jnp.where(s_index < t_index, per_token[h : h + 1, 128 * j : 128 * j + 128],
                                     per_token[4 + h : 5 + h, 128 * j : 128 * j + 128])
                    weight[0, :, 128 * j : 128 * j + 128] = score * jnp.exp(spread) * step
                outs.append(jnp.dot(weight[0].astype(BF16), val[:, 128 * pair : 128 * pair + 128],
                                    preferred_element_type=F32))
            local[r, 128 * pair : 128 * pair + 128] += jnp.where(low_lane, outs[0], outs[1])
        return 0

    lax.fori_loop(0, tiles // 2, tile_step, 0)
    ring.step(4)
    lax.fori_loop(tiles // 2, tiles, tile_step, 0)
    ring.step(5)
    ring.step(6)

    for copy in state_sends:
        copy.wait()
    carried = []
    for m, got in enumerate((got0, got1)):
        through = jnp.ones((1, 256), F32)
        state = jnp.zeros((STATE, 256), F32)
        for d in range(1, REACH + 1):
            state = state + got[d - 1, 0:STATE, :].astype(F32) * (through * source_mask[REACH * m + d - 1])
            tail = got[d - 1, STATE : STATE + 16, :].astype(F32)
            through = through * (tail[0:1] + tail[1:2])
        carried.append(state.astype(BF16))

    for t in range(tiles):
        r = pl.ds(128 * t, 128)
        here = rdo[r, :]
        y = local[r, :]
        y += jnp.dot(here, carried[0], preferred_element_type=F32) * lanes_of(cols, r, A0)
        y += jnp.dot(here, carried[1], preferred_element_type=F32) * lanes_of(cols, r, A1)
        z = gate[r, :].astype(F32)
        y = y * (z * jax.nn.sigmoid(z))
        y = y * lax.rsqrt(jnp.mean(y * y, axis=1, keepdims=True) + norm_eps)
        norm_out[r, :] = (y * gain[...]).astype(BF16)

    norm_in[:, my_cols] = norm_out[mine, :]
    sends += exchange(2, token_rows(norm_out), norm_in)
    ring.step(7)
    ring.step(8)
    wo.relay()
    exchanged(0, stream_in)
    exchanged(1, gains)
    exchanged(2, norm_in)
    ring.step(9)
    wo.far()
    for k in (2, 5, 6, 7):
        wo.sibling(k)
    for n in range(4):
        c = pl.ds(512 * n, 512)
        first[:, c] = (resid_scale * stream_in[:, c].astype(F32)
                       + jnp.dot(norm_in[...], wout[:, c], preferred_element_type=F32))
    f = first[...]
    mean = jnp.sum(f, axis=1, keepdims=True) * (1.0 / D)
    var = jnp.sum(f * f, axis=1, keepdims=True) * (1.0 / D) - mean * mean
    tok[mine, :] = ((f - mean) * lax.rsqrt(var + norm_eps) * gains[0:1, :]).astype(BF16)
    tg = TpGather(tok.at[mine], tok, share, tk_s, tk_r, sp, tp)
    tg.begin()
    for n in range(10, 15):
        ring.step(n)
    ring.finish()

    x, c = tp // 2, lax.rem(tp, 2)

    def chip(d):
        return lax.rem(x + d + 4, 4)

    def chunk_rows(d):
        return pl.ds(pl.multiple_of(chip(d) * 2 * share, 64), 2 * share)

    order = (0, -1, 1, 2)
    away = (1, -1, 2)

    def compute(k):
        chunk = tok[chunk_rows(order[k]), :]
        for n in range(4):
            hidden = jnp.maximum(jnp.dot(chunk, up[:, 256 * n : 256 * n + 256], preferred_element_type=F32), 0.0)
            squares[:, 256 * n : 256 * n + 256] = (hidden * hidden).astype(BF16)
        sq = squares[...]
        for e in range(4):
            for other in (True, False):
                q = 2 * e + (1 - c if other else c)
                w = down[pl.ds(pl.multiple_of(q * 256, 256), 256), :]
                part = lax.dot_general(sq, w, (((1,), (1,)), ((), ())), preferred_element_type=F32)
                if other:
                    sib_out[k, e] = part.astype(BF16)
                else:
                    own_part[k % 2, e] = part
        copy = copy_to(sib_out.at[k], sib_in.at[k], sb_s.at[k], sb_r.at[k], (sp, 2 * x + 1 - c))
        copy.start()
        return copy

    def pass_on(k, copy):
        copy.wait()
        local[chunk_rows(order[k]), :] = own_part[k % 2, x] + sib_in[k, x].astype(F32)
        for e, d in enumerate(away):
            outgoing[k, e] = (own_part[k % 2, chip(d)] + sib_in[k, chip(d)].astype(F32)).astype(BF16)
        for e, d in enumerate(away):
            push = copy_to(outgoing.at[k, e], parts.at[e, chunk_rows(order[k])], rs_s.at[k, e], rs_r.at[k, e],
                           (sp, 2 * chip(d) + c))
            push.start()
            sends.append(push)

    tg.sibling(2)
    copy0 = compute(0)
    tg.relay()
    tg.sibling(5)
    copy1 = compute(1)
    pass_on(0, copy0)
    tg.sibling(6)
    copy2 = compute(2)
    pass_on(1, copy1)
    tg.far()
    tg.sibling(7)
    copy3 = compute(3)
    pass_on(2, copy2)
    pass_on(3, copy3)
    for k in range(4):
        for e, d in enumerate(away):
            r = parts.at[e, chunk_rows(order[k] - d)]
            copy_to(r, r, rs_s.at[k, e], rs_r.at[k, e], (sp, 2 * chip(d) + c)).wait_recv()

    lane_at = lax.broadcasted_iota(jnp.int32, (128, 128), 1)
    for t in range(tiles):
        r = pl.ds(128 * t, 128)
        y = local[r, :] + resid_scale * tok[r, my_cols].astype(F32)
        for e in range(3):
            y += parts[e, r, :].astype(F32)
        local[r, :] = y
        one = jnp.sum(y, axis=1, keepdims=True)
        two = jnp.sum(y * y, axis=1, keepdims=True)
        pair = jnp.where(lane_at == 0, one, jnp.where(lane_at == 1, two, 0.0))
        stat_out[:, 128 * t : 128 * t + 128] = jnp.transpose(pair)[0:8, :]
    for d in range(1, n_tp):
        push = copy_to(stat_out, stat_in.at[d - 1], st_s.at[d - 1], st_r.at[d - 1], (sp, peer(d)))
        push.start()
        sends.append(push)
    for copy in sends + ring.sent + wo.sent + tg.sent:
        copy.wait_send()
    stats = stat_out[...]
    for d in range(1, n_tp):
        copy_to(stat_in.at[d - 1], stat_in.at[d - 1], st_s.at[d - 1], st_r.at[d - 1], (sp, peer(d))).wait_recv()
        stats += stat_in[d - 1]
    mean = stats[0:1] * (1.0 / D)
    scale = lax.rsqrt(stats[1:2] * (1.0 / D) - mean * mean + norm_eps)
    rowq[0:1, :] = mean
    rowq[1:2, :] = scale
    for t in range(tiles):
        r = pl.ds(128 * t, 128)
        both = jnp.transpose(rowq[:, 128 * t : 128 * t + 128])
        out[r, :] = ((local[r, :] - both[:, 0:1]) * both[:, 1:2] * last_gain[...]).astype(BF16)


def per_device(hv, em, rm, gate, step, sudden, document_index, rate, bias, tv, te, tr, gain,
               out_weight, stream, first_gain, last_gain, up_in, down_in):
    rows = hv.shape[0]
    n_sp = lax.axis_size("sp")
    sp = lax.axis_index("sp")
    raw, sud = step.astype(F32).T, sudden.T
    dts, lds = [], []
    for k in range(2):
        dt = jax.nn.softplus(raw + bias[k][:, None])
        dts.append(dt)
        lds.append(-jnp.exp(rate[k])[:, None] * dt + sud)
    pad = jnp.pad(document_index, 3, constant_values=-1).astype(F32)
    window = lax.dynamic_slice_in_dim(pad, sp * rows, rows + 6)
    shifted = [window[1 + o : 1 + o + rows][None] for o in range(5)]
    before = jnp.broadcast_to(window[2:3], (1, rows))
    after = jnp.broadcast_to(window[rows + 3 : rows + 4], (1, rows))
    per_token = jnp.concatenate(dts + lds + shifted + [before, after, jnp.zeros((1, rows), F32)], axis=0)
    grid = document_index.reshape(n_sp, rows)
    last = lax.dynamic_slice_in_dim(jnp.pad(grid[:, rows - 1], REACH, constant_values=-1), sp, REACH)[::-1]
    first = lax.dynamic_slice_in_dim(jnp.pad(grid[:, 0], REACH, constant_values=-1), sp + REACH + 1, REACH)
    mask = jnp.concatenate([(last == last[0]) & (last >= 0), (first == first[0]) & (first >= 0)]).astype(F32)
    taps = jnp.pad(jnp.concatenate([tv, te, tr], axis=1).astype(F32), ((0, 3), (0, 0)))
    gains = jnp.broadcast_to(first_gain[None, :], (8, 256))
    vmem = pl.BlockSpec(memory_space=pltpu.VMEM)
    dma = pltpu.SemaphoreType.DMA
    share = rows // 8
    return pl.pallas_call(
        layer_kernel,
        out_shape=jax.ShapeDtypeStruct((rows, 256), BF16),
        in_specs=[vmem] * 5 + [pl.BlockSpec(memory_space=pltpu.SMEM)] + [vmem] * 8,
        out_specs=vmem,
        scratch_shapes=[
            pltpu.VMEM((16, 256), BF16), pltpu.VMEM((16, 128), BF16), pltpu.VMEM((16, 128), BF16),
            pltpu.VMEM((16, 256), BF16), pltpu.VMEM((16, 128), BF16), pltpu.VMEM((16, 128), BF16),
            pltpu.VMEM((rows + 16, 512), F32),
            pltpu.VMEM((128, rows), F32),
            pltpu.VMEM((rows, 128), F32),
            pltpu.VMEM((rows, 256), BF16), pltpu.VMEM((rows, 128), BF16), pltpu.VMEM((rows, 128), F32),
            pltpu.VMEM((rows, 128), BF16),
            pltpu.VMEM((2, 128, rows), F32),
            pltpu.VMEM((rows, 256), F32),
            pltpu.VMEM((STATE + 16, 256), BF16), pltpu.VMEM((STATE + 16, 256), BF16),
            pltpu.VMEM((REACH, STATE + 16, 256), BF16), pltpu.VMEM((REACH, STATE + 16, 256), BF16),
            pltpu.VMEM((D, 1024), BF16), pltpu.VMEM((D, 1024), BF16), pltpu.VMEM((D, D), BF16),
            pltpu.VMEM((rows, 256), BF16), pltpu.VMEM((share, D), BF16), pltpu.VMEM((share, D), BF16),
            pltpu.VMEM((8, D), F32), pltpu.VMEM((share, D), F32), pltpu.VMEM((rows, D), BF16),
            pltpu.VMEM((2 * share, 1024), BF16),
            pltpu.VMEM((4, 4, 2 * share, 256), BF16), pltpu.VMEM((4, 4, 2 * share, 256), BF16),
            pltpu.VMEM((2, 4, 2 * share, 256), F32), pltpu.VMEM((4, 3, 2 * share, 256), BF16),
            pltpu.VMEM((3, rows, 256), BF16), pltpu.VMEM((8, rows), F32), pltpu.VMEM((7, 8, rows), F32),
            dma((6,)), dma((6,)), dma((2 * REACH,)), dma((2 * REACH,)),
            dma((2,)), dma((2,)), dma((2,)), dma((2,)), dma((2, 4, 4)), dma((2, 4, 4)),
            dma((2, 4)), dma((2, 4)), dma((8, 2)), dma((8, 2)), dma((8, 2)), dma((8, 2)),
            dma((8,)), dma((8,)), dma((8,)), dma((8,)), dma((3, 7)), dma((3, 7)),
            dma((4,)), dma((4,)), dma((4, 3)), dma((4, 3)), dma((7,)), dma((7,)),
        ],
        compiler_params=pltpu.CompilerParams(
            collective_id=0, has_side_effects=True, vmem_limit_bytes=60 * 1024 * 1024),
        cost_estimate=pl.CostEstimate(flops=9_000_000_000, bytes_accessed=8_000_000, transcendentals=0),
        name="layer",
    )(hv, em, rm, gate, per_token, mask, taps, gain[None, :], up_in, down_in, out_weight, stream, gains,
      last_gain[None, :])


SPECS = (
    P("sp", "tp"), P("sp", "tp"), P("sp", "tp"), P("sp", "tp"), P("sp", "tp"), P("sp", "tp"), P(),
    P(None, "tp"), P(None, "tp"), P(None, "tp"), P(None, "tp"), P(None, "tp"), P("tp"),
    P("tp", None), P("sp", "tp"), P("tp"), P("tp"), P("sp", "tp"), P("sp", "tp"),
)


def solution(mesh):
    return jax.shard_map(per_device, mesh=mesh, in_specs=SPECS, out_specs=P("sp", "tp"), check_vma=False)
```

```python
import functools

import jax
import jax.numpy as jnp
from jax import lax
from jax.experimental import pallas as pl
from jax.experimental.pallas import tpu as pltpu
from jax.sharding import PartitionSpec as P

D = 2048
HEAD_DIM = 64
STATE = 128
REACH = 8
MESH = pl.DeviceIdType.MESH
norm_eps = 1e-05
resid_scale = 1.4142135623730951
F32 = jnp.float32
BF16 = jnp.bfloat16


def lanes_of(cols, rows, base):
    n = rows.size
    low = lax.broadcasted_iota(jnp.int32, (n, 128), 1) < HEAD_DIM
    halves = []
    for k in (0, 2):
        a = jnp.broadcast_to(cols[rows, base + k : base + k + 1], (n, 128))
        b = jnp.broadcast_to(cols[rows, base + k + 1 : base + k + 2], (n, 128))
        halves.append(jnp.where(low, a, b))
    return jnp.concatenate(halves, axis=1)


def head_lanes(column):
    return jnp.concatenate([jnp.broadcast_to(c, (1, HEAD_DIM)) for c in column], axis=1)


C0, D1, W0, W1, A0, A1, DT0, CM, DOC = 0, 4, 8, 12, 16, 20, 24, 28, 33


def copy_to(src, dst, send, recv, device):
    return pltpu.make_async_remote_copy(src_ref=src, dst_ref=dst, send_sem=send, recv_sem=recv,
                                        device_id=device, device_id_type=MESH)


class WeightRing:
    def __init__(self, up_in, down_in, up, down, sems, sp, tp):
        (self.uy_s, self.uy_r, self.uh_s, self.uh_r, self.uz_s, self.uz_r,
         self.dz_s, self.dz_r, self.dy_s, self.dy_r, self.dh_s, self.dh_r) = sems
        self.up_in, self.down_in, self.up, self.down, self.tp = up_in, down_in, up, down, tp
        self.y, self.z = lax.rem(sp, 4), sp // 4
        self.sent = []

    def dev(self, dz, dy):
        return (lax.rem(self.z + dz + 8, 8) * 4 + lax.rem(self.y + dy + 4, 4), self.tp)

    def rows(self, dz, dy, low=0, count=64):
        shard = lax.rem(self.z + dz + 8, 8) * 4 + lax.rem(self.y + dy + 4, 4)
        return pl.ds(pl.multiple_of(shard * 64 + low, 32), count)

    def send(self, src, dst, send, recv, device):
        copy = copy_to(src, dst, send, recv, device)
        copy.start()
        self.sent.append(copy)

    def arrived(self, dst, send, recv):
        copy_to(dst, dst, send, recv, self.dev(1, 0)).wait_recv()

    def up_z(self, s, p, receive):
        for m, sign in enumerate((1, -1)):
            low, count = (32 * m, 32) if s == 3 else (0, 64)
            if receive:
                r = self.rows(-sign * (s + 1), p, low, count)
                self.arrived(self.up.at[r], self.uz_s.at[m, s, p], self.uz_r.at[m, s, p])
            else:
                r = self.rows(-sign * s, p, low, count)
                src = self.up_in if s == 0 and p == 0 else self.up.at[r]
                self.send(src, self.up.at[r], self.uz_s.at[m, s, p], self.uz_r.at[m, s, p], self.dev(sign, 0))

    def down_z(self, s, receive):
        for m, sign in enumerate((1, -1)):
            low, count = (32 * m, 32) if s == 3 else (0, 64)
            if receive:
                r = self.rows(-sign * (s + 1), 0, low, count)
                self.arrived(self.down.at[r], self.dz_s.at[m, s], self.dz_r.at[m, s])
            else:
                r = self.rows(-sign * s, 0, low, count)
                src = self.down_in if s == 0 else self.down.at[r]
                self.send(src, self.down.at[r], self.dz_s.at[m, s], self.dz_r.at[m, s], self.dev(sign, 0))

    def planes(self, s):
        return [(0, 0)] if s == 0 else [(7, 4)] if s == 4 else [(2 * s - 1, -s), (2 * s, s)]

    def down_y(self, s):
        for k, dz in self.planes(s):
            for m, sign in enumerate((1, -1)):
                r = self.rows(dz, 0)
                src = self.down_in if s == 0 else self.down.at[r]
                self.send(src, self.down.at[r], self.dy_s.at[k, m], self.dy_r.at[k, m], self.dev(0, sign))

    def down_half(self, s, receive):
        for k, dz in self.planes(s):
            for m, sign in enumerate((1, -1)):
                if receive:
                    r = self.rows(dz, -2 * sign, 32 * m, 32)
                    self.arrived(self.down.at[r], self.dh_s.at[k, m], self.dh_r.at[k, m])
                else:
                    self.arrived(self.down.at[self.rows(dz, -sign)], self.dy_s.at[k, m], self.dy_r.at[k, m])
                    r = self.rows(dz, -sign, 32 * m, 32)
                    self.send(self.down.at[r], self.down.at[r], self.dh_s.at[k, m], self.dh_r.at[k, m],
                              self.dev(0, sign))

    def up_step(self, n):
        s, part = divmod(n, 3)
        if part == 0:
            if s == 0:
                for m, sign in enumerate((1, -1)):
                    self.send(self.up_in, self.up.at[self.rows(0, 0)], self.uy_s.at[m], self.uy_r.at[m],
                              self.dev(0, sign))
            else:
                self.up_z(s - 1, 0, True)
            if s < 4:
                self.up_z(s, 0, False)
        elif part == 1:
            if s == 0:
                for m, sign in enumerate((1, -1)):
                    self.arrived(self.up.at[self.rows(0, -sign)], self.uy_s.at[m], self.uy_r.at[m])
                    r = self.rows(0, -sign, 32 * m, 32)
                    self.send(self.up.at[r], self.up.at[r], self.uh_s.at[m], self.uh_r.at[m], self.dev(0, sign))
            else:
                self.up_z(s - 1, 1, True)
                self.up_z(s - 1, 3, True)
            if s < 4:
                self.up_z(s, 1, False)
                self.up_z(s, 3, False)
        else:
            if s == 0:
                for m, sign in enumerate((1, -1)):
                    self.arrived(self.up.at[self.rows(0, -2 * sign, 32 * m, 32)], self.uh_s.at[m], self.uh_r.at[m])
            else:
                self.up_z(s - 1, 2, True)
            if s < 4:
                self.up_z(s, 2, False)

    def down_step(self, s):
        if s > 0:
            self.down_z(s - 1, True)
        if s < 4:
            self.down_z(s, False)
        self.down_y(s)

    def finish(self):
        for s in range(5):
            self.down_half(s, True)


class TpGather:
    def __init__(self, own, buf, size, send, recv, sp, tp):
        self.own, self.buf, self.size, self.s, self.r, self.sp = own, buf, size, send, recv, sp
        self.x, self.c = tp // 2, lax.rem(tp, 2)
        self.sent = []

    def slot(self, dx, other):
        return lax.rem(self.x + dx + 4, 4) * 2 + (1 - self.c if other else self.c)

    def rows(self, dx, other, half=None):
        low, count = (0, self.size) if half is None else (half * (self.size // 2), self.size // 2)
        return self.buf.at[pl.ds(pl.multiple_of(self.slot(dx, other) * self.size + low, 16), count)]

    def send(self, src, dst, k, dx, other):
        copy = copy_to(src, dst, self.s.at[k], self.r.at[k], (self.sp, self.slot(dx, other)))
        copy.start()
        self.sent.append(copy)

    def arrived(self, dst, k):
        copy_to(dst, dst, self.s.at[k], self.r.at[k], (self.sp, self.slot(0, True))).wait_recv()

    def begin(self):
        mine = self.rows(0, False)
        self.send(self.own, mine, 0, 1, False)
        self.send(self.own, mine, 1, -1, False)
        self.send(self.own, mine, 2, 0, True)

    def relay(self):
        left, right = self.rows(-1, False), self.rows(1, False)
        self.arrived(left, 0)
        self.send(self.rows(-1, False, 0), self.rows(-1, False, 0), 3, 1, False)
        self.send(left, left, 5, 0, True)
        self.arrived(right, 1)
        self.send(self.rows(1, False, 1), self.rows(1, False, 1), 4, -1, False)
        self.send(right, right, 6, 0, True)

    def far(self):
        self.arrived(self.rows(2, False, 0), 3)
        self.arrived(self.rows(2, False, 1), 4)
        self.send(self.rows(2, False), self.rows(2, False), 7, 0, True)

    def sibling(self, k):
        self.arrived(self.rows({2: 0, 5: -1, 6: 1, 7: 2}[k], True), k)


def layer_kernel(
    hv, em, rm, gate, step_in, sudden_in, docs_in, rate, bias, tap_v, tap_e, tap_r, gain, up_in, down_in, wout_in,
    stream, first_gain, last_gain, out,
    prev_v, prev_e, prev_r, next_v, next_e, next_r,
    per_token, gains_in, wide, rowq, cols, val, ent, ent32, rdo, weight, local,
    msg0, msg1, got0, got1, wmsg0, wmsg1, wgot0, wgot1, states,
    up, down, wout, norm_out, norm_in, stream_in, gains, first, tok, squares,
    sib_out, sib_in, own_part, outgoing, parts, relay, stat_out, stat_in,
    halo_send, halo_recv, state_send, state_recv,
    uy_s, uy_r, uh_s, uh_r, uz_s, uz_r, dz_s, dz_r, dy_s, dy_r, dh_s, dh_r,
    wo_s, wo_r, tk_s, tk_r, ex_s, ex_r, sb_s, sb_r, rs_s, rs_r, st_s, st_r,
):
    sp, tp = lax.axis_index("sp"), lax.axis_index("tp")
    n_sp = lax.axis_size("sp")
    n_tp = lax.axis_size("tp")
    rows = hv.shape[0]
    tiles = rows // 128
    share = rows // n_tp

    def at(d):
        return (lax.rem(sp + d + n_sp, n_sp), tp)

    def peer(d):
        return lax.rem(tp + d + n_tp, n_tp)

    gains_in[...] = jnp.broadcast_to(first_gain[...].reshape(1, 256), (8, 256))
    barrier = pltpu.get_barrier_semaphore()
    for d in range(1, REACH + 1):
        for s in (d, -d):
            pl.semaphore_signal(barrier, inc=1, device_id=at(s), device_id_type=MESH)
    for d in range(1, n_tp):
        pl.semaphore_signal(barrier, inc=1, device_id=(sp, peer(d)), device_id_type=MESH)
    pl.semaphore_wait(barrier, 2 * REACH + n_tp - 1)

    halos = []
    for k, (src, low, high) in enumerate(((hv, prev_v, next_v), (em, prev_e, next_e), (rm, prev_r, next_r))):
        for m, (start, dst, step) in enumerate(((rows - 16, low, 1), (0, high, -1))):
            halos.append(copy_to(src.at[pl.ds(start, 16)], dst, halo_send.at[2 * k + m], halo_recv.at[2 * k + m],
                                 at(step)))
    for copy in halos:
        copy.start()
    ring = WeightRing(up_in, down_in, up, down,
                      (uy_s, uy_r, uh_s, uh_r, uz_s, uz_r, dz_s, dz_r, dy_s, dy_r, dh_s, dh_r), sp, tp)
    ring.down_step(0)
    ring.up_step(0)
    wo = TpGather(wout_in, wout, 256, wo_s, wo_r, sp, tp)
    wo.begin()

    def my_lanes(ref, q):
        return ref.at[:, pl.ds(pl.multiple_of(q * 256, 256), 256)]

    def exchange(k, src_of, dst):
        sent = []
        for d in range(1, n_tp):
            q = peer(d)
            copy = copy_to(src_of(q), my_lanes(dst, tp), ex_s.at[k, d - 1], ex_r.at[k, d - 1], (sp, q))
            copy.start()
            sent.append(copy)
        return sent

    def exchanged(k, dst):
        for d in range(1, n_tp):
            r = my_lanes(dst, peer(-d))
            copy_to(r, r, ex_s.at[k, d - 1], ex_r.at[k, d - 1], (sp, peer(d))).wait_recv()

    def token_rows(ref):
        return lambda q: ref.at[pl.ds(pl.multiple_of(q * share, 16), share)]

    sends = exchange(0, token_rows(stream), stream_in)
    sends += exchange(1, lambda q: gains_in, gains)
    mine = pl.ds(pl.multiple_of(tp * share, 16), share)
    my_cols = pl.ds(pl.multiple_of(tp * 256, 256), 256)
    own_rows = pl.ds(pl.multiple_of(sp * 64, 64), 64)
    stream_in[:, my_cols] = stream[mine, :]
    gains[:, my_cols] = gains_in[...]
    up[own_rows, :] = up_in[...]
    down[own_rows, :] = down_in[...]
    wout[pl.ds(pl.multiple_of(tp * 256, 256), 256), :] = wout_in[...]

    raw = step_in[...].astype(F32)
    sudden = sudden_in[...]

    def eight(ref):
        return jnp.concatenate([jnp.full((1, rows), ref[k, h], F32) for k in range(2) for h in range(4)], axis=0)

    before_softplus = jnp.concatenate([raw, raw], axis=0) + eight(bias)
    per_token[0:8, :] = jnp.maximum(before_softplus, 0.0) + jnp.log1p(jnp.exp(-jnp.abs(before_softplus)))
    per_token[8:16, :] = -jnp.exp(eight(rate)) * per_token[0:8, :] + jnp.concatenate([sudden, sudden], axis=0)

    def doc_at(row, lane_no):
        return docs_in[pl.ds(row, 1), lane_no : lane_no + 1].astype(F32)

    own_doc = jnp.concatenate([docs_in[pl.ds(tiles * sp + t, 1), :] for t in range(tiles)], axis=1).astype(F32)
    own8 = jnp.broadcast_to(own_doc, (8, rows))
    low_row, high_row = jnp.maximum(tiles * sp - 1, 0), jnp.minimum(tiles * sp + tiles, tiles * n_sp - 1)
    prev_two, prev_one = (jnp.where(sp > 0, doc_at(low_row, k), -1.0) for k in (126, 127))
    next_one, next_two = (jnp.where(sp < n_sp - 1, doc_at(high_row, k), -1.0) for k in (0, 1))
    lane8 = lax.broadcasted_iota(jnp.int32, (8, rows), 1)
    back_one = jnp.where(lane8 == 0, prev_one, pltpu.roll(own8, 1, 1))
    back_two = jnp.where(lane8 == 0, prev_two, jnp.where(lane8 == 1, prev_one, pltpu.roll(own8, 2, 1)))
    on_one = jnp.where(lane8 == rows - 1, next_one, pltpu.roll(own8, rows - 1, 1))
    on_two = jnp.where(lane8 == rows - 1, next_two, jnp.where(lane8 == rows - 2, next_one, pltpu.roll(own8, rows - 2, 1)))
    for k, row in enumerate((back_two, back_one, own8, on_one, on_two)):
        per_token[16 + k : 17 + k, :] = row[0:1]
    per_token[21:22, :] = jnp.broadcast_to(prev_one, (1, rows))
    per_token[22:23, :] = jnp.broadcast_to(next_one, (1, rows))
    per_token[23:24, :] = jnp.zeros((1, rows), F32)

    def last_doc(d):
        return doc_at(tiles * lax.rem(sp - d + n_sp, n_sp) + tiles - 1, 127)

    def first_doc(d):
        return doc_at(tiles * lax.rem(sp + d, n_sp), 0)

    source_mask = []
    for edge, room in ((last_doc, sp), (first_doc, n_sp - 1 - sp)):
        for d, to in ((1, 0), (2, 0), (4, 1), (7, 1)):
            source_mask.append(jnp.where((edge(d) == edge(to)) & (room >= d), 1.0, 0.0))

    dt = per_token[0:8, :]
    log_decay = per_token[8:16, :]
    lane = lax.broadcasted_iota(jnp.int32, (8, rows), 1)
    total = log_decay
    shift = 1
    while shift < rows:
        total = total + jnp.where(lane >= shift, pltpu.roll(total, shift, 1), 0.0)
        shift *= 2
    c0 = total[0:4]
    d1 = total[4:8] - log_decay[4:8]
    all0, all1 = total[0:4, rows - 1 : rows], total[4:8, rows - 1 : rows]
    docs = per_token[16:24, :]
    own = docs[2:3]
    same_end = jnp.where(own == own[:, rows - 1 : rows], 1.0, 0.0)
    same_start = jnp.where(own == own[:, 0:1], 1.0, 0.0)
    from_prev = jnp.where(own == docs[5:6], 1.0, 0.0)
    from_next = jnp.where(own == docs[6:7], 1.0, 0.0)
    rowq[...] = jnp.zeros_like(rowq)
    rowq[C0 : C0 + 4, :] = c0
    rowq[D1 : D1 + 4, :] = d1
    rowq[W0 : W0 + 4, :] = jnp.exp(all0 - c0) * dt[0:4] * same_end
    rowq[W1 : W1 + 4, :] = jnp.exp(d1) * dt[4:8] * same_start
    rowq[A0 : A0 + 4, :] = jnp.exp(c0) * from_prev
    rowq[A1 : A1 + 4, :] = jnp.exp(all1 - d1) * from_next
    rowq[DT0 : DT0 + 4, :] = dt[0:4]
    rowq[CM : CM + 5, :] = jnp.where(docs[0:5] == own, 1.0, 0.0)
    rowq[DOC : DOC + 1, :] = own
    for t in range(tiles):
        cols[pl.ds(128 * t, 128), :] = jnp.transpose(rowq[:, 128 * t : 128 * t + 128])

    wide[8 : 8 + rows, 0:256] = hv[...].astype(F32)
    wide[8 : 8 + rows, 256:384] = em[...].astype(F32)
    wide[8 : 8 + rows, 384:512] = rm[...].astype(F32)
    for copy in halos:
        copy.wait()
    wide[0:8, 0:256] = prev_v[8:16, :].astype(F32)
    wide[0:8, 256:384] = prev_e[8:16, :].astype(F32)
    wide[0:8, 384:512] = prev_r[8:16, :].astype(F32)
    wide[8 + rows : 16 + rows, 0:256] = next_v[0:8, :].astype(F32)
    wide[8 + rows : 16 + rows, 256:384] = next_e[0:8, :].astype(F32)
    wide[8 + rows : 16 + rows, 384:512] = next_r[0:8, :].astype(F32)

    whole_taps = tap_v[...].astype(F32)
    taps = (whole_taps[:, 0:128], whole_taps[:, 128:256], tap_e[...].astype(F32), tap_r[...].astype(F32))
    for t in range(tiles):
        lo = 128 * t
        masks = [jnp.broadcast_to(cols[lo : lo + 128, CM + o : CM + o + 1], (128, 128)) for o in range(5)]
        for g in range(4):
            acc = jnp.zeros((128, 128), F32)
            for o in range(5):
                part = wide[lo + 6 + o : lo + 134 + o, 128 * g : 128 * g + 128]
                if o != 2:
                    part = part * masks[o]
                acc = acc + taps[g][o : o + 1] * part
            act = acc * jax.nn.sigmoid(acc)
            if g < 2:
                val[lo : lo + 128, 128 * g : 128 * g + 128] = act.astype(BF16)
            elif g == 2:
                ent32[lo : lo + 128, :] = act
                ent[lo : lo + 128, :] = act.astype(BF16)
            else:
                rdo[lo : lo + 128, :] = act.astype(BF16)

    ring.up_step(1)
    ring.down_step(1)
    ring.down_half(0, False)
    state0 = jnp.zeros((STATE, 256), F32)
    state1 = jnp.zeros((STATE, 256), F32)
    for t in range(tiles):
        r = pl.ds(128 * t, 128)
        ent_t = jnp.transpose(ent32[r, :]).astype(BF16)
        v = val[r, :].astype(F32)
        state0 += jnp.dot(ent_t, (v * lanes_of(cols, r, W0)).astype(BF16), preferred_element_type=F32)
        state1 += jnp.dot(ent_t, (v * lanes_of(cols, r, W1)).astype(BF16), preferred_element_type=F32)
    def fill(msg, state, passing):
        msg[0:STATE, :] = state.astype(BF16)
        coarse = passing.astype(BF16)
        fine = (passing - coarse.astype(F32)).astype(BF16)
        row = lax.broadcasted_iota(jnp.int32, (16, 256), 0)
        both = jnp.where(row == 0, coarse.astype(F32), jnp.where(row == 1, fine.astype(F32), 0.0))
        msg[STATE : STATE + 16, :] = both.astype(BF16)

    def passing_of(msg):
        tail = msg[STATE : STATE + 16, :].astype(F32)
        return tail[0:1] + tail[1:2]

    pass_own = [head_lanes([jnp.exp(whole[h : h + 1, :]) for h in range(4)]) for whole in (all0, all1)]
    for m, (msg, state) in enumerate(((msg0, state0), (msg1, state1))):
        states[m] = state
        fill(msg, state, pass_own[m])

    for t in range(tiles):
        r = pl.ds(128 * t, 128)
        own_score = jnp.sum(rdo[r, :].astype(F32) * ent[r, :].astype(F32), axis=1, keepdims=True)
        local[r, :] = own_score * lanes_of(cols, r, DT0) * val[r, :].astype(F32)

    near_sends = []
    for k, d in enumerate((1, 2)):
        for m, (msg, got, step) in enumerate(((msg0, got0, d), (msg1, got1, -d))):
            near_sends.append(copy_to(msg, got.at[k], state_send.at[2 * k + m], state_recv.at[2 * k + m], at(step)))
    for copy in near_sends:
        copy.start()

    low_lane = lax.broadcasted_iota(jnp.int32, (128, 128), 1) < HEAD_DIM

    def tile_step(i, _):
        r = pl.ds(pl.multiple_of(i * 128, 128), 128)
        here = rdo[r, :]
        doc_t = jnp.broadcast_to(cols[r, DOC : DOC + 1], (128, 128))
        t_index = lax.broadcasted_iota(jnp.int32, (128, 128), 0) + i * 128
        for pair in range(2):
            outs = []
            for h in (2 * pair, 2 * pair + 1):
                ct = jnp.broadcast_to(cols[r, C0 + h : C0 + h + 1], (128, 128))
                dd = jnp.broadcast_to(cols[r, D1 + h : D1 + h + 1], (128, 128))
                for j in range(tiles):
                    s = pl.ds(128 * j, 128)
                    if h == 0:
                        score = lax.dot_general(here, ent[s, :], (((1,), (1,)), ((), ())), preferred_element_type=F32)
                        score = jnp.where(doc_t == per_token[18:19, 128 * j : 128 * j + 128], score, 0.0)
                        weight[1, :, 128 * j : 128 * j + 128] = score
                    score = weight[1, :, 128 * j : 128 * j + 128]
                    s_index = lax.broadcasted_iota(jnp.int32, (128, 128), 1) + 128 * j
                    spread = jnp.minimum(ct - rowq[C0 + h : C0 + h + 1, 128 * j : 128 * j + 128],
                                         rowq[D1 + h : D1 + h + 1, 128 * j : 128 * j + 128] - dd)
                    step = jnp.where(s_index < t_index, per_token[h : h + 1, 128 * j : 128 * j + 128],
                                     per_token[4 + h : 5 + h, 128 * j : 128 * j + 128])
                    weight[0, :, 128 * j : 128 * j + 128] = score * jnp.exp(spread) * step
                outs.append(jnp.dot(weight[0].astype(BF16), val[:, 128 * pair : 128 * pair + 128],
                                    preferred_element_type=F32))
            local[r, 128 * pair : 128 * pair + 128] += jnp.where(low_lane, outs[0], outs[1])
        return 0

    lax.fori_loop(0, tiles // 2, tile_step, 0)
    ring.up_step(2)
    for copy in near_sends:
        copy.wait()
    for m, (got, wmsg) in enumerate(((got0, wmsg0), (got1, wmsg1))):
        through = [pass_own[m]]
        for k in range(2):
            through.append(through[k] * passing_of(got.at[k]))
        window = states[m]
        for k in range(2):
            window += got[k, 0:STATE, :].astype(F32) * (through[k] * source_mask[4 * m + k])
        fill(wmsg, window, through[2])
    far_sends = []
    lax.fori_loop(tiles // 2, tiles // 2 + 1, tile_step, 0)
    for k, d in enumerate((1, 4, 7)):
        for m, (wmsg, wgot, step) in enumerate(((wmsg0, wgot0, d), (wmsg1, wgot1, -d))):
            n = 4 + 2 * k + m
            far_sends.append(copy_to(wmsg, wgot.at[k], state_send.at[n], state_recv.at[n], at(step)))
    for copy in far_sends:
        copy.start()
    lax.fori_loop(tiles // 2 + 1, tiles, tile_step, 0)
    ring.up_step(3)
    ring.down_step(2)
    ring.down_half(1, False)
    for copy in far_sends:
        copy.wait()
    carried = []
    for m, wgot in enumerate((wgot0, wgot1)):
        once = passing_of(wgot.at[0])
        twice = once * passing_of(wgot.at[1])
        state = (wgot[0, 0:STATE, :].astype(F32)
                 + wgot[1, 0:STATE, :].astype(F32) * (once * source_mask[4 * m + 2])
                 + wgot[2, 0:STATE, :].astype(F32) * (twice * source_mask[4 * m + 3]))
        carried.append(state.astype(BF16))

    for t in range(tiles):
        r = pl.ds(128 * t, 128)
        here = rdo[r, :]
        y = local[r, :]
        y += jnp.dot(here, carried[0], preferred_element_type=F32) * lanes_of(cols, r, A0)
        y += jnp.dot(here, carried[1], preferred_element_type=F32) * lanes_of(cols, r, A1)
        z = gate[r, :].astype(F32)
        y = y * (z * jax.nn.sigmoid(z))
        y = y * lax.rsqrt(jnp.mean(y * y, axis=1, keepdims=True) + norm_eps)
        norm_out[r, :] = (y * gain[...].reshape(1, 256)).astype(BF16)

    norm_in[:, my_cols] = norm_out[mine, :]
    sends += exchange(2, token_rows(norm_out), norm_in)
    ring.up_step(4)
    ring.down_step(3)
    wo.relay()
    ring.up_step(5)
    ring.up_step(6)
    ring.down_half(2, False)
    ring.down_step(4)
    ring.up_step(7)
    ring.up_step(8)
    ring.down_half(3, False)
    exchanged(0, stream_in)
    exchanged(1, gains)
    exchanged(2, norm_in)
    wo.far()
    for k in (2, 5, 6, 7):
        wo.sibling(k)
    for n in range(4):
        c = pl.ds(512 * n, 512)
        first[:, c] = (resid_scale * stream_in[:, c].astype(F32)
                       + jnp.dot(norm_in[...], wout[:, c], preferred_element_type=F32))
    f = first[...]
    mean = jnp.sum(f, axis=1, keepdims=True) * (1.0 / D)
    var = jnp.sum(f * f, axis=1, keepdims=True) * (1.0 / D) - mean * mean
    tok[mine, :] = ((f - mean) * lax.rsqrt(var + norm_eps) * gains[0:1, :]).astype(BF16)
    tg = TpGather(tok.at[mine], tok, share, tk_s, tk_r, sp, tp)
    tg.begin()
    ring.up_step(9)
    ring.down_half(4, False)
    ring.up_step(10)
    tg.relay()
    ring.up_step(11)
    tg.far()
    ring.up_step(12)
    ring.up_step(13)
    ring.up_step(14)
    ring.finish()
    for k in (2, 5, 6, 7):
        tg.sibling(k)

    x, c = tp // 2, lax.rem(tp, 2)

    def chip(d):
        return lax.rem(x + d + 4, 4)

    def chunk_rows(k):
        return pl.ds(2 * share * k, 2 * share)

    def compute(k):
        chunk = tok[chunk_rows(k), :]
        for n in range(4):
            hidden = jnp.maximum(jnp.dot(chunk, up[:, 256 * n : 256 * n + 256], preferred_element_type=F32), 0.0)
            squares[:, 256 * n : 256 * n + 256] = (hidden * hidden).astype(BF16)
        sq = squares[...]
        for e in range(4):
            for other in (True, False):
                q = 2 * e + (1 - c if other else c)
                w = down[pl.ds(pl.multiple_of(q * 256, 256), 256), :]
                part = lax.dot_general(sq, w, (((1,), (1,)), ((), ())), preferred_element_type=F32)
                if other:
                    sib_out[k, e] = part.astype(BF16)
                else:
                    own_part[k % 3, e] = part
        copy = copy_to(sib_out.at[k], sib_in.at[k], sb_s.at[k], sb_r.at[k], (sp, 2 * x + 1 - c))
        copy.start()
        return copy

    def push(src, dst, k, e, d):
        copy = copy_to(src, dst, rs_s.at[k, e], rs_r.at[k, e], (sp, 2 * chip(d) + c))
        copy.start()
        sends.append(copy)

    def pass_on(k, copy):
        copy.wait()
        outgoing[k, 2] = (own_part[k % 3, chip(2)] + sib_in[k, chip(2)].astype(F32)).astype(BF16)
        local[chunk_rows(k), :] = own_part[k % 3, x] + sib_in[k, x].astype(F32)
        for e, d in enumerate((1, -1)):
            half = pl.ds(share * e, share)
            push(outgoing.at[k, 2, half], relay.at[k, e], k, 2 + e, d)

    def push_near(k):
        for e, d in enumerate((1, -1)):
            copy_to(relay.at[k, e], relay.at[k, e], rs_s.at[k, 2 + e], rs_r.at[k, 2 + e], (sp, 2 * chip(d) + c)).wait_recv()
            half, rest = pl.ds(share * e, share), pl.ds(share * (1 - e), share)
            total = own_part[k % 3, chip(d), half] + sib_in[k, chip(d), half].astype(F32)
            outgoing[k, e, half] = (total + relay[k, e].astype(F32)).astype(BF16)
            total = own_part[k % 3, chip(d), rest] + sib_in[k, chip(d), rest].astype(F32)
            outgoing[k, e, rest] = total.astype(BF16)
        for e, d in enumerate((1, -1)):
            push(outgoing.at[k, e], parts.at[e, chunk_rows(k)], k, e, d)

    copy0 = compute(0)
    copy1 = compute(1)
    pass_on(0, copy0)
    copy2 = compute(2)
    pass_on(1, copy1)
    push_near(0)
    copy3 = compute(3)
    pass_on(2, copy2)
    push_near(1)
    pass_on(3, copy3)
    push_near(2)
    push_near(3)
    def parts_arrived(k):
        for e, d in enumerate((1, -1)):
            r = parts.at[e, chunk_rows(k)]
            copy_to(r, r, rs_s.at[k, e], rs_r.at[k, e], (sp, 2 * chip(d) + c)).wait_recv()

    parts_arrived(0)
    parts_arrived(1)
    parts_arrived(2)
    parts_arrived(3)

    lane_at = lax.broadcasted_iota(jnp.int32, (128, 128), 1)
    for t in range(tiles):
        r = pl.ds(128 * t, 128)
        y = local[r, :] + resid_scale * tok[r, my_cols].astype(F32)
        for e in range(2):
            y += parts[e, r, :].astype(F32)
        local[r, :] = y
        one = jnp.sum(y, axis=1, keepdims=True)
        two = jnp.sum(y * y, axis=1, keepdims=True)
        pair = jnp.where(lane_at == 0, one, jnp.where(lane_at == 1, two, 0.0))
        stat_out[:, 128 * t : 128 * t + 128] = jnp.transpose(pair)[0:8, :]
    for d in range(1, n_tp):
        copy = copy_to(stat_out, stat_in.at[d - 1], st_s.at[d - 1], st_r.at[d - 1], (sp, peer(d)))
        copy.start()
        sends.append(copy)

    def stats_arrived():
        for d in range(1, n_tp):
            copy_to(stat_in.at[d - 1], stat_in.at[d - 1], st_s.at[d - 1], st_r.at[d - 1], (sp, peer(d))).wait_recv()

    def all_sent():
        for copy in sends + ring.sent + wo.sent + tg.sent:
            copy.wait_send()

    stats_arrived()
    stats = stat_out[...]
    for d in range(1, n_tp):
        stats += stat_in[d - 1]
    mean = stats[0:1] * (1.0 / D)
    scale = lax.rsqrt(stats[1:2] * (1.0 / D) - mean * mean + norm_eps)
    rowq[0:1, :] = mean
    rowq[1:2, :] = scale
    for t in range(tiles):
        r = pl.ds(128 * t, 128)
        both = jnp.transpose(rowq[:, 128 * t : 128 * t + 128])
        out[r, :] = ((local[r, :] - both[:, 0:1]) * both[:, 1:2] * last_gain[...].reshape(1, 256)).astype(BF16)
    all_sent()


def per_device(hv, em, rm, gate, step, sudden, document_index, rate, bias, tv, te, tr, gain,
               out_weight, stream, first_gain, last_gain, up_in, down_in):
    rows = hv.shape[0]
    docs = document_index.reshape(-1, 128)
    vmem = pl.BlockSpec(memory_space=pltpu.VMEM)
    dma = pltpu.SemaphoreType.DMA
    share = rows // 8
    return pl.pallas_call(
        layer_kernel,
        out_shape=jax.ShapeDtypeStruct((rows, 256), BF16),
        in_specs=[vmem] * 7 + [pl.BlockSpec(memory_space=pltpu.SMEM)] * 2 + [vmem] * 10,
        out_specs=vmem,
        scratch_shapes=[
            pltpu.VMEM((16, 256), BF16), pltpu.VMEM((16, 128), BF16), pltpu.VMEM((16, 128), BF16),
            pltpu.VMEM((16, 256), BF16), pltpu.VMEM((16, 128), BF16), pltpu.VMEM((16, 128), BF16),
            pltpu.VMEM((24, rows), F32), pltpu.VMEM((8, 256), F32),
            pltpu.VMEM((rows + 16, 512), F32),
            pltpu.VMEM((128, rows), F32),
            pltpu.VMEM((rows, 128), F32),
            pltpu.VMEM((rows, 256), BF16), pltpu.VMEM((rows, 128), BF16), pltpu.VMEM((rows, 128), F32),
            pltpu.VMEM((rows, 128), BF16),
            pltpu.VMEM((2, 128, rows), F32),
            pltpu.VMEM((rows, 256), F32),
            pltpu.VMEM((STATE + 16, 256), BF16), pltpu.VMEM((STATE + 16, 256), BF16),
            pltpu.VMEM((2, STATE + 16, 256), BF16), pltpu.VMEM((2, STATE + 16, 256), BF16),
            pltpu.VMEM((STATE + 16, 256), BF16), pltpu.VMEM((STATE + 16, 256), BF16),
            pltpu.VMEM((3, STATE + 16, 256), BF16), pltpu.VMEM((3, STATE + 16, 256), BF16),
            pltpu.VMEM((2, STATE, 256), F32),
            pltpu.VMEM((D, 1024), BF16), pltpu.VMEM((D, 1024), BF16), pltpu.VMEM((D, D), BF16),
            pltpu.VMEM((rows, 256), BF16), pltpu.VMEM((share, D), BF16), pltpu.VMEM((share, D), BF16),
            pltpu.VMEM((8, D), F32), pltpu.VMEM((share, D), F32), pltpu.VMEM((rows, D), BF16),
            pltpu.VMEM((2 * share, 1024), BF16),
            pltpu.VMEM((4, 4, 2 * share, 256), BF16), pltpu.VMEM((4, 4, 2 * share, 256), BF16),
            pltpu.VMEM((3, 4, 2 * share, 256), F32), pltpu.VMEM((4, 3, 2 * share, 256), BF16),
            pltpu.VMEM((2, rows, 256), BF16), pltpu.VMEM((4, 2, share, 256), BF16), pltpu.VMEM((8, rows), F32), pltpu.VMEM((7, 8, rows), F32),
            dma((6,)), dma((6,)), dma((10,)), dma((10,)),
            dma((2,)), dma((2,)), dma((2,)), dma((2,)), dma((2, 4, 4)), dma((2, 4, 4)),
            dma((2, 4)), dma((2, 4)), dma((8, 2)), dma((8, 2)), dma((8, 2)), dma((8, 2)),
            dma((8,)), dma((8,)), dma((8,)), dma((8,)), dma((3, 7)), dma((3, 7)),
            dma((4,)), dma((4,)), dma((4, 4)), dma((4, 4)), dma((7,)), dma((7,)),
        ],
        compiler_params=pltpu.CompilerParams(
            collective_id=0, has_side_effects=True, vmem_limit_bytes=60 * 1024 * 1024),
        cost_estimate=pl.CostEstimate(flops=9_000_000_000, bytes_accessed=8_000_000, transcendentals=0),
        name="layer",
    )(hv, em, rm, gate, step.T, sudden.T, docs, rate, bias, tv, te, tr, gain, up_in, down_in, out_weight, stream,
      first_gain, last_gain)


SPECS = (
    P("sp", "tp"), P("sp", "tp"), P("sp", "tp"), P("sp", "tp"), P("sp", "tp"), P("sp", "tp"), P(),
    P(None, "tp"), P(None, "tp"), P(None, "tp"), P(None, "tp"), P(None, "tp"), P("tp"),
    P("tp", None), P("sp", "tp"), P("tp"), P("tp"), P("sp", "tp"), P("sp", "tp"),
)


def solution(mesh):
    return jax.shard_map(per_device, mesh=mesh, in_specs=SPECS, out_specs=P("sp", "tp"), check_vma=False)
```

```python
import functools

import jax
import jax.numpy as jnp
from jax import lax
from jax.experimental import pallas as pl
from jax.experimental.pallas import tpu as pltpu
from jax.sharding import PartitionSpec as P

D = 2048
HEAD_DIM = 64
STATE = 128
REACH = 8
MESH = pl.DeviceIdType.MESH
norm_eps = 1e-05
resid_scale = 1.4142135623730951
F32 = jnp.float32
BF16 = jnp.bfloat16


def lanes_of(cols, rows, base):
    n = rows.size
    low = lax.broadcasted_iota(jnp.int32, (n, 128), 1) < HEAD_DIM
    halves = []
    for k in (0, 2):
        a = jnp.broadcast_to(cols[rows, base + k : base + k + 1], (n, 128))
        b = jnp.broadcast_to(cols[rows, base + k + 1 : base + k + 2], (n, 128))
        halves.append(jnp.where(low, a, b))
    return jnp.concatenate(halves, axis=1)


def head_lanes(column):
    return jnp.concatenate([jnp.broadcast_to(c, (1, HEAD_DIM)) for c in column], axis=1)


C0, D1, W0, W1, A0, A1, DT0, CM, DOC = 0, 4, 8, 12, 16, 20, 24, 28, 33


def copy_to(src, dst, send, recv, device):
    return pltpu.make_async_remote_copy(src_ref=src, dst_ref=dst, send_sem=send, recv_sem=recv,
                                        device_id=device, device_id_type=MESH)


class WeightRing:
    def __init__(self, up_in, down_in, up, down, sems, sp, tp):
        (self.uy_s, self.uy_r, self.uh_s, self.uh_r, self.uz_s, self.uz_r,
         self.dz_s, self.dz_r, self.dy_s, self.dy_r, self.dh_s, self.dh_r) = sems
        self.up_in, self.down_in, self.up, self.down, self.tp = up_in, down_in, up, down, tp
        self.y, self.z = lax.rem(sp, 4), sp // 4
        self.sent = []

    def dev(self, dz, dy):
        return (lax.rem(self.z + dz + 8, 8) * 4 + lax.rem(self.y + dy + 4, 4), self.tp)

    def rows(self, dz, dy, low=0, count=64):
        shard = lax.rem(self.z + dz + 8, 8) * 4 + lax.rem(self.y + dy + 4, 4)
        return pl.ds(pl.multiple_of(shard * 64 + low, 32), count)

    def send(self, src, dst, send, recv, device):
        copy = copy_to(src, dst, send, recv, device)
        copy.start()
        self.sent.append(copy)

    def arrived(self, dst, send, recv):
        copy_to(dst, dst, send, recv, self.dev(1, 0)).wait_recv()

    def up_z(self, s, p, receive):
        for m, sign in enumerate((1, -1)):
            low, count = (32 * m, 32) if s == 3 else (0, 64)
            if receive:
                r = self.rows(-sign * (s + 1), p, low, count)
                self.arrived(self.up.at[r], self.uz_s.at[m, s, p], self.uz_r.at[m, s, p])
            else:
                r = self.rows(-sign * s, p, low, count)
                src = self.up_in if s == 0 and p == 0 else self.up.at[r]
                self.send(src, self.up.at[r], self.uz_s.at[m, s, p], self.uz_r.at[m, s, p], self.dev(sign, 0))

    def down_z(self, s, receive):
        for m, sign in enumerate((1, -1)):
            low, count = (32 * m, 32) if s == 3 else (0, 64)
            if receive:
                r = self.rows(-sign * (s + 1), 0, low, count)
                self.arrived(self.down.at[r], self.dz_s.at[m, s], self.dz_r.at[m, s])
            else:
                r = self.rows(-sign * s, 0, low, count)
                src = self.down_in if s == 0 else self.down.at[r]
                self.send(src, self.down.at[r], self.dz_s.at[m, s], self.dz_r.at[m, s], self.dev(sign, 0))

    def planes(self, s):
        return [(0, 0)] if s == 0 else [(7, 4)] if s == 4 else [(2 * s - 1, -s), (2 * s, s)]

    def down_y(self, s):
        for k, dz in self.planes(s):
            for m, sign in enumerate((1, -1)):
                r = self.rows(dz, 0)
                src = self.down_in if s == 0 else self.down.at[r]
                self.send(src, self.down.at[r], self.dy_s.at[k, m], self.dy_r.at[k, m], self.dev(0, sign))

    def down_half(self, s, receive):
        for k, dz in self.planes(s):
            for m, sign in enumerate((1, -1)):
                if receive:
                    r = self.rows(dz, -2 * sign, 32 * m, 32)
                    self.arrived(self.down.at[r], self.dh_s.at[k, m], self.dh_r.at[k, m])
                else:
                    self.arrived(self.down.at[self.rows(dz, -sign)], self.dy_s.at[k, m], self.dy_r.at[k, m])
                    r = self.rows(dz, -sign, 32 * m, 32)
                    self.send(self.down.at[r], self.down.at[r], self.dh_s.at[k, m], self.dh_r.at[k, m],
                              self.dev(0, sign))

    def up_step(self, n):
        s, part = divmod(n, 3)
        if part == 0:
            if s == 0:
                for m, sign in enumerate((1, -1)):
                    self.send(self.up_in, self.up.at[self.rows(0, 0)], self.uy_s.at[m], self.uy_r.at[m],
                              self.dev(0, sign))
            else:
                self.up_z(s - 1, 0, True)
            if s < 4:
                self.up_z(s, 0, False)
        elif part == 1:
            if s == 0:
                for m, sign in enumerate((1, -1)):
                    self.arrived(self.up.at[self.rows(0, -sign)], self.uy_s.at[m], self.uy_r.at[m])
                    r = self.rows(0, -sign, 32 * m, 32)
                    self.send(self.up.at[r], self.up.at[r], self.uh_s.at[m], self.uh_r.at[m], self.dev(0, sign))
            else:
                self.up_z(s - 1, 1, True)
                self.up_z(s - 1, 3, True)
            if s < 4:
                self.up_z(s, 1, False)
                self.up_z(s, 3, False)
        else:
            if s == 0:
                for m, sign in enumerate((1, -1)):
                    self.arrived(self.up.at[self.rows(0, -2 * sign, 32 * m, 32)], self.uh_s.at[m], self.uh_r.at[m])
            else:
                self.up_z(s - 1, 2, True)
            if s < 4:
                self.up_z(s, 2, False)

    def down_step(self, s):
        if s > 0:
            self.down_z(s - 1, True)
        if s < 4:
            self.down_z(s, False)
        self.down_y(s)

    def finish(self):
        for s in range(5):
            self.down_half(s, True)


class TpGather:
    def __init__(self, own, buf, size, send, recv, sp, tp):
        self.own, self.buf, self.size, self.s, self.r, self.sp = own, buf, size, send, recv, sp
        self.x, self.c = tp // 2, lax.rem(tp, 2)
        self.sent = []

    def slot(self, dx, other):
        return lax.rem(self.x + dx + 4, 4) * 2 + (1 - self.c if other else self.c)

    def rows(self, dx, other, half=None):
        low, count = (0, self.size) if half is None else (half * (self.size // 2), self.size // 2)
        return self.buf.at[pl.ds(pl.multiple_of(self.slot(dx, other) * self.size + low, 16), count)]

    def send(self, src, dst, k, dx, other):
        copy = copy_to(src, dst, self.s.at[k], self.r.at[k], (self.sp, self.slot(dx, other)))
        copy.start()
        self.sent.append(copy)

    def arrived(self, dst, k):
        copy_to(dst, dst, self.s.at[k], self.r.at[k], (self.sp, self.slot(0, True))).wait_recv()

    def begin(self):
        mine = self.rows(0, False)
        self.send(self.own, mine, 0, 1, False)
        self.send(self.own, mine, 1, -1, False)
        self.send(self.own, mine, 2, 0, True)

    def relay(self):
        left, right = self.rows(-1, False), self.rows(1, False)
        self.arrived(left, 0)
        self.send(self.rows(-1, False, 0), self.rows(-1, False, 0), 3, 1, False)
        self.send(left, left, 5, 0, True)
        self.arrived(right, 1)
        self.send(self.rows(1, False, 1), self.rows(1, False, 1), 4, -1, False)
        self.send(right, right, 6, 0, True)

    def far(self):
        self.arrived(self.rows(2, False, 0), 3)
        self.arrived(self.rows(2, False, 1), 4)
        self.send(self.rows(2, False), self.rows(2, False), 7, 0, True)

    def sibling(self, k):
        self.arrived(self.rows({2: 0, 5: -1, 6: 1, 7: 2}[k], True), k)


def layer_kernel(
    hv_any, em_any, rm_any, gate_any, stream_any, wout_any, up_any, down_any,
    step_in, sudden_in, docs_in, rate, bias, tap_v, tap_e, tap_r, gain, first_gain, last_gain, out,
    hv, em, rm, gate, stream, wout_in,
    prev_v, prev_e, prev_r, next_v, next_e, next_r,
    per_token, gains_in, wide, rowq, cols, val, ent, ent32, rdo, weight, local,
    msg0, msg1, got0, got1, wmsg0, wmsg1, wgot0, wgot1, states,
    up, down, norm_out, mix_sib, mix_got, mix_own, mix_far, mix_near, mix_relay, mix_in, stream_in, gains, first, tok, squares,
    sib_out, sib_in, own_part, outgoing, parts, relay, stat_out, stat_in,
    pull, halo_send, halo_recv, state_send, state_recv,
    uy_s, uy_r, uh_s, uh_r, uz_s, uz_r, dz_s, dz_r, dy_s, dy_r, dh_s, dh_r,
    mx_s, mx_r, tk_s, tk_r, ex_s, ex_r, sb_s, sb_r, rs_s, rs_r, st_s, st_r,
):
    sp, tp = lax.axis_index("sp"), lax.axis_index("tp")
    n_sp = lax.axis_size("sp")
    n_tp = lax.axis_size("tp")
    rows = hv.shape[0]
    tiles = rows // 128
    share = rows // n_tp

    def at(d):
        return (lax.rem(sp + d + n_sp, n_sp), tp)

    def peer(d):
        return lax.rem(tp + d + n_tp, n_tp)

    own_rows = pl.ds(pl.multiple_of(sp * 64, 64), 64)
    up_in, down_in = up.at[own_rows], down.at[own_rows]
    barrier = pltpu.get_barrier_semaphore()
    gains_in[...] = jnp.broadcast_to(first_gain[...].reshape(1, 256), (8, 256))
    for d in range(1, REACH + 1):
        for s in (d, -d):
            pl.semaphore_signal(barrier, inc=1, device_id=at(s), device_id_type=MESH)
    for d in range(1, n_tp):
        pl.semaphore_signal(barrier, inc=1, device_id=(sp, peer(d)), device_id_type=MESH)
    pulls = [pltpu.make_async_copy(src, dst, pull.at[k]) for k, (src, dst) in enumerate((
        (hv_any, hv), (em_any, em), (rm_any, rm), (up_any, up_in), (down_any, down_in), (stream_any, stream),
        (gate_any, gate), (wout_any, wout_in)))]
    for copy in pulls:
        copy.start()
    pl.semaphore_wait(barrier, 2 * REACH + n_tp - 1)
    for copy in pulls:
        copy.wait()

    halos = []
    for k, (src, low, high) in enumerate(((hv, prev_v, next_v), (em, prev_e, next_e), (rm, prev_r, next_r))):
        for m, (start, dst, step) in enumerate(((rows - 16, low, 1), (0, high, -1))):
            halos.append(copy_to(src.at[pl.ds(start, 16)], dst, halo_send.at[2 * k + m], halo_recv.at[2 * k + m],
                                 at(step)))
    for copy in halos:
        copy.start()
    ring = WeightRing(up_in, down_in, up, down,
                      (uy_s, uy_r, uh_s, uh_r, uz_s, uz_r, dz_s, dz_r, dy_s, dy_r, dh_s, dh_r), sp, tp)
    ring.down_step(0)
    ring.up_step(0)

    def my_lanes(ref, q):
        return ref.at[:, pl.ds(pl.multiple_of(q * 256, 256), 256)]

    def exchange(k, src_of, dst):
        sent = []
        for d in range(1, n_tp):
            q = peer(d)
            copy = copy_to(src_of(q), my_lanes(dst, tp), ex_s.at[k, d - 1], ex_r.at[k, d - 1], (sp, q))
            copy.start()
            sent.append(copy)
        return sent

    def exchanged(k, dst):
        for d in range(1, n_tp):
            r = my_lanes(dst, peer(-d))
            copy_to(r, r, ex_s.at[k, d - 1], ex_r.at[k, d - 1], (sp, peer(d))).wait_recv()

    def token_rows(ref):
        return lambda q: ref.at[pl.ds(pl.multiple_of(q * share, 16), share)]

    sends = exchange(0, token_rows(stream), stream_in)
    sends += exchange(1, lambda q: gains_in, gains)
    mine = pl.ds(pl.multiple_of(tp * share, 16), share)
    my_cols = pl.ds(pl.multiple_of(tp * 256, 256), 256)
    stream_in[:, my_cols] = stream[mine, :]
    gains[:, my_cols] = gains_in[...]

    raw = step_in[...].astype(F32)
    sudden = sudden_in[...]

    def eight(ref):
        return jnp.concatenate([jnp.full((1, rows), ref[k, h], F32) for k in range(2) for h in range(4)], axis=0)

    before_softplus = jnp.concatenate([raw, raw], axis=0) + eight(bias)
    per_token[0:8, :] = jnp.maximum(before_softplus, 0.0) + jnp.log1p(jnp.exp(-jnp.abs(before_softplus)))
    per_token[8:16, :] = -jnp.exp(eight(rate)) * per_token[0:8, :] + jnp.concatenate([sudden, sudden], axis=0)

    def doc_at(row, lane_no):
        return docs_in[pl.ds(row, 1), lane_no : lane_no + 1].astype(F32)

    own_doc = jnp.concatenate([docs_in[pl.ds(tiles * sp + t, 1), :] for t in range(tiles)], axis=1).astype(F32)
    own8 = jnp.broadcast_to(own_doc, (8, rows))
    low_row, high_row = jnp.maximum(tiles * sp - 1, 0), jnp.minimum(tiles * sp + tiles, tiles * n_sp - 1)
    prev_two, prev_one = (jnp.where(sp > 0, doc_at(low_row, k), -1.0) for k in (126, 127))
    next_one, next_two = (jnp.where(sp < n_sp - 1, doc_at(high_row, k), -1.0) for k in (0, 1))
    lane8 = lax.broadcasted_iota(jnp.int32, (8, rows), 1)
    back_one = jnp.where(lane8 == 0, prev_one, pltpu.roll(own8, 1, 1))
    back_two = jnp.where(lane8 == 0, prev_two, jnp.where(lane8 == 1, prev_one, pltpu.roll(own8, 2, 1)))
    on_one = jnp.where(lane8 == rows - 1, next_one, pltpu.roll(own8, rows - 1, 1))
    on_two = jnp.where(lane8 == rows - 1, next_two, jnp.where(lane8 == rows - 2, next_one, pltpu.roll(own8, rows - 2, 1)))
    for k, row in enumerate((back_two, back_one, own8, on_one, on_two)):
        per_token[16 + k : 17 + k, :] = row[0:1]
    per_token[21:22, :] = jnp.broadcast_to(prev_one, (1, rows))
    per_token[22:23, :] = jnp.broadcast_to(next_one, (1, rows))
    per_token[23:24, :] = jnp.zeros((1, rows), F32)

    def last_doc(d):
        return doc_at(tiles * lax.rem(sp - d + n_sp, n_sp) + tiles - 1, 127)

    def first_doc(d):
        return doc_at(tiles * lax.rem(sp + d, n_sp), 0)

    source_mask = []
    for edge, room in ((last_doc, sp), (first_doc, n_sp - 1 - sp)):
        for d, to in ((1, 0), (2, 0), (4, 1), (7, 1)):
            source_mask.append(jnp.where((edge(d) == edge(to)) & (room >= d), 1.0, 0.0))

    dt = per_token[0:8, :]
    log_decay = per_token[8:16, :]
    lane = lax.broadcasted_iota(jnp.int32, (8, rows), 1)
    total = log_decay
    shift = 1
    while shift < rows:
        total = total + jnp.where(lane >= shift, pltpu.roll(total, shift, 1), 0.0)
        shift *= 2
    c0 = total[0:4]
    d1 = total[4:8] - log_decay[4:8]
    all0, all1 = total[0:4, rows - 1 : rows], total[4:8, rows - 1 : rows]
    docs = per_token[16:24, :]
    own = docs[2:3]
    same_end = jnp.where(own == own[:, rows - 1 : rows], 1.0, 0.0)
    same_start = jnp.where(own == own[:, 0:1], 1.0, 0.0)
    from_prev = jnp.where(own == docs[5:6], 1.0, 0.0)
    from_next = jnp.where(own == docs[6:7], 1.0, 0.0)
    rowq[...] = jnp.zeros_like(rowq)
    rowq[C0 : C0 + 4, :] = c0
    rowq[D1 : D1 + 4, :] = d1
    rowq[W0 : W0 + 4, :] = jnp.exp(all0 - c0) * dt[0:4] * same_end
    rowq[W1 : W1 + 4, :] = jnp.exp(d1) * dt[4:8] * same_start
    rowq[A0 : A0 + 4, :] = jnp.exp(c0) * from_prev
    rowq[A1 : A1 + 4, :] = jnp.exp(all1 - d1) * from_next
    rowq[DT0 : DT0 + 4, :] = dt[0:4]
    rowq[CM : CM + 5, :] = jnp.where(docs[0:5] == own, 1.0, 0.0)
    rowq[DOC : DOC + 1, :] = own
    for t in range(tiles):
        cols[pl.ds(128 * t, 128), :] = jnp.transpose(rowq[:, 128 * t : 128 * t + 128])

    wide[8 : 8 + rows, 0:256] = hv[...].astype(F32)
    wide[8 : 8 + rows, 256:384] = em[...].astype(F32)
    wide[8 : 8 + rows, 384:512] = rm[...].astype(F32)
    for copy in halos:
        copy.wait()
    wide[0:8, 0:256] = prev_v[8:16, :].astype(F32)
    wide[0:8, 256:384] = prev_e[8:16, :].astype(F32)
    wide[0:8, 384:512] = prev_r[8:16, :].astype(F32)
    wide[8 + rows : 16 + rows, 0:256] = next_v[0:8, :].astype(F32)
    wide[8 + rows : 16 + rows, 256:384] = next_e[0:8, :].astype(F32)
    wide[8 + rows : 16 + rows, 384:512] = next_r[0:8, :].astype(F32)

    whole_taps = tap_v[...].astype(F32)
    taps = (whole_taps[:, 0:128], whole_taps[:, 128:256], tap_e[...].astype(F32), tap_r[...].astype(F32))
    for t in range(tiles):
        lo = 128 * t
        masks = [jnp.broadcast_to(cols[lo : lo + 128, CM + o : CM + o + 1], (128, 128)) for o in range(5)]
        for g in range(4):
            acc = jnp.zeros((128, 128), F32)
            for o in range(5):
                part = wide[lo + 6 + o : lo + 134 + o, 128 * g : 128 * g + 128]
                if o != 2:
                    part = part * masks[o]
                acc = acc + taps[g][o : o + 1] * part
            act = acc * jax.nn.sigmoid(acc)
            if g < 2:
                val[lo : lo + 128, 128 * g : 128 * g + 128] = act.astype(BF16)
            elif g == 2:
                ent32[lo : lo + 128, :] = act
                ent[lo : lo + 128, :] = act.astype(BF16)
            else:
                rdo[lo : lo + 128, :] = act.astype(BF16)

    state0 = jnp.zeros((STATE, 256), F32)
    state1 = jnp.zeros((STATE, 256), F32)
    for t in range(tiles):
        r = pl.ds(128 * t, 128)
        ent_t = jnp.transpose(ent32[r, :]).astype(BF16)
        v = val[r, :].astype(F32)
        state0 += jnp.dot(ent_t, (v * lanes_of(cols, r, W0)).astype(BF16), preferred_element_type=F32)
        state1 += jnp.dot(ent_t, (v * lanes_of(cols, r, W1)).astype(BF16), preferred_element_type=F32)
    def fill(msg, state, passing):
        msg[0:STATE, :] = state.astype(BF16)
        coarse = passing.astype(BF16)
        fine = (passing - coarse.astype(F32)).astype(BF16)
        row = lax.broadcasted_iota(jnp.int32, (16, 256), 0)
        both = jnp.where(row == 0, coarse.astype(F32), jnp.where(row == 1, fine.astype(F32), 0.0))
        msg[STATE : STATE + 16, :] = both.astype(BF16)

    def passing_of(msg):
        tail = msg[STATE : STATE + 16, :].astype(F32)
        return tail[0:1] + tail[1:2]

    pass_own = [head_lanes([jnp.exp(whole[h : h + 1, :]) for h in range(4)]) for whole in (all0, all1)]
    for m, (msg, state) in enumerate(((msg0, state0), (msg1, state1))):
        states[m] = state
        fill(msg, state, pass_own[m])

    for t in range(tiles):
        r = pl.ds(128 * t, 128)
        own_score = jnp.sum(rdo[r, :].astype(F32) * ent[r, :].astype(F32), axis=1, keepdims=True)
        local[r, :] = own_score * lanes_of(cols, r, DT0) * val[r, :].astype(F32)

    near_sends = []
    for k, d in enumerate((1, 2)):
        for m, (msg, got, step) in enumerate(((msg0, got0, d), (msg1, got1, -d))):
            near_sends.append(copy_to(msg, got.at[k], state_send.at[2 * k + m], state_recv.at[2 * k + m], at(step)))
    for copy in near_sends:
        copy.start()
    ring.down_step(1)
    ring.up_step(1)
    ring.down_half(0, False)

    low_lane = lax.broadcasted_iota(jnp.int32, (128, 128), 1) < HEAD_DIM

    def tile_step(i, _):
        r = pl.ds(pl.multiple_of(i * 128, 128), 128)
        here = rdo[r, :]
        doc_t = jnp.broadcast_to(cols[r, DOC : DOC + 1], (128, 128))
        t_index = lax.broadcasted_iota(jnp.int32, (128, 128), 0) + i * 128
        for pair in range(2):
            outs = []
            for h in (2 * pair, 2 * pair + 1):
                ct = jnp.broadcast_to(cols[r, C0 + h : C0 + h + 1], (128, 128))
                dd = jnp.broadcast_to(cols[r, D1 + h : D1 + h + 1], (128, 128))
                for j in range(tiles):
                    s = pl.ds(128 * j, 128)
                    if h == 0:
                        score = lax.dot_general(here, ent[s, :], (((1,), (1,)), ((), ())), preferred_element_type=F32)
                        score = jnp.where(doc_t == per_token[18:19, 128 * j : 128 * j + 128], score, 0.0)
                        weight[1, :, 128 * j : 128 * j + 128] = score
                    score = weight[1, :, 128 * j : 128 * j + 128]
                    s_index = lax.broadcasted_iota(jnp.int32, (128, 128), 1) + 128 * j
                    spread = jnp.minimum(ct - rowq[C0 + h : C0 + h + 1, 128 * j : 128 * j + 128],
                                         rowq[D1 + h : D1 + h + 1, 128 * j : 128 * j + 128] - dd)
                    step = jnp.where(s_index < t_index, per_token[h : h + 1, 128 * j : 128 * j + 128],
                                     per_token[4 + h : 5 + h, 128 * j : 128 * j + 128])
                    weight[0, :, 128 * j : 128 * j + 128] = score * jnp.exp(spread) * step
                outs.append(jnp.dot(weight[0].astype(BF16), val[:, 128 * pair : 128 * pair + 128],
                                    preferred_element_type=F32))
            local[r, 128 * pair : 128 * pair + 128] += jnp.where(low_lane, outs[0], outs[1])
        return 0

    lax.fori_loop(0, tiles // 2, tile_step, 0)
    for copy in near_sends:
        copy.wait()
    for m, (got, wmsg) in enumerate(((got0, wmsg0), (got1, wmsg1))):
        through = [pass_own[m]]
        for k in range(2):
            through.append(through[k] * passing_of(got.at[k]))
        window = states[m]
        for k in range(2):
            window += got[k, 0:STATE, :].astype(F32) * (through[k] * source_mask[4 * m + k])
        fill(wmsg, window, through[2])
    far_sends = []
    lax.fori_loop(tiles // 2, tiles // 2 + 1, tile_step, 0)
    for k, d in enumerate((1, 4, 7)):
        for m, (wmsg, wgot, step) in enumerate(((wmsg0, wgot0, d), (wmsg1, wgot1, -d))):
            n = 4 + 2 * k + m
            far_sends.append(copy_to(wmsg, wgot.at[k], state_send.at[n], state_recv.at[n], at(step)))
    for copy in far_sends:
        copy.start()
    lax.fori_loop(tiles // 2 + 1, tiles, tile_step, 0)
    ring.down_step(2)
    ring.up_step(3)
    ring.down_half(1, False)
    for copy in far_sends:
        copy.wait()
    ring.up_step(2)
    carried = []
    for m, wgot in enumerate((wgot0, wgot1)):
        once = passing_of(wgot.at[0])
        twice = once * passing_of(wgot.at[1])
        state = (wgot[0, 0:STATE, :].astype(F32)
                 + wgot[1, 0:STATE, :].astype(F32) * (once * source_mask[4 * m + 2])
                 + wgot[2, 0:STATE, :].astype(F32) * (twice * source_mask[4 * m + 3]))
        carried.append(state.astype(BF16))

    for t in range(tiles):
        r = pl.ds(128 * t, 128)
        here = rdo[r, :]
        y = local[r, :]
        y += jnp.dot(here, carried[0], preferred_element_type=F32) * lanes_of(cols, r, A0)
        y += jnp.dot(here, carried[1], preferred_element_type=F32) * lanes_of(cols, r, A1)
        z = gate[r, :].astype(F32)
        y = y * (z * jax.nn.sigmoid(z))
        y = y * lax.rsqrt(jnp.mean(y * y, axis=1, keepdims=True) + norm_eps)
        norm_out[r, :] = (y * gain[...].reshape(1, 256)).astype(BF16)

    x, c = tp // 2, lax.rem(tp, 2)
    half_share = share // 2

    def chip(d):
        return lax.rem(x + d + 4, 4)

    def project(k, d):
        for other in (True, False):
            q = 2 * chip(d) + (1 - c if other else c)
            part = jnp.dot(norm_out[pl.ds(pl.multiple_of(q * share, 16), share), :], wout_in[...],
                           preferred_element_type=F32)
            if other:
                mix_sib[k] = part.astype(BF16)
            else:
                mix_own[k] = part
        copy = copy_to(mix_sib.at[k], mix_got.at[k], mx_s.at[k], mx_r.at[k], (sp, 2 * x + 1 - c))
        copy.start()
        return copy

    def mix_push(src, dst, n, d):
        copy = copy_to(src, dst, mx_s.at[n], mx_r.at[n], (sp, 2 * chip(d) + c))
        copy.start()
        sends.append(copy)

    def mix_arrived(dst, n):
        copy_to(dst, dst, mx_s.at[n], mx_r.at[n], (sp, 2 * x + 1 - c)).wait_recv()

    def mix_far_out():
        crossing[0].wait()
        mix_far[...] = (mix_own[0] + mix_got[0].astype(F32)).astype(BF16)
        for e, d in enumerate((1, -1)):
            mix_push(mix_far.at[pl.ds(half_share * e, half_share)], mix_relay.at[e], 4 + e, d)

    def mix_near_rest():
        for e, d in enumerate((1, -1)):
            crossing[1 + e].wait()
            rest = pl.ds(half_share * (1 - e), half_share)
            mix_near[e, rest] = (mix_own[1 + e, rest] + mix_got[1 + e, rest].astype(F32)).astype(BF16)
            mix_push(mix_near.at[e, rest], mix_in.at[e, rest], 6 + e, d)
        crossing[3].wait()

    def mix_near_last():
        for e, d in enumerate((1, -1)):
            mix_arrived(mix_relay.at[e], 4 + e)
            half = pl.ds(half_share * e, half_share)
            total = mix_own[1 + e, half] + mix_got[1 + e, half].astype(F32) + mix_relay[e].astype(F32)
            mix_near[e, half] = total.astype(BF16)
            mix_push(mix_near.at[e, half], mix_in.at[e, half], 8 + e, d)

    def mix_finish():
        for e in range(2):
            mix_arrived(mix_in.at[e, pl.ds(half_share * (1 - e), half_share)], 6 + e)
            mix_arrived(mix_in.at[e, pl.ds(half_share * e, half_share)], 8 + e)
        first[...] = (resid_scale * stream_in[...].astype(F32) + mix_own[3] + mix_got[3].astype(F32)
                      + mix_in[0].astype(F32) + mix_in[1].astype(F32))

    crossing = [project(0, 2)]
    crossing.append(project(1, 1))
    mix_far_out()
    crossing.append(project(2, -1))
    crossing.append(project(3, 0))
    mix_near_rest()
    ring.up_step(4)
    mix_near_last()
    ring.down_step(3)
    ring.up_step(5)
    ring.up_step(6)
    ring.down_half(2, False)
    exchanged(0, stream_in)
    exchanged(1, gains)
    mix_finish()
    f = first[...]
    mean = jnp.sum(f, axis=1, keepdims=True) * (1.0 / D)
    var = jnp.sum(f * f, axis=1, keepdims=True) * (1.0 / D) - mean * mean
    tok[mine, :] = ((f - mean) * lax.rsqrt(var + norm_eps) * gains[0:1, :]).astype(BF16)
    tg = TpGather(tok.at[mine], tok, share, tk_s, tk_r, sp, tp)
    tg.begin()
    ring.down_step(4)
    ring.up_step(7)
    ring.up_step(8)
    ring.down_half(3, False)
    ring.up_step(9)
    tg.relay()
    ring.down_half(4, False)
    ring.up_step(10)
    ring.up_step(11)
    tg.far()
    ring.up_step(12)
    ring.up_step(13)
    ring.up_step(14)
    ring.finish()
    for k in (2, 5, 6, 7):
        tg.sibling(k)

    def chunk_rows(k):
        return pl.ds(2 * share * k, 2 * share)

    def hidden(k):
        chunk = tok[chunk_rows(k), :]
        for n in range(4):
            h = jnp.maximum(jnp.dot(chunk, up[:, 256 * n : 256 * n + 256], preferred_element_type=F32), 0.0)
            squares[:, 256 * n : 256 * n + 256] = (h * h).astype(BF16)

    def compute(k):
        sq = squares[...]
        for n, d in enumerate((2, 1, -1, 0)):
            for other in (True, False):
                q = 2 * chip(d) + (1 - c if other else c)
                w = down[pl.ds(pl.multiple_of(q * 256, 256), 256), :]
                part = lax.dot_general(sq, w, (((1,), (1,)), ((), ())), preferred_element_type=F32)
                if other:
                    sib_out[k, n] = part.astype(BF16)
                else:
                    own_part[k % 3, n] = part
        crossing = []
        for n, r in enumerate((pl.ds(0, 1), pl.ds(1, 3))):
            copy = copy_to(sib_out.at[k, r], sib_in.at[k, r], sb_s.at[k, n], sb_r.at[k, n], (sp, 2 * x + 1 - c))
            copy.start()
            crossing.append(copy)
        return crossing

    def push(src, dst, k, e, d):
        copy = copy_to(src, dst, rs_s.at[k, e], rs_r.at[k, e], (sp, 2 * chip(d) + c))
        copy.start()
        sends.append(copy)

    def pass_on(k, crossing):
        crossing[0].wait()
        outgoing[k, 2] = (own_part[k % 3, 0] + sib_in[k, 0].astype(F32)).astype(BF16)
        for e, d in enumerate((1, -1)):
            half = pl.ds(share * e, share)
            push(outgoing.at[k, 2, half], relay.at[k, e], k, 2 + e, d)
        for copy in crossing[1:]:
            copy.wait()
        local[chunk_rows(k), :] = own_part[k % 3, 3] + sib_in[k, 3].astype(F32)

    def push_near(k):
        for e, d in enumerate((1, -1)):
            copy_to(relay.at[k, e], relay.at[k, e], rs_s.at[k, 2 + e], rs_r.at[k, 2 + e], (sp, 2 * chip(d) + c)).wait_recv()
            half, rest = pl.ds(share * e, share), pl.ds(share * (1 - e), share)
            total = own_part[k % 3, 1 + e, half] + sib_in[k, 1 + e, half].astype(F32)
            outgoing[k, e, half] = (total + relay[k, e].astype(F32)).astype(BF16)
            total = own_part[k % 3, 1 + e, rest] + sib_in[k, 1 + e, rest].astype(F32)
            outgoing[k, e, rest] = total.astype(BF16)
            push(outgoing.at[k, e], parts.at[e, chunk_rows(k)], k, e, d)

    hidden(0)
    copy0 = compute(0)
    hidden(1)
    pass_on(0, copy0)
    copy1 = compute(1)
    hidden(2)
    pass_on(1, copy1)
    push_near(0)
    copy2 = compute(2)
    hidden(3)
    pass_on(2, copy2)
    push_near(1)
    copy3 = compute(3)
    pass_on(3, copy3)

    def parts_arrived(k):
        for e, d in enumerate((1, -1)):
            r = parts.at[e, chunk_rows(k)]
            copy_to(r, r, rs_s.at[k, e], rs_r.at[k, e], (sp, 2 * chip(d) + c)).wait_recv()

    lane_at = lax.broadcasted_iota(jnp.int32, (128, 128), 1)
    group = tiles // 2

    def row_sums(g):
        for t in range(group * g, group * g + group):
            r = pl.ds(128 * t, 128)
            y = local[r, :] + resid_scale * tok[r, my_cols].astype(F32)
            for e in range(2):
                y += parts[e, r, :].astype(F32)
            local[r, :] = y
            one = jnp.sum(y, axis=1, keepdims=True)
            two = jnp.sum(y * y, axis=1, keepdims=True)
            pair = jnp.where(lane_at == 0, one, jnp.where(lane_at == 1, two, 0.0))
            at_lane = 128 * (t - group * g)
            stat_out[g, :, at_lane : at_lane + 128] = jnp.transpose(pair)[0:2, :]
        for d in range(1, n_tp):
            copy = copy_to(stat_out.at[g], stat_in.at[g, d - 1], st_s.at[g, d - 1], st_r.at[g, d - 1], (sp, peer(d)))
            copy.start()
            sends.append(copy)

    def stats_arrived(g):
        for d in range(1, n_tp):
            dst = stat_in.at[g, d - 1]
            copy_to(dst, dst, st_s.at[g, d - 1], st_r.at[g, d - 1], (sp, peer(d))).wait_recv()

    def all_sent():
        for copy in sends + ring.sent + tg.sent:
            copy.wait_send()

    def second_norm(g):
        stats = stat_out[g]
        for d in range(1, n_tp):
            stats += stat_in[g, d - 1]
        mean = stats[0:1] * (1.0 / D)
        scale = lax.rsqrt(stats[1:2] * (1.0 / D) - mean * mean + norm_eps)
        lanes = pl.ds(128 * group * g, 128 * group)
        rowq[0:1, lanes] = mean
        rowq[1:2, lanes] = scale
        for t in range(group * g, group * g + group):
            r = pl.ds(128 * t, 128)
            both = jnp.transpose(rowq[:, 128 * t : 128 * t + 128])
            out[r, :] = ((local[r, :] - both[:, 0:1]) * both[:, 1:2] * last_gain[...].reshape(1, 256)).astype(BF16)

    push_near(2)
    parts_arrived(0)
    parts_arrived(1)
    row_sums(0)
    push_near(3)
    parts_arrived(2)
    parts_arrived(3)
    row_sums(1)
    stats_arrived(0)
    second_norm(0)
    stats_arrived(1)
    second_norm(1)
    all_sent()


def per_device(hv, em, rm, gate, step, sudden, document_index, rate, bias, tv, te, tr, gain,
               out_weight, stream, first_gain, last_gain, up_in, down_in):
    rows = hv.shape[0]
    docs = document_index.reshape(-1, 128)
    vmem = pl.BlockSpec(memory_space=pltpu.VMEM)
    dma = pltpu.SemaphoreType.DMA
    share = rows // 8
    return pl.pallas_call(
        layer_kernel,
        out_shape=jax.ShapeDtypeStruct((rows, 256), BF16),
        in_specs=[pl.BlockSpec(memory_space=pl.ANY)] * 8 + [vmem] * 3 + [pl.BlockSpec(memory_space=pltpu.SMEM)] * 2
        + [vmem] * 6,
        out_specs=vmem,
        scratch_shapes=[
            pltpu.VMEM((rows, 256), BF16), pltpu.VMEM((rows, 128), BF16), pltpu.VMEM((rows, 128), BF16),
            pltpu.VMEM((rows, 256), BF16), pltpu.VMEM((rows, 256), BF16), pltpu.VMEM((256, D), BF16),
            pltpu.VMEM((16, 256), BF16), pltpu.VMEM((16, 128), BF16), pltpu.VMEM((16, 128), BF16),
            pltpu.VMEM((16, 256), BF16), pltpu.VMEM((16, 128), BF16), pltpu.VMEM((16, 128), BF16),
            pltpu.VMEM((24, rows), F32), pltpu.VMEM((8, 256), F32),
            pltpu.VMEM((rows + 16, 512), F32),
            pltpu.VMEM((128, rows), F32),
            pltpu.VMEM((rows, 128), F32),
            pltpu.VMEM((rows, 256), BF16), pltpu.VMEM((rows, 128), BF16), pltpu.VMEM((rows, 128), F32),
            pltpu.VMEM((rows, 128), BF16),
            pltpu.VMEM((2, 128, rows), F32),
            pltpu.VMEM((rows, 256), F32),
            pltpu.VMEM((STATE + 16, 256), BF16), pltpu.VMEM((STATE + 16, 256), BF16),
            pltpu.VMEM((2, STATE + 16, 256), BF16), pltpu.VMEM((2, STATE + 16, 256), BF16),
            pltpu.VMEM((STATE + 16, 256), BF16), pltpu.VMEM((STATE + 16, 256), BF16),
            pltpu.VMEM((3, STATE + 16, 256), BF16), pltpu.VMEM((3, STATE + 16, 256), BF16),
            pltpu.VMEM((2, STATE, 256), F32),
            pltpu.VMEM((D, 1024), BF16), pltpu.VMEM((D, 1024), BF16),
            pltpu.VMEM((rows, 256), BF16), pltpu.VMEM((4, share, D), BF16), pltpu.VMEM((4, share, D), BF16),
            pltpu.VMEM((4, share, D), F32), pltpu.VMEM((share, D), BF16), pltpu.VMEM((2, share, D), BF16),
            pltpu.VMEM((2, share // 2, D), BF16), pltpu.VMEM((2, share, D), BF16), pltpu.VMEM((share, D), BF16),
            pltpu.VMEM((8, D), F32), pltpu.VMEM((share, D), F32), pltpu.VMEM((rows, D), BF16),
            pltpu.VMEM((2 * share, 1024), BF16),
            pltpu.VMEM((4, 4, 2 * share, 256), BF16), pltpu.VMEM((4, 4, 2 * share, 256), BF16),
            pltpu.VMEM((3, 4, 2 * share, 256), F32), pltpu.VMEM((4, 3, 2 * share, 256), BF16),
            pltpu.VMEM((2, rows, 256), BF16), pltpu.VMEM((4, 2, share, 256), BF16), pltpu.VMEM((2, 2, rows // 2), F32),
            pltpu.VMEM((2, 7, 2, rows // 2), F32),
            dma((8,)), dma((6,)), dma((6,)), dma((10,)), dma((10,)),
            dma((2,)), dma((2,)), dma((2,)), dma((2,)), dma((2, 4, 4)), dma((2, 4, 4)),
            dma((2, 4)), dma((2, 4)), dma((8, 2)), dma((8, 2)), dma((8, 2)), dma((8, 2)),
            dma((10,)), dma((10,)), dma((8,)), dma((8,)), dma((2, 7)), dma((2, 7)),
            dma((4, 2)), dma((4, 2)), dma((4, 4)), dma((4, 4)), dma((2, 7)), dma((2, 7)),
        ],
        compiler_params=pltpu.CompilerParams(
            collective_id=0, has_side_effects=True, vmem_limit_bytes=60 * 1024 * 1024),
        cost_estimate=pl.CostEstimate(flops=9_000_000_000, bytes_accessed=8_000_000, transcendentals=0),
        name="layer",
    )(hv, em, rm, gate, stream, out_weight, up_in, down_in, step.T, sudden.T, docs, rate, bias, tv, te, tr, gain,
      first_gain, last_gain)


SPECS = (
    P("sp", "tp"), P("sp", "tp"), P("sp", "tp"), P("sp", "tp"), P("sp", "tp"), P("sp", "tp"), P(),
    P(None, "tp"), P(None, "tp"), P(None, "tp"), P(None, "tp"), P(None, "tp"), P("tp"),
    P("tp", None), P("sp", "tp"), P("tp"), P("tp"), P("sp", "tp"), P("sp", "tp"),
)


def solution(mesh):
    return jax.shard_map(per_device, mesh=mesh, in_specs=SPECS, out_specs=P("sp", "tp"), check_vma=False)
```

```python
import functools

import jax
import jax.numpy as jnp
from jax import lax
from jax.experimental import pallas as pl
from jax.experimental.pallas import tpu as pltpu
from jax.sharding import PartitionSpec as P

D = 2048
HEAD_DIM = 64
STATE = 128
REACH = 8
MESH = pl.DeviceIdType.MESH
norm_eps = 1e-05
resid_scale = 1.4142135623730951
F32 = jnp.float32
BF16 = jnp.bfloat16


def lanes_of(cols, rows, base):
    n = rows.size
    low = lax.broadcasted_iota(jnp.int32, (n, 128), 1) < HEAD_DIM
    halves = []
    for k in (0, 2):
        a = jnp.broadcast_to(cols[rows, base + k : base + k + 1], (n, 128))
        b = jnp.broadcast_to(cols[rows, base + k + 1 : base + k + 2], (n, 128))
        halves.append(jnp.where(low, a, b))
    return jnp.concatenate(halves, axis=1)


def head_lanes(column):
    return jnp.concatenate([jnp.broadcast_to(c, (1, HEAD_DIM)) for c in column], axis=1)


C0, D1, W0, W1, A0, A1, DT0, CM, DOC = 0, 4, 8, 12, 16, 20, 24, 28, 33


def copy_to(src, dst, send, recv, device):
    return pltpu.make_async_remote_copy(src_ref=src, dst_ref=dst, send_sem=send, recv_sem=recv,
                                        device_id=device, device_id_type=MESH)


class WeightRing:
    def __init__(self, up_in, down_in, up, down, turned, sems, sp, tp):
        (self.uy_s, self.uy_r, self.uh_s, self.uh_r, self.uz_s, self.uz_r,
         self.dz_s, self.dz_r, self.dy_s, self.dy_r, self.dh_s, self.dh_r) = sems
        self.up_in, self.down_in, self.up, self.down, self.tp = up_in, down_in, up, down, tp
        self.turned = turned
        self.y, self.z = lax.rem(sp, 4), sp // 4
        self.sent = []

    def dev(self, dz, dy):
        return (lax.rem(self.z + dz + 8, 8) * 4 + lax.rem(self.y + dy + 4, 4), self.tp)

    def rows(self, dz, dy, low=0, count=64):
        shard = lax.rem(self.z + dz + 8, 8) * 4 + lax.rem(self.y + dy + 4, 4)
        return pl.ds(pl.multiple_of(shard * 64 + low, 32), count)

    def send(self, src, dst, send, recv, device):
        copy = copy_to(src, dst, send, recv, device)
        copy.start()
        self.sent.append(copy)

    def arrived(self, dst, send, recv):
        copy_to(dst, dst, send, recv, self.dev(1, 0)).wait_recv()

    def up_z(self, s, p, receive):
        for m, sign in enumerate((1, -1)):
            low, count = (32 * m, 32) if s == 3 else (0, 64)
            if receive:
                r = self.rows(-sign * (s + 1), p, low, count)
                self.arrived(self.up.at[r], self.uz_s.at[m, s, p], self.uz_r.at[m, s, p])
            else:
                r = self.rows(-sign * s, p, low, count)
                src = self.up_in if s == 0 and p == 0 else self.up.at[r]
                self.send(src, self.up.at[r], self.uz_s.at[m, s, p], self.uz_r.at[m, s, p], self.dev(sign, 0))

    def down_z(self, s, receive):
        for m, sign in enumerate((1, -1)):
            low, count = (32 * m, 32) if s == 3 else (0, 64)
            if receive:
                r = self.rows(-sign * (s + 1), 0, low, count)
                self.arrived(self.down.at[r], self.dz_s.at[m, s], self.dz_r.at[m, s])
            else:
                r = self.rows(-sign * s, 0, low, count)
                src = self.down_in if s == 0 else self.down.at[r]
                self.send(src, self.down.at[r], self.dz_s.at[m, s], self.dz_r.at[m, s], self.dev(sign, 0))

    def planes(self, s):
        return [(0, 0)] if s == 0 else [(7, 4)] if s == 4 else [(2 * s - 1, -s), (2 * s, s)]

    def down_y(self, s):
        for k, dz in self.planes(s):
            for m, sign in enumerate((1, -1)):
                r = self.rows(dz, 0)
                src = self.down_in if s == 0 else self.down.at[r]
                self.send(src, self.down.at[r], self.dy_s.at[k, m], self.dy_r.at[k, m], self.dev(0, sign))

    def down_half(self, s, receive):
        for k, dz in self.planes(s):
            for m, sign in enumerate((1, -1)):
                if receive:
                    r = self.rows(dz, -2 * sign, 32 * m, 32)
                    self.arrived(self.down.at[r], self.dh_s.at[k, m], self.dh_r.at[k, m])
                else:
                    self.arrived(self.down.at[self.rows(dz, -sign)], self.dy_s.at[k, m], self.dy_r.at[k, m])
                    r = self.rows(dz, -sign, 32 * m, 32)
                    self.send(self.down.at[r], self.down.at[r], self.dh_s.at[k, m], self.dh_r.at[k, m],
                              self.dev(0, sign))

    def up_step(self, n):
        s, part = divmod(n, 3)
        if part == 0:
            if s == 0:
                for m, sign in enumerate((1, -1)):
                    self.send(self.up_in, self.up.at[self.rows(0, 0)], self.uy_s.at[m], self.uy_r.at[m],
                              self.dev(0, sign))
            else:
                self.up_z(s - 1, 0, True)
            if s < 4:
                self.up_z(s, 0, False)
        elif part == 1:
            if s == 0:
                for m, sign in enumerate((1, -1)):
                    self.arrived(self.up.at[self.rows(0, -sign)], self.uy_s.at[m], self.uy_r.at[m])
                    r = self.rows(0, -sign, 32 * m, 32)
                    self.send(self.up.at[r], self.up.at[r], self.uh_s.at[m], self.uh_r.at[m], self.dev(0, sign))
            else:
                self.up_z(s - 1, 1, True)
                self.up_z(s - 1, 3, True)
            if s < 4:
                self.up_z(s, 1, False)
                self.up_z(s, 3, False)
        else:
            if s == 0:
                for m, sign in enumerate((1, -1)):
                    self.arrived(self.up.at[self.rows(0, -2 * sign, 32 * m, 32)], self.uh_s.at[m], self.uh_r.at[m])
            else:
                self.up_z(s - 1, 2, True)
            if s < 4:
                self.up_z(s, 2, False)

    def down_step(self, s):
        if s > 0:
            self.down_z(s - 1, True)
        if s < 4:
            self.down_z(s, False)
        self.down_y(s)

    def turn(self, s):
        self.down_half(s, True)
        for _, dz in self.planes(s):
            plane = lax.rem(self.z + dz + 8, 8)
            span = pl.ds(pl.multiple_of(plane * 256, 256), 256)
            for j in range(4):
                block = self.down[span, 256 * j : 256 * j + 256]
                self.turned[256 * j : 256 * j + 256, span] = jnp.transpose(block)


class TpGather:
    def __init__(self, buf, size, send, recv, sp, tp):
        self.buf, self.size, self.s, self.r, self.sp = buf, size, send, recv, sp
        self.x, self.c = tp // 2, lax.rem(tp, 2)
        self.sent = []

    def slot(self, dx, other):
        return lax.rem(self.x + dx + 4, 4) * 2 + (1 - self.c if other else self.c)

    def rows(self, dx, other, half=None):
        low, count = (0, self.size) if half is None else (half * (self.size // 2), self.size // 2)
        return self.buf.at[pl.ds(pl.multiple_of(self.slot(dx, other) * self.size + low, 16), count)]

    def send(self, src, dst, k, dx, other):
        copy = copy_to(src, dst, self.s.at[k], self.r.at[k], (self.sp, self.slot(dx, other)))
        copy.start()
        self.sent.append(copy)

    def arrived(self, dst, k):
        copy_to(dst, dst, self.s.at[k], self.r.at[k], (self.sp, self.slot(0, True))).wait_recv()

    def begin(self):
        for half in range(2):
            for k, dx in ((0, 1), (1, -1)):
                part = half if dx == 1 else 1 - half
                mine = self.rows(0, False, part)
                self.send(mine, mine, k + 8 * half, dx, False)
        self.send(self.rows(0, False), self.rows(0, False), 2, 0, True)

    def relay(self):
        left, right = self.rows(-1, False), self.rows(1, False)
        self.arrived(self.rows(-1, False, 0), 0)
        self.send(self.rows(-1, False, 0), self.rows(-1, False, 0), 3, 1, False)
        self.arrived(self.rows(1, False, 1), 1)
        self.send(self.rows(1, False, 1), self.rows(1, False, 1), 4, -1, False)
        self.arrived(self.rows(-1, False, 1), 8)
        self.send(left, left, 5, 0, True)
        self.arrived(self.rows(1, False, 0), 9)
        self.send(right, right, 6, 0, True)

    def far(self):
        self.arrived(self.rows(2, False, 0), 3)
        self.arrived(self.rows(2, False, 1), 4)
        self.send(self.rows(2, False), self.rows(2, False), 7, 0, True)

    def sibling(self, k):
        self.arrived(self.rows({2: 0, 5: -1, 6: 1, 7: 2}[k], True), k)


def layer_kernel(
    hv_any, em_any, rm_any, gate_any, stream_any, wout_any, up_any, down_any,
    step_in, sudden_in, docs_in, rate, bias, tap_v, tap_e, tap_r, gain, first_gain, last_gain, out,
    hv, em, rm, gate, stream, wout_in,
    prev_v, prev_e, prev_r, next_v, next_e, next_r,
    per_token, gains_in, wide, rowq, cols, val, ent, ent32, rdo, weight, local,
    msg0, msg1, got0, got1, wmsg0, wmsg1, wgot0, wgot1, states,
    up, down, turned, norm_out, mix_sib, mix_got, mix_own, mix_far, mix_near, mix_relay, mix_in, stream_in, gains, first, tok, squares,
    sib_out, sib_in, own_part, outgoing, parts, relay, stat_out, stat_in,
    pull, halo_send, halo_recv, state_send, state_recv,
    uy_s, uy_r, uh_s, uh_r, uz_s, uz_r, dz_s, dz_r, dy_s, dy_r, dh_s, dh_r,
    mx_s, mx_r, tk_s, tk_r, ex_s, ex_r, sb_s, sb_r, rs_s, rs_r, st_s, st_r,
):
    sp, tp = lax.axis_index("sp"), lax.axis_index("tp")
    n_sp = lax.axis_size("sp")
    n_tp = lax.axis_size("tp")
    rows = hv.shape[0]
    tiles = rows // 128
    share = rows // n_tp

    def at(d):
        return (lax.rem(sp + d + n_sp, n_sp), tp)

    def peer(d):
        return lax.rem(tp + d + n_tp, n_tp)

    own_rows = pl.ds(pl.multiple_of(sp * 64, 64), 64)
    up_in, down_in = up.at[own_rows], down.at[own_rows]
    barrier = pltpu.get_barrier_semaphore()
    gains_in[...] = jnp.broadcast_to(first_gain[...].reshape(1, 256), (8, 256))
    for d in range(1, REACH + 1):
        for s in (d, -d):
            pl.semaphore_signal(barrier, inc=1, device_id=at(s), device_id_type=MESH)
    for d in range(1, n_tp):
        pl.semaphore_signal(barrier, inc=1, device_id=(sp, peer(d)), device_id_type=MESH)
    pulls = [pltpu.make_async_copy(src, dst, pull.at[k]) for k, (src, dst) in enumerate((
        (hv_any, hv), (em_any, em), (rm_any, rm), (up_any, up_in), (down_any, down_in), (stream_any, stream),
        (gate_any, gate), (wout_any, wout_in)))]
    for copy in pulls:
        copy.start()
    pl.semaphore_wait(barrier, 2 * REACH + n_tp - 1)
    for copy in pulls:
        copy.wait()

    halos = []
    for k, (src, low, high) in enumerate(((hv, prev_v, next_v), (em, prev_e, next_e), (rm, prev_r, next_r))):
        for m, (start, dst, step) in enumerate(((rows - 16, low, 1), (0, high, -1))):
            halos.append(copy_to(src.at[pl.ds(start, 16)], dst, halo_send.at[2 * k + m], halo_recv.at[2 * k + m],
                                 at(step)))
    for copy in halos:
        copy.start()
    ring = WeightRing(up_in, down_in, up, down, turned,
                      (uy_s, uy_r, uh_s, uh_r, uz_s, uz_r, dz_s, dz_r, dy_s, dy_r, dh_s, dh_r), sp, tp)
    ring.up_step(0)
    ring.down_step(0)

    def my_lanes(ref, q):
        return ref.at[:, pl.ds(pl.multiple_of(q * 256, 256), 256)]

    def exchange(k, src_of, dst):
        sent = []
        for d in range(1, n_tp):
            q = peer(d)
            copy = copy_to(src_of(q), my_lanes(dst, tp), ex_s.at[k, d - 1], ex_r.at[k, d - 1], (sp, q))
            copy.start()
            sent.append(copy)
        return sent

    def exchanged(k, dst):
        for d in range(1, n_tp):
            r = my_lanes(dst, peer(-d))
            copy_to(r, r, ex_s.at[k, d - 1], ex_r.at[k, d - 1], (sp, peer(d))).wait_recv()

    def token_rows(ref):
        return lambda q: ref.at[pl.ds(pl.multiple_of(q * share, 16), share)]

    sends = exchange(0, token_rows(stream), stream_in)
    sends += exchange(1, lambda q: gains_in, gains)
    mine = pl.ds(pl.multiple_of(tp * share, 16), share)
    my_cols = pl.ds(pl.multiple_of(tp * 256, 256), 256)
    stream_in[:, my_cols] = stream[mine, :]
    gains[:, my_cols] = gains_in[...]

    raw = step_in[...].astype(F32)
    sudden = sudden_in[...]

    def eight(ref):
        return jnp.concatenate([jnp.full((1, rows), ref[k, h], F32) for k in range(2) for h in range(4)], axis=0)

    before_softplus = jnp.concatenate([raw, raw], axis=0) + eight(bias)
    per_token[0:8, :] = jnp.maximum(before_softplus, 0.0) + jnp.log1p(jnp.exp(-jnp.abs(before_softplus)))
    per_token[8:16, :] = -jnp.exp(eight(rate)) * per_token[0:8, :] + jnp.concatenate([sudden, sudden], axis=0)

    def doc_at(row, lane_no):
        return docs_in[pl.ds(row, 1), lane_no : lane_no + 1].astype(F32)

    own_doc = jnp.concatenate([docs_in[pl.ds(tiles * sp + t, 1), :] for t in range(tiles)], axis=1).astype(F32)
    own8 = jnp.broadcast_to(own_doc, (8, rows))
    low_row, high_row = jnp.maximum(tiles * sp - 1, 0), jnp.minimum(tiles * sp + tiles, tiles * n_sp - 1)
    prev_two, prev_one = (jnp.where(sp > 0, doc_at(low_row, k), -1.0) for k in (126, 127))
    next_one, next_two = (jnp.where(sp < n_sp - 1, doc_at(high_row, k), -1.0) for k in (0, 1))
    lane8 = lax.broadcasted_iota(jnp.int32, (8, rows), 1)
    back_one = jnp.where(lane8 == 0, prev_one, pltpu.roll(own8, 1, 1))
    back_two = jnp.where(lane8 == 0, prev_two, jnp.where(lane8 == 1, prev_one, pltpu.roll(own8, 2, 1)))
    on_one = jnp.where(lane8 == rows - 1, next_one, pltpu.roll(own8, rows - 1, 1))
    on_two = jnp.where(lane8 == rows - 1, next_two, jnp.where(lane8 == rows - 2, next_one, pltpu.roll(own8, rows - 2, 1)))
    for k, row in enumerate((back_two, back_one, own8, on_one, on_two)):
        per_token[16 + k : 17 + k, :] = row[0:1]
    per_token[21:22, :] = jnp.broadcast_to(prev_one, (1, rows))
    per_token[22:23, :] = jnp.broadcast_to(next_one, (1, rows))
    per_token[23:24, :] = jnp.zeros((1, rows), F32)

    def last_doc(d):
        return doc_at(tiles * lax.rem(sp - d + n_sp, n_sp) + tiles - 1, 127)

    def first_doc(d):
        return doc_at(tiles * lax.rem(sp + d, n_sp), 0)

    source_mask = []
    for edge, room in ((last_doc, sp), (first_doc, n_sp - 1 - sp)):
        for d, to in ((1, 0), (2, 0), (4, 1), (7, 1)):
            source_mask.append(jnp.where((edge(d) == edge(to)) & (room >= d), 1.0, 0.0))

    dt = per_token[0:8, :]
    log_decay = per_token[8:16, :]
    lane = lax.broadcasted_iota(jnp.int32, (8, rows), 1)
    total = log_decay
    shift = 1
    while shift < rows:
        total = total + jnp.where(lane >= shift, pltpu.roll(total, shift, 1), 0.0)
        shift *= 2
    c0 = total[0:4]
    d1 = total[4:8] - log_decay[4:8]
    all0, all1 = total[0:4, rows - 1 : rows], total[4:8, rows - 1 : rows]
    docs = per_token[16:24, :]
    own = docs[2:3]
    same_end = jnp.where(own == own[:, rows - 1 : rows], 1.0, 0.0)
    same_start = jnp.where(own == own[:, 0:1], 1.0, 0.0)
    from_prev = jnp.where(own == docs[5:6], 1.0, 0.0)
    from_next = jnp.where(own == docs[6:7], 1.0, 0.0)
    rowq[...] = jnp.zeros_like(rowq)
    rowq[C0 : C0 + 4, :] = c0
    rowq[D1 : D1 + 4, :] = d1
    rowq[W0 : W0 + 4, :] = jnp.exp(all0 - c0) * dt[0:4] * same_end
    rowq[W1 : W1 + 4, :] = jnp.exp(d1) * dt[4:8] * same_start
    rowq[A0 : A0 + 4, :] = jnp.exp(c0) * from_prev
    rowq[A1 : A1 + 4, :] = jnp.exp(all1 - d1) * from_next
    rowq[DT0 : DT0 + 4, :] = dt[0:4]
    rowq[CM : CM + 5, :] = jnp.where(docs[0:5] == own, 1.0, 0.0)
    rowq[DOC : DOC + 1, :] = own
    for t in range(tiles):
        cols[pl.ds(128 * t, 128), :] = jnp.transpose(rowq[:, 128 * t : 128 * t + 128])

    wide[8 : 8 + rows, 0:256] = hv[...].astype(F32)
    wide[8 : 8 + rows, 256:384] = em[...].astype(F32)
    wide[8 : 8 + rows, 384:512] = rm[...].astype(F32)
    whole_taps = tap_v[...].astype(F32)
    taps = (whole_taps[:, 0:128], whole_taps[:, 128:256], tap_e[...].astype(F32), tap_r[...].astype(F32))

    def convolve(t):
        lo = 128 * t
        masks = [jnp.broadcast_to(cols[lo : lo + 128, CM + o : CM + o + 1], (128, 128)) for o in range(5)]
        for g in range(4):
            acc = jnp.zeros((128, 128), F32)
            for o in range(5):
                part = wide[lo + 6 + o : lo + 134 + o, 128 * g : 128 * g + 128]
                if o != 2:
                    part = part * masks[o]
                acc = acc + taps[g][o : o + 1] * part
            act = acc * jax.nn.sigmoid(acc)
            if g < 2:
                val[lo : lo + 128, 128 * g : 128 * g + 128] = act.astype(BF16)
            elif g == 2:
                ent32[lo : lo + 128, :] = act
                ent[lo : lo + 128, :] = act.astype(BF16)
            else:
                rdo[lo : lo + 128, :] = act.astype(BF16)

    def state_of(t, state0, state1):
        r = pl.ds(128 * t, 128)
        ent_t = jnp.transpose(ent32[r, :]).astype(BF16)
        v = val[r, :].astype(F32)
        state0 += jnp.dot(ent_t, (v * lanes_of(cols, r, W0)).astype(BF16), preferred_element_type=F32)
        state1 += jnp.dot(ent_t, (v * lanes_of(cols, r, W1)).astype(BF16), preferred_element_type=F32)
        return state0, state1

    state0 = state1 = jnp.zeros((STATE, 256), F32)
    for t in range(1, tiles - 1):
        convolve(t)
        state0, state1 = state_of(t, state0, state1)
    for copy in halos:
        copy.wait()
    wide[0:8, 0:256] = prev_v[8:16, :].astype(F32)
    wide[0:8, 256:384] = prev_e[8:16, :].astype(F32)
    wide[0:8, 384:512] = prev_r[8:16, :].astype(F32)
    wide[8 + rows : 16 + rows, 0:256] = next_v[0:8, :].astype(F32)
    wide[8 + rows : 16 + rows, 256:384] = next_e[0:8, :].astype(F32)
    wide[8 + rows : 16 + rows, 384:512] = next_r[0:8, :].astype(F32)

    for t in (0, tiles - 1):
        convolve(t)
        state0, state1 = state_of(t, state0, state1)

    def fill(msg, state, passing):
        msg[0:STATE, :] = state.astype(BF16)
        coarse = passing.astype(BF16)
        fine = (passing - coarse.astype(F32)).astype(BF16)
        row = lax.broadcasted_iota(jnp.int32, (16, 256), 0)
        both = jnp.where(row == 0, coarse.astype(F32), jnp.where(row == 1, fine.astype(F32), 0.0))
        msg[STATE : STATE + 16, :] = both.astype(BF16)

    def passing_of(msg):
        tail = msg[STATE : STATE + 16, :].astype(F32)
        return tail[0:1] + tail[1:2]

    pass_own = [head_lanes([jnp.exp(whole[h : h + 1, :]) for h in range(4)]) for whole in (all0, all1)]
    for m, (msg, state) in enumerate(((msg0, state0), (msg1, state1))):
        states[m] = state
        fill(msg, state, pass_own[m])

    for t in range(tiles):
        r = pl.ds(128 * t, 128)
        own_score = jnp.sum(rdo[r, :].astype(F32) * ent[r, :].astype(F32), axis=1, keepdims=True)
        local[r, :] = own_score * lanes_of(cols, r, DT0) * val[r, :].astype(F32)

    near_sends = []
    for k, d in enumerate((1, 2)):
        for m, (msg, got, step) in enumerate(((msg0, got0, d), (msg1, got1, -d))):
            near_sends.append(copy_to(msg, got.at[k], state_send.at[2 * k + m], state_recv.at[2 * k + m], at(step)))
    for copy in near_sends:
        copy.start()
    ring.down_step(1)
    ring.up_step(1)
    ring.down_half(0, False)

    low_lane = lax.broadcasted_iota(jnp.int32, (128, 128), 1) < HEAD_DIM

    def tile_step(i, _):
        r = pl.ds(pl.multiple_of(i * 128, 128), 128)
        here = rdo[r, :]
        doc_t = jnp.broadcast_to(cols[r, DOC : DOC + 1], (128, 128))
        t_index = lax.broadcasted_iota(jnp.int32, (128, 128), 0) + i * 128
        for pair in range(2):
            outs = []
            for h in (2 * pair, 2 * pair + 1):
                ct = jnp.broadcast_to(cols[r, C0 + h : C0 + h + 1], (128, 128))
                dd = jnp.broadcast_to(cols[r, D1 + h : D1 + h + 1], (128, 128))
                for j in range(tiles):
                    s = pl.ds(128 * j, 128)
                    if h == 0:
                        score = lax.dot_general(here, ent[s, :], (((1,), (1,)), ((), ())), preferred_element_type=F32)
                        score = jnp.where(doc_t == per_token[18:19, 128 * j : 128 * j + 128], score, 0.0)
                        weight[1, :, 128 * j : 128 * j + 128] = score
                    score = weight[1, :, 128 * j : 128 * j + 128]
                    s_index = lax.broadcasted_iota(jnp.int32, (128, 128), 1) + 128 * j
                    spread = jnp.minimum(ct - rowq[C0 + h : C0 + h + 1, 128 * j : 128 * j + 128],
                                         rowq[D1 + h : D1 + h + 1, 128 * j : 128 * j + 128] - dd)
                    step = jnp.where(s_index < t_index, per_token[h : h + 1, 128 * j : 128 * j + 128],
                                     per_token[4 + h : 5 + h, 128 * j : 128 * j + 128])
                    weight[0, :, 128 * j : 128 * j + 128] = score * jnp.exp(spread) * step
                outs.append(jnp.dot(weight[0].astype(BF16), val[:, 128 * pair : 128 * pair + 128],
                                    preferred_element_type=F32))
            local[r, 128 * pair : 128 * pair + 128] += jnp.where(low_lane, outs[0], outs[1])
        return 0

    lax.fori_loop(0, tiles // 2, tile_step, 0)
    for copy in near_sends:
        copy.wait()
    for m, (got, wmsg) in enumerate(((got0, wmsg0), (got1, wmsg1))):
        through = [pass_own[m]]
        for k in range(2):
            through.append(through[k] * passing_of(got.at[k]))
        window = states[m]
        for k in range(2):
            window += got[k, 0:STATE, :].astype(F32) * (through[k] * source_mask[4 * m + k])
        fill(wmsg, window, through[2])
    far_sends = []
    lax.fori_loop(tiles // 2, tiles // 2 + 1, tile_step, 0)
    for k, d in enumerate((1, 4, 7)):
        for m, (wmsg, wgot, step) in enumerate(((wmsg0, wgot0, d), (wmsg1, wgot1, -d))):
            n = 4 + 2 * k + m
            far_sends.append(copy_to(wmsg, wgot.at[k], state_send.at[n], state_recv.at[n], at(step)))
    for copy in far_sends:
        copy.start()
    lax.fori_loop(tiles // 2 + 1, tiles, tile_step, 0)
    ring.down_step(2)
    ring.up_step(3)
    for copy in far_sends:
        copy.wait()
    ring.up_step(2)
    ring.up_step(4)
    carried = []
    for m, wgot in enumerate((wgot0, wgot1)):
        once = passing_of(wgot.at[0])
        twice = once * passing_of(wgot.at[1])
        state = (wgot[0, 0:STATE, :].astype(F32)
                 + wgot[1, 0:STATE, :].astype(F32) * (once * source_mask[4 * m + 2])
                 + wgot[2, 0:STATE, :].astype(F32) * (twice * source_mask[4 * m + 3]))
        carried.append(state.astype(BF16))

    for t in range(tiles):
        r = pl.ds(128 * t, 128)
        here = rdo[r, :]
        y = local[r, :]
        y += jnp.dot(here, carried[0], preferred_element_type=F32) * lanes_of(cols, r, A0)
        y += jnp.dot(here, carried[1], preferred_element_type=F32) * lanes_of(cols, r, A1)
        z = gate[r, :].astype(F32)
        y = y * (z * jax.nn.sigmoid(z))
        y = y * lax.rsqrt(jnp.mean(y * y, axis=1, keepdims=True) + norm_eps)
        norm_out[r, :] = (y * gain[...].reshape(1, 256)).astype(BF16)

    x, c = tp // 2, lax.rem(tp, 2)
    half_share = share // 2

    def chip(d):
        return lax.rem(x + d + 4, 4)

    def project(k, d):
        for other in (True, False):
            q = 2 * chip(d) + (1 - c if other else c)
            part = jnp.dot(norm_out[pl.ds(pl.multiple_of(q * share, 16), share), :], wout_in[...],
                           preferred_element_type=F32)
            if other:
                mix_sib[k] = part.astype(BF16)
            else:
                mix_own[k] = part
        copy = copy_to(mix_sib.at[k], mix_got.at[k], mx_s.at[k], mx_r.at[k], (sp, 2 * x + 1 - c))
        copy.start()
        return copy

    def mix_push(src, dst, n, d):
        copy = copy_to(src, dst, mx_s.at[n], mx_r.at[n], (sp, 2 * chip(d) + c))
        copy.start()
        sends.append(copy)

    def mix_arrived(dst, n):
        copy_to(dst, dst, mx_s.at[n], mx_r.at[n], (sp, 2 * x + 1 - c)).wait_recv()

    def mix_far_out():
        crossing[0].wait()
        mix_far[...] = (mix_own[0] + mix_got[0].astype(F32)).astype(BF16)
        for e, d in enumerate((1, -1)):
            mix_push(mix_far.at[pl.ds(half_share * e, half_share)], mix_relay.at[e], 4 + e, d)
        return [sends.pop(), sends.pop()]

    def mix_near_rest():
        for copy in far_out:
            copy.wait_send()
        for e, d in enumerate((1, -1)):
            crossing[1 + e].wait()
            rest = pl.ds(half_share * (1 - e), half_share)
            mix_near[e, rest] = (mix_own[1 + e, rest] + mix_got[1 + e, rest].astype(F32)).astype(BF16)
            mix_push(mix_near.at[e, rest], mix_in.at[e, rest], 6 + e, d)
        crossing[3].wait()

    def mix_near_last():
        for e, d in enumerate((1, -1)):
            mix_arrived(mix_relay.at[e], 4 + e)
            half = pl.ds(half_share * e, half_share)
            total = mix_own[1 + e, half] + mix_got[1 + e, half].astype(F32) + mix_relay[e].astype(F32)
            mix_near[e, half] = total.astype(BF16)
            mix_push(mix_near.at[e, half], mix_in.at[e, half], 8 + e, d)

    def mix_finish():
        for e in range(2):
            mix_arrived(mix_in.at[e, pl.ds(half_share * (1 - e), half_share)], 6 + e)
            mix_arrived(mix_in.at[e, pl.ds(half_share * e, half_share)], 8 + e)
        first[...] = (resid_scale * stream_in[...].astype(F32) + mix_own[3] + mix_got[3].astype(F32)
                      + mix_in[0].astype(F32) + mix_in[1].astype(F32))

    crossing = [project(0, 2)]
    crossing.append(project(1, 1))
    far_out = mix_far_out()
    crossing.append(project(2, -1))
    crossing.append(project(3, 0))
    ring.up_step(6)
    ring.down_half(1, False)
    ring.down_step(3)
    mix_near_rest()
    ring.up_step(5)
    ring.down_half(2, False)
    mix_near_last()
    ring.turn(0)
    ring.turn(1)
    ring.up_step(7)
    ring.up_step(9)
    ring.down_step(4)
    ring.down_half(3, False)
    exchanged(0, stream_in)
    exchanged(1, gains)
    mix_finish()
    f = first[...]
    mean = jnp.sum(f, axis=1, keepdims=True) * (1.0 / D)
    var = jnp.sum(f * f, axis=1, keepdims=True) * (1.0 / D) - mean * mean
    tok[mine, :] = ((f - mean) * lax.rsqrt(var + norm_eps) * gains[0:1, :]).astype(BF16)
    tg = TpGather(tok, share, tk_s, tk_r, sp, tp)
    tg.begin()
    ring.up_step(8)
    ring.up_step(10)
    ring.turn(2)
    ring.down_half(4, False)
    tg.relay()
    ring.up_step(11)
    ring.up_step(12)
    ring.turn(3)
    ring.up_step(13)
    tg.far()
    ring.up_step(14)
    ring.turn(4)
    for k in (2, 5, 6, 7):
        tg.sibling(k)

    def chunk_rows(k):
        return pl.ds(2 * share * k, 2 * share)

    def hidden(k):
        chunk = tok[chunk_rows(k), :]
        for n in range(4):
            h = jnp.maximum(jnp.dot(chunk, up[:, 256 * n : 256 * n + 256], preferred_element_type=F32), 0.0)
            squares[:, 256 * n : 256 * n + 256] = (h * h).astype(BF16)

    def compute(k):
        sq = squares[...]
        for n, d in enumerate((2, 1, -1, 0)):
            for other in (True, False):
                q = 2 * chip(d) + (1 - c if other else c)
                w = turned[:, pl.ds(pl.multiple_of(q * 256, 256), 256)]
                part = jnp.dot(sq, w, preferred_element_type=F32)
                if other:
                    sib_out[k, n] = part.astype(BF16)
                else:
                    own_part[k % 3, n] = part
        crossing = []
        for n, r in enumerate((pl.ds(0, 1), pl.ds(1, 3))):
            copy = copy_to(sib_out.at[k, r], sib_in.at[k, r], sb_s.at[k, n], sb_r.at[k, n], (sp, 2 * x + 1 - c))
            copy.start()
            crossing.append(copy)
        return crossing

    def push(src, dst, k, e, d):
        copy = copy_to(src, dst, rs_s.at[k, e], rs_r.at[k, e], (sp, 2 * chip(d) + c))
        copy.start()
        sends.append(copy)

    def pass_on(k, crossing):
        crossing[0].wait()
        outgoing[k, 2] = (own_part[k % 3, 0] + sib_in[k, 0].astype(F32)).astype(BF16)
        for e, d in enumerate((1, -1)):
            half = pl.ds(share * e, share)
            push(outgoing.at[k, 2, half], relay.at[k, e], k, 2 + e, d)
        for copy in crossing[1:]:
            copy.wait()
        local[chunk_rows(k), :] = own_part[k % 3, 3] + sib_in[k, 3].astype(F32)

    def push_near(k):
        for e, d in enumerate((1, -1)):
            copy_to(relay.at[k, e], relay.at[k, e], rs_s.at[k, 2 + e], rs_r.at[k, 2 + e], (sp, 2 * chip(d) + c)).wait_recv()
            half, rest = pl.ds(share * e, share), pl.ds(share * (1 - e), share)
            total = own_part[k % 3, 1 + e, half] + sib_in[k, 1 + e, half].astype(F32)
            outgoing[k, e, half] = (total + relay[k, e].astype(F32)).astype(BF16)
            total = own_part[k % 3, 1 + e, rest] + sib_in[k, 1 + e, rest].astype(F32)
            outgoing[k, e, rest] = total.astype(BF16)
            push(outgoing.at[k, e], parts.at[e, chunk_rows(k)], k, e, d)

    hidden(0)
    copy0 = compute(0)
    hidden(1)
    pass_on(0, copy0)
    copy1 = compute(1)
    hidden(2)
    pass_on(1, copy1)
    push_near(0)
    copy2 = compute(2)
    hidden(3)
    pass_on(2, copy2)
    push_near(1)
    copy3 = compute(3)
    pass_on(3, copy3)

    def parts_arrived(k):
        for e, d in enumerate((1, -1)):
            r = parts.at[e, chunk_rows(k)]
            copy_to(r, r, rs_s.at[k, e], rs_r.at[k, e], (sp, 2 * chip(d) + c)).wait_recv()

    lane_at = lax.broadcasted_iota(jnp.int32, (128, 128), 1)
    group = tiles // 2

    def row_sums(g):
        for t in range(group * g, group * g + group):
            r = pl.ds(128 * t, 128)
            y = local[r, :] + resid_scale * tok[r, my_cols].astype(F32)
            for e in range(2):
                y += parts[e, r, :].astype(F32)
            local[r, :] = y
            one = jnp.sum(y, axis=1, keepdims=True)
            two = jnp.sum(y * y, axis=1, keepdims=True)
            pair = jnp.where(lane_at == 0, one, jnp.where(lane_at == 1, two, 0.0))
            at_lane = 128 * (t - group * g)
            stat_out[g, :, at_lane : at_lane + 128] = jnp.transpose(pair)[0:2, :]
        for d in range(1, n_tp):
            copy = copy_to(stat_out.at[g], stat_in.at[g, d - 1], st_s.at[g, d - 1], st_r.at[g, d - 1], (sp, peer(d)))
            copy.start()
            sends.append(copy)

    def stats_arrived(g):
        for d in range(1, n_tp):
            dst = stat_in.at[g, d - 1]
            copy_to(dst, dst, st_s.at[g, d - 1], st_r.at[g, d - 1], (sp, peer(d))).wait_recv()

    def all_sent():
        for copy in sends + ring.sent + tg.sent:
            copy.wait_send()

    def second_norm(g):
        stats = stat_out[g]
        for d in range(1, n_tp):
            stats += stat_in[g, d - 1]
        mean = stats[0:1] * (1.0 / D)
        scale = lax.rsqrt(stats[1:2] * (1.0 / D) - mean * mean + norm_eps)
        lanes = pl.ds(128 * group * g, 128 * group)
        rowq[0:1, lanes] = mean
        rowq[1:2, lanes] = scale
        for t in range(group * g, group * g + group):
            r = pl.ds(128 * t, 128)
            both = jnp.transpose(rowq[:, 128 * t : 128 * t + 128])
            out[r, :] = ((local[r, :] - both[:, 0:1]) * both[:, 1:2] * last_gain[...].reshape(1, 256)).astype(BF16)

    push_near(2)
    parts_arrived(0)
    parts_arrived(1)
    row_sums(0)
    push_near(3)
    parts_arrived(2)
    parts_arrived(3)
    row_sums(1)
    stats_arrived(0)
    second_norm(0)
    stats_arrived(1)
    second_norm(1)
    all_sent()


def per_device(hv, em, rm, gate, step, sudden, document_index, rate, bias, tv, te, tr, gain,
               out_weight, stream, first_gain, last_gain, up_in, down_in):
    rows = hv.shape[0]
    docs = document_index.reshape(-1, 128)
    vmem = pl.BlockSpec(memory_space=pltpu.VMEM)
    dma = pltpu.SemaphoreType.DMA
    share = rows // 8
    return pl.pallas_call(
        layer_kernel,
        out_shape=jax.ShapeDtypeStruct((rows, 256), BF16),
        in_specs=[pl.BlockSpec(memory_space=pl.ANY)] * 8 + [vmem] * 3 + [pl.BlockSpec(memory_space=pltpu.SMEM)] * 2
        + [vmem] * 6,
        out_specs=vmem,
        scratch_shapes=[
            pltpu.VMEM((rows, 256), BF16), pltpu.VMEM((rows, 128), BF16), pltpu.VMEM((rows, 128), BF16),
            pltpu.VMEM((rows, 256), BF16), pltpu.VMEM((rows, 256), BF16), pltpu.VMEM((256, D), BF16),
            pltpu.VMEM((16, 256), BF16), pltpu.VMEM((16, 128), BF16), pltpu.VMEM((16, 128), BF16),
            pltpu.VMEM((16, 256), BF16), pltpu.VMEM((16, 128), BF16), pltpu.VMEM((16, 128), BF16),
            pltpu.VMEM((24, rows), F32), pltpu.VMEM((8, 256), F32),
            pltpu.VMEM((rows + 16, 512), F32),
            pltpu.VMEM((128, rows), F32),
            pltpu.VMEM((rows, 128), F32),
            pltpu.VMEM((rows, 256), BF16), pltpu.VMEM((rows, 128), BF16), pltpu.VMEM((rows, 128), F32),
            pltpu.VMEM((rows, 128), BF16),
            pltpu.VMEM((2, 128, rows), F32),
            pltpu.VMEM((rows, 256), F32),
            pltpu.VMEM((STATE + 16, 256), BF16), pltpu.VMEM((STATE + 16, 256), BF16),
            pltpu.VMEM((2, STATE + 16, 256), BF16), pltpu.VMEM((2, STATE + 16, 256), BF16),
            pltpu.VMEM((STATE + 16, 256), BF16), pltpu.VMEM((STATE + 16, 256), BF16),
            pltpu.VMEM((3, STATE + 16, 256), BF16), pltpu.VMEM((3, STATE + 16, 256), BF16),
            pltpu.VMEM((2, STATE, 256), F32),
            pltpu.VMEM((D, 1024), BF16), pltpu.VMEM((D, 1024), BF16), pltpu.VMEM((1024, D), BF16),
            pltpu.VMEM((rows, 256), BF16), pltpu.VMEM((4, share, D), BF16), pltpu.VMEM((4, share, D), BF16),
            pltpu.VMEM((4, share, D), F32), pltpu.VMEM((share, D), BF16), pltpu.VMEM((2, share, D), BF16),
            pltpu.VMEM((2, share // 2, D), BF16), pltpu.VMEM((2, share, D), BF16), pltpu.VMEM((share, D), BF16),
            pltpu.VMEM((8, D), F32), pltpu.VMEM((share, D), F32), pltpu.VMEM((rows, D), BF16),
            pltpu.VMEM((2 * share, 1024), BF16),
            pltpu.VMEM((4, 4, 2 * share, 256), BF16), pltpu.VMEM((4, 4, 2 * share, 256), BF16),
            pltpu.VMEM((3, 4, 2 * share, 256), F32), pltpu.VMEM((4, 3, 2 * share, 256), BF16),
            pltpu.VMEM((2, rows, 256), BF16), pltpu.VMEM((4, 2, share, 256), BF16), pltpu.VMEM((2, 2, rows // 2), F32),
            pltpu.VMEM((2, 7, 2, rows // 2), F32),
            dma((8,)), dma((6,)), dma((6,)), dma((10,)), dma((10,)),
            dma((2,)), dma((2,)), dma((2,)), dma((2,)), dma((2, 4, 4)), dma((2, 4, 4)),
            dma((2, 4)), dma((2, 4)), dma((8, 2)), dma((8, 2)), dma((8, 2)), dma((8, 2)),
            dma((10,)), dma((10,)), dma((10,)), dma((10,)), dma((2, 7)), dma((2, 7)),
            dma((4, 2)), dma((4, 2)), dma((4, 4)), dma((4, 4)), dma((2, 7)), dma((2, 7)),
        ],
        compiler_params=pltpu.CompilerParams(
            collective_id=0, has_side_effects=True, vmem_limit_bytes=60 * 1024 * 1024),
        cost_estimate=pl.CostEstimate(flops=9_000_000_000, bytes_accessed=8_000_000, transcendentals=0),
        name="layer",
    )(hv, em, rm, gate, stream, out_weight, up_in, down_in, step.T, sudden.T, docs, rate, bias, tv, te, tr, gain,
      first_gain, last_gain)


SPECS = (
    P("sp", "tp"), P("sp", "tp"), P("sp", "tp"), P("sp", "tp"), P("sp", "tp"), P("sp", "tp"), P(),
    P(None, "tp"), P(None, "tp"), P(None, "tp"), P(None, "tp"), P(None, "tp"), P("tp"),
    P("tp", None), P("sp", "tp"), P("tp"), P("tp"), P("sp", "tp"), P("sp", "tp"),
)


def solution(mesh):
    return jax.shard_map(per_device, mesh=mesh, in_specs=SPECS, out_specs=P("sp", "tp"), check_vma=False)
```

```python
import functools

import jax
import jax.numpy as jnp
from jax import lax
from jax.experimental import pallas as pl
from jax.experimental.pallas import tpu as pltpu
from jax.sharding import PartitionSpec as P

D = 2048
HEAD_DIM = 64
STATE = 128
REACH = 8
CUT = 896
MESH = pl.DeviceIdType.MESH
norm_eps = 1e-05
resid_scale = 1.4142135623730951
F32 = jnp.float32
BF16 = jnp.bfloat16


def lanes_of(cols, rows, base):
    n = rows.size
    low = lax.broadcasted_iota(jnp.int32, (n, 128), 1) < HEAD_DIM
    halves = []
    for k in (0, 2):
        a = jnp.broadcast_to(cols[rows, base + k : base + k + 1], (n, 128))
        b = jnp.broadcast_to(cols[rows, base + k + 1 : base + k + 2], (n, 128))
        halves.append(jnp.where(low, a, b))
    return jnp.concatenate(halves, axis=1)


def head_lanes(column):
    return jnp.concatenate([jnp.broadcast_to(c, (1, HEAD_DIM)) for c in column], axis=1)


C0, D1, W0, W1, A0, A1, DT0, CM, DOC = 0, 4, 8, 12, 16, 20, 24, 28, 33


def copy_to(src, dst, send, recv, device):
    return pltpu.make_async_remote_copy(src_ref=src, dst_ref=dst, send_sem=send, recv_sem=recv,
                                        device_id=device, device_id_type=MESH)


class WeightRing:
    def __init__(self, up_in, down_in, up, down, turned, sems, sp, tp):
        (self.uy_s, self.uy_r, self.uh_s, self.uh_r, self.uz_s, self.uz_r,
         self.dz_s, self.dz_r, self.dy_s, self.dy_r, self.dh_s, self.dh_r) = sems
        self.up_in, self.down_in, self.up, self.down, self.tp = up_in, down_in, up, down, tp
        self.turned = turned
        self.y, self.z = lax.rem(sp, 4), sp // 4
        self.sent = []

    def dev(self, dz, dy):
        return (lax.rem(self.z + dz + 8, 8) * 4 + lax.rem(self.y + dy + 4, 4), self.tp)

    def rows(self, dz, dy, low=0, count=64):
        shard = lax.rem(self.z + dz + 8, 8) * 4 + lax.rem(self.y + dy + 4, 4)
        return pl.ds(pl.multiple_of(shard * 64 + low, 32), count)

    def send(self, src, dst, send, recv, device):
        copy = copy_to(src, dst, send, recv, device)
        copy.start()
        self.sent.append(copy)

    def arrived(self, dst, send, recv):
        copy_to(dst, dst, send, recv, self.dev(1, 0)).wait_recv()

    def up_z(self, s, p, receive):
        for m, sign in enumerate((1, -1)):
            low, count = (32 * m, 32) if s == 3 else (0, 64)
            r = self.rows(-sign * (s + 1 if receive else s), p, low, count)
            piece = self.up.at[r, pl.ds(0, CUT)]
            if receive:
                self.arrived(piece, self.uz_s.at[m, s, p], self.uz_r.at[m, s, p])
            else:
                self.send(piece, piece, self.uz_s.at[m, s, p], self.uz_r.at[m, s, p], self.dev(sign, 0))

    def both(self, r):
        return enumerate((self.down.at[r], self.up.at[r, pl.ds(CUT, 1024 - CUT)]))

    def down_z(self, s, receive):
        for m, sign in enumerate((1, -1)):
            low, count = (32 * m, 32) if s == 3 else (0, 64)
            r = self.rows(-sign * (s + 1 if receive else s), 0, low, count)
            for w, piece in self.both(r):
                if receive:
                    self.arrived(piece, self.dz_s.at[w, m, s], self.dz_r.at[w, m, s])
                else:
                    self.send(piece, piece, self.dz_s.at[w, m, s], self.dz_r.at[w, m, s], self.dev(sign, 0))

    def planes(self, s):
        return [(0, 0)] if s == 0 else [(7, 4)] if s == 4 else [(2 * s - 1, -s), (2 * s, s)]

    def down_y(self, s):
        for k, dz in self.planes(s):
            for m, sign in enumerate((1, -1)):
                for w, piece in self.both(self.rows(dz, 0)):
                    self.send(piece, piece, self.dy_s.at[w, k, m], self.dy_r.at[w, k, m], self.dev(0, sign))

    def down_half(self, s, receive):
        for k, dz in self.planes(s):
            for m, sign in enumerate((1, -1)):
                if receive:
                    for w, piece in self.both(self.rows(dz, -2 * sign, 32 * m, 32)):
                        self.arrived(piece, self.dh_s.at[w, k, m], self.dh_r.at[w, k, m])
                else:
                    for w, piece in self.both(self.rows(dz, -sign)):
                        self.arrived(piece, self.dy_s.at[w, k, m], self.dy_r.at[w, k, m])
                    for w, piece in self.both(self.rows(dz, -sign, 32 * m, 32)):
                        self.send(piece, piece, self.dh_s.at[w, k, m], self.dh_r.at[w, k, m], self.dev(0, sign))

    def up_step(self, n):
        s, part = divmod(n, 3)
        if part == 0:
            if s == 0:
                for m, sign in enumerate((1, -1)):
                    piece = self.up.at[self.rows(0, 0), pl.ds(0, CUT)]
                    self.send(piece, piece, self.uy_s.at[m], self.uy_r.at[m], self.dev(0, sign))
            else:
                self.up_z(s - 1, 0, True)
            if s < 4:
                self.up_z(s, 0, False)
        elif part == 1:
            if s == 0:
                for m, sign in enumerate((1, -1)):
                    self.arrived(self.up.at[self.rows(0, -sign), pl.ds(0, CUT)], self.uy_s.at[m], self.uy_r.at[m])
                    piece = self.up.at[self.rows(0, -sign, 32 * m, 32), pl.ds(0, CUT)]
                    self.send(piece, piece, self.uh_s.at[m], self.uh_r.at[m], self.dev(0, sign))
            else:
                self.up_z(s - 1, 1, True)
                self.up_z(s - 1, 3, True)
            if s < 4:
                self.up_z(s, 1, False)
                self.up_z(s, 3, False)
        else:
            if s == 0:
                for m, sign in enumerate((1, -1)):
                    piece = self.up.at[self.rows(0, -2 * sign, 32 * m, 32), pl.ds(0, CUT)]
                    self.arrived(piece, self.uh_s.at[m], self.uh_r.at[m])
            else:
                self.up_z(s - 1, 2, True)
            if s < 4:
                self.up_z(s, 2, False)

    def down_step(self, s):
        if s > 0:
            self.down_z(s - 1, True)
        if s < 4:
            self.down_z(s, False)
        self.down_y(s)

    def turn(self, s):
        self.down_half(s, True)
        for _, dz in self.planes(s):
            plane = lax.rem(self.z + dz + 8, 8)
            span = pl.ds(pl.multiple_of(plane * 256, 256), 256)
            for j in range(4):
                block = self.down[span, 256 * j : 256 * j + 256]
                self.turned[256 * j : 256 * j + 256, span] = jnp.transpose(block)


class TpGather:
    def __init__(self, buf, size, send, recv, sp, tp):
        self.buf, self.size, self.s, self.r, self.sp = buf, size, send, recv, sp
        self.x, self.c = tp // 2, lax.rem(tp, 2)
        self.sent = []

    def slot(self, dx, other):
        return lax.rem(self.x + dx + 4, 4) * 2 + (1 - self.c if other else self.c)

    def rows(self, dx, other, half=None):
        low, count = (0, self.size) if half is None else (half * (self.size // 2), self.size // 2)
        return self.buf.at[pl.ds(pl.multiple_of(self.slot(dx, other) * self.size + low, 16), count)]

    def send(self, src, dst, k, dx, other):
        copy = copy_to(src, dst, self.s.at[k], self.r.at[k], (self.sp, self.slot(dx, other)))
        copy.start()
        self.sent.append(copy)

    def arrived(self, dst, k):
        copy_to(dst, dst, self.s.at[k], self.r.at[k], (self.sp, self.slot(0, True))).wait_recv()

    def begin(self):
        for half in range(2):
            for k, dx in ((0, 1), (1, -1)):
                part = half if dx == 1 else 1 - half
                mine = self.rows(0, False, part)
                self.send(mine, mine, k + 8 * half, dx, False)
        self.send(self.rows(0, False), self.rows(0, False), 2, 0, True)

    def relay(self):
        left, right = self.rows(-1, False), self.rows(1, False)
        self.arrived(self.rows(-1, False, 0), 0)
        self.send(self.rows(-1, False, 0), self.rows(-1, False, 0), 3, 1, False)
        self.arrived(self.rows(1, False, 1), 1)
        self.send(self.rows(1, False, 1), self.rows(1, False, 1), 4, -1, False)
        self.arrived(self.rows(-1, False, 1), 8)
        self.send(left, left, 5, 0, True)
        self.arrived(self.rows(1, False, 0), 9)
        self.send(right, right, 6, 0, True)

    def far(self):
        self.arrived(self.rows(2, False, 0), 3)
        self.arrived(self.rows(2, False, 1), 4)
        self.send(self.rows(2, False), self.rows(2, False), 7, 0, True)

    def sibling(self, k):
        self.arrived(self.rows({2: 0, 5: -1, 6: 1, 7: 2}[k], True), k)


def layer_kernel(
    hv_any, em_any, rm_any, gate_any, stream_any, wout_any, up_any, down_any,
    step_in, sudden_in, docs_in, rate, bias, tap_v, tap_e, tap_r, gain, first_gain, last_gain, out,
    hv, em, rm, gate, stream, wout_in,
    prev_v, prev_e, prev_r, next_v, next_e, next_r,
    per_token, gains_in, wide, rowq, cols, val, ent, ent32, rdo, weight, local,
    msg0, msg1, got0, got1, wmsg0, wmsg1, wgot0, wgot1, states,
    up, down, turned, norm_out, mix_sib, mix_got, mix_own, mix_far, mix_near, mix_relay, mix_in, stream_in, gains, first, tok, squares,
    sib_out, sib_in, own_part, outgoing, parts, relay, stat_out, stat_in,
    pull, halo_send, halo_recv, state_send, state_recv,
    uy_s, uy_r, uh_s, uh_r, uz_s, uz_r, dz_s, dz_r, dy_s, dy_r, dh_s, dh_r,
    mx_s, mx_r, tk_s, tk_r, ex_s, ex_r, sb_s, sb_r, rs_s, rs_r, st_s, st_r,
):
    sp, tp = lax.axis_index("sp"), lax.axis_index("tp")
    n_sp = lax.axis_size("sp")
    n_tp = lax.axis_size("tp")
    rows = hv.shape[0]
    tiles = rows // 128
    share = rows // n_tp

    def at(d):
        return (lax.rem(sp + d + n_sp, n_sp), tp)

    def peer(d):
        return lax.rem(tp + d + n_tp, n_tp)

    own_rows = pl.ds(pl.multiple_of(sp * 64, 64), 64)
    up_in, down_in = up.at[own_rows], down.at[own_rows]
    barrier = pltpu.get_barrier_semaphore()
    gains_in[...] = jnp.broadcast_to(first_gain[...].reshape(1, 256), (8, 256))
    for d in range(1, REACH + 1):
        for s in (d, -d):
            pl.semaphore_signal(barrier, inc=1, device_id=at(s), device_id_type=MESH)
    for d in range(1, n_tp):
        pl.semaphore_signal(barrier, inc=1, device_id=(sp, peer(d)), device_id_type=MESH)
    pulls = [pltpu.make_async_copy(src, dst, pull.at[k]) for k, (src, dst) in enumerate((
        (hv_any, hv), (em_any, em), (rm_any, rm), (up_any, up_in), (down_any, down_in), (stream_any, stream),
        (gate_any, gate), (wout_any, wout_in)))]
    for copy in pulls:
        copy.start()
    pl.semaphore_wait(barrier, 2 * REACH + n_tp - 1)
    for copy in pulls:
        copy.wait()

    halos = []
    for k, (src, low, high) in enumerate(((hv, prev_v, next_v), (em, prev_e, next_e), (rm, prev_r, next_r))):
        for m, (start, dst, step) in enumerate(((rows - 16, low, 1), (0, high, -1))):
            halos.append(copy_to(src.at[pl.ds(start, 16)], dst, halo_send.at[2 * k + m], halo_recv.at[2 * k + m],
                                 at(step)))
    for copy in halos:
        copy.start()
    ring = WeightRing(up_in, down_in, up, down, turned,
                      (uy_s, uy_r, uh_s, uh_r, uz_s, uz_r, dz_s, dz_r, dy_s, dy_r, dh_s, dh_r), sp, tp)
    ring.up_step(0)
    ring.down_step(0)

    def my_lanes(ref, q):
        return ref.at[:, pl.ds(pl.multiple_of(q * 256, 256), 256)]

    def exchange(k, src_of, dst):
        sent = []
        for d in range(1, n_tp):
            q = peer(d)
            copy = copy_to(src_of(q), my_lanes(dst, tp), ex_s.at[k, d - 1], ex_r.at[k, d - 1], (sp, q))
            copy.start()
            sent.append(copy)
        return sent

    def exchanged(k, dst):
        for d in range(1, n_tp):
            r = my_lanes(dst, peer(-d))
            copy_to(r, r, ex_s.at[k, d - 1], ex_r.at[k, d - 1], (sp, peer(d))).wait_recv()

    def token_rows(ref):
        return lambda q: ref.at[pl.ds(pl.multiple_of(q * share, 16), share)]

    sends = exchange(0, token_rows(stream), stream_in)
    sends += exchange(1, lambda q: gains_in, gains)
    mine = pl.ds(pl.multiple_of(tp * share, 16), share)
    my_cols = pl.ds(pl.multiple_of(tp * 256, 256), 256)
    stream_in[:, my_cols] = stream[mine, :]
    gains[:, my_cols] = gains_in[...]

    raw = step_in[...].astype(F32)
    sudden = sudden_in[...]

    def eight(ref):
        return jnp.concatenate([jnp.full((1, rows), ref[k, h], F32) for k in range(2) for h in range(4)], axis=0)

    before_softplus = jnp.concatenate([raw, raw], axis=0) + eight(bias)
    per_token[0:8, :] = jnp.maximum(before_softplus, 0.0) + jnp.log1p(jnp.exp(-jnp.abs(before_softplus)))
    per_token[8:16, :] = -jnp.exp(eight(rate)) * per_token[0:8, :] + jnp.concatenate([sudden, sudden], axis=0)

    def doc_at(row, lane_no):
        return docs_in[pl.ds(row, 1), lane_no : lane_no + 1].astype(F32)

    own_doc = jnp.concatenate([docs_in[pl.ds(tiles * sp + t, 1), :] for t in range(tiles)], axis=1).astype(F32)
    own8 = jnp.broadcast_to(own_doc, (8, rows))
    low_row, high_row = jnp.maximum(tiles * sp - 1, 0), jnp.minimum(tiles * sp + tiles, tiles * n_sp - 1)
    prev_two, prev_one = (jnp.where(sp > 0, doc_at(low_row, k), -1.0) for k in (126, 127))
    next_one, next_two = (jnp.where(sp < n_sp - 1, doc_at(high_row, k), -1.0) for k in (0, 1))
    lane8 = lax.broadcasted_iota(jnp.int32, (8, rows), 1)
    back_one = jnp.where(lane8 == 0, prev_one, pltpu.roll(own8, 1, 1))
    back_two = jnp.where(lane8 == 0, prev_two, jnp.where(lane8 == 1, prev_one, pltpu.roll(own8, 2, 1)))
    on_one = jnp.where(lane8 == rows - 1, next_one, pltpu.roll(own8, rows - 1, 1))
    on_two = jnp.where(lane8 == rows - 1, next_two, jnp.where(lane8 == rows - 2, next_one, pltpu.roll(own8, rows - 2, 1)))
    for k, row in enumerate((back_two, back_one, own8, on_one, on_two)):
        per_token[16 + k : 17 + k, :] = row[0:1]
    per_token[21:22, :] = jnp.broadcast_to(prev_one, (1, rows))
    per_token[22:23, :] = jnp.broadcast_to(next_one, (1, rows))
    per_token[23:24, :] = jnp.zeros((1, rows), F32)

    def last_doc(d):
        return doc_at(tiles * lax.rem(sp - d + n_sp, n_sp) + tiles - 1, 127)

    def first_doc(d):
        return doc_at(tiles * lax.rem(sp + d, n_sp), 0)

    source_mask = []
    for edge, room in ((last_doc, sp), (first_doc, n_sp - 1 - sp)):
        for d, to in ((1, 0), (2, 0), (4, 1), (7, 1)):
            source_mask.append(jnp.where((edge(d) == edge(to)) & (room >= d), 1.0, 0.0))

    dt = per_token[0:8, :]
    log_decay = per_token[8:16, :]
    lane = lax.broadcasted_iota(jnp.int32, (8, rows), 1)
    total = log_decay
    shift = 1
    while shift < rows:
        total = total + jnp.where(lane >= shift, pltpu.roll(total, shift, 1), 0.0)
        shift *= 2
    c0 = total[0:4]
    d1 = total[4:8] - log_decay[4:8]
    all0, all1 = total[0:4, rows - 1 : rows], total[4:8, rows - 1 : rows]
    docs = per_token[16:24, :]
    own = docs[2:3]
    same_end = jnp.where(own == own[:, rows - 1 : rows], 1.0, 0.0)
    same_start = jnp.where(own == own[:, 0:1], 1.0, 0.0)
    from_prev = jnp.where(own == docs[5:6], 1.0, 0.0)
    from_next = jnp.where(own == docs[6:7], 1.0, 0.0)
    rowq[...] = jnp.zeros_like(rowq)
    rowq[C0 : C0 + 4, :] = c0
    rowq[D1 : D1 + 4, :] = d1
    rowq[W0 : W0 + 4, :] = jnp.exp(all0 - c0) * dt[0:4] * same_end
    rowq[W1 : W1 + 4, :] = jnp.exp(d1) * dt[4:8] * same_start
    rowq[A0 : A0 + 4, :] = jnp.exp(c0) * from_prev
    rowq[A1 : A1 + 4, :] = jnp.exp(all1 - d1) * from_next
    rowq[DT0 : DT0 + 4, :] = dt[0:4]
    rowq[CM : CM + 5, :] = jnp.where(docs[0:5] == own, 1.0, 0.0)
    rowq[DOC : DOC + 1, :] = own
    for t in range(tiles):
        cols[pl.ds(128 * t, 128), :] = jnp.transpose(rowq[:, 128 * t : 128 * t + 128])

    wide[8 : 8 + rows, 0:256] = hv[...].astype(F32)
    wide[8 : 8 + rows, 256:384] = em[...].astype(F32)
    wide[8 : 8 + rows, 384:512] = rm[...].astype(F32)
    whole_taps = tap_v[...].astype(F32)
    taps = (whole_taps[:, 0:128], whole_taps[:, 128:256], tap_e[...].astype(F32), tap_r[...].astype(F32))

    def convolve(t):
        lo = 128 * t
        masks = [jnp.broadcast_to(cols[lo : lo + 128, CM + o : CM + o + 1], (128, 128)) for o in range(5)]
        for g in range(4):
            acc = jnp.zeros((128, 128), F32)
            for o in range(5):
                part = wide[lo + 6 + o : lo + 134 + o, 128 * g : 128 * g + 128]
                if o != 2:
                    part = part * masks[o]
                acc = acc + taps[g][o : o + 1] * part
            act = acc * jax.nn.sigmoid(acc)
            if g < 2:
                val[lo : lo + 128, 128 * g : 128 * g + 128] = act.astype(BF16)
            elif g == 2:
                ent32[lo : lo + 128, :] = act
                ent[lo : lo + 128, :] = act.astype(BF16)
            else:
                rdo[lo : lo + 128, :] = act.astype(BF16)

    def state_of(t, state0, state1):
        r = pl.ds(128 * t, 128)
        ent_t = jnp.transpose(ent32[r, :]).astype(BF16)
        v = val[r, :].astype(F32)
        state0 += jnp.dot(ent_t, (v * lanes_of(cols, r, W0)).astype(BF16), preferred_element_type=F32)
        state1 += jnp.dot(ent_t, (v * lanes_of(cols, r, W1)).astype(BF16), preferred_element_type=F32)
        return state0, state1

    state0 = state1 = jnp.zeros((STATE, 256), F32)
    for t in range(1, tiles - 1):
        convolve(t)
        state0, state1 = state_of(t, state0, state1)
    for copy in halos:
        copy.wait()
    wide[0:8, 0:256] = prev_v[8:16, :].astype(F32)
    wide[0:8, 256:384] = prev_e[8:16, :].astype(F32)
    wide[0:8, 384:512] = prev_r[8:16, :].astype(F32)
    wide[8 + rows : 16 + rows, 0:256] = next_v[0:8, :].astype(F32)
    wide[8 + rows : 16 + rows, 256:384] = next_e[0:8, :].astype(F32)
    wide[8 + rows : 16 + rows, 384:512] = next_r[0:8, :].astype(F32)

    for t in (0, tiles - 1):
        convolve(t)
        state0, state1 = state_of(t, state0, state1)

    def fill(msg, state, passing):
        msg[0:STATE, :] = state.astype(BF16)
        coarse = passing.astype(BF16)
        fine = (passing - coarse.astype(F32)).astype(BF16)
        row = lax.broadcasted_iota(jnp.int32, (16, 256), 0)
        both = jnp.where(row == 0, coarse.astype(F32), jnp.where(row == 1, fine.astype(F32), 0.0))
        msg[STATE : STATE + 16, :] = both.astype(BF16)

    def passing_of(msg):
        tail = msg[STATE : STATE + 16, :].astype(F32)
        return tail[0:1] + tail[1:2]

    pass_own = [head_lanes([jnp.exp(whole[h : h + 1, :]) for h in range(4)]) for whole in (all0, all1)]
    for m, (msg, state) in enumerate(((msg0, state0), (msg1, state1))):
        states[m] = state
        fill(msg, state, pass_own[m])

    for t in range(tiles):
        r = pl.ds(128 * t, 128)
        own_score = jnp.sum(rdo[r, :].astype(F32) * ent[r, :].astype(F32), axis=1, keepdims=True)
        local[r, :] = own_score * lanes_of(cols, r, DT0) * val[r, :].astype(F32)

    near_sends = []
    for k, d in enumerate((1, 2)):
        for m, (msg, got, step) in enumerate(((msg0, got0, d), (msg1, got1, -d))):
            near_sends.append(copy_to(msg, got.at[k], state_send.at[2 * k + m], state_recv.at[2 * k + m], at(step)))
    for copy in reversed(near_sends):
        copy.start()
    ring.up_step(1)

    low_lane = lax.broadcasted_iota(jnp.int32, (128, 128), 1) < HEAD_DIM

    def tile_step(i, _):
        r = pl.ds(pl.multiple_of(i * 128, 128), 128)
        here = rdo[r, :]
        doc_t = jnp.broadcast_to(cols[r, DOC : DOC + 1], (128, 128))
        t_index = lax.broadcasted_iota(jnp.int32, (128, 128), 0) + i * 128
        for pair in range(2):
            outs = []
            for h in (2 * pair, 2 * pair + 1):
                ct = jnp.broadcast_to(cols[r, C0 + h : C0 + h + 1], (128, 128))
                dd = jnp.broadcast_to(cols[r, D1 + h : D1 + h + 1], (128, 128))
                for j in range(tiles):
                    s = pl.ds(128 * j, 128)
                    if h == 0:
                        score = lax.dot_general(here, ent[s, :], (((1,), (1,)), ((), ())), preferred_element_type=F32)
                        score = jnp.where(doc_t == per_token[18:19, 128 * j : 128 * j + 128], score, 0.0)
                        weight[1, :, 128 * j : 128 * j + 128] = score
                    score = weight[1, :, 128 * j : 128 * j + 128]
                    s_index = lax.broadcasted_iota(jnp.int32, (128, 128), 1) + 128 * j
                    spread = jnp.minimum(ct - rowq[C0 + h : C0 + h + 1, 128 * j : 128 * j + 128],
                                         rowq[D1 + h : D1 + h + 1, 128 * j : 128 * j + 128] - dd)
                    step = jnp.where(s_index < t_index, per_token[h : h + 1, 128 * j : 128 * j + 128],
                                     per_token[4 + h : 5 + h, 128 * j : 128 * j + 128])
                    weight[0, :, 128 * j : 128 * j + 128] = score * jnp.exp(spread) * step
                outs.append(jnp.dot(weight[0].astype(BF16), val[:, 128 * pair : 128 * pair + 128],
                                    preferred_element_type=F32))
            local[r, 128 * pair : 128 * pair + 128] += jnp.where(low_lane, outs[0], outs[1])
        return 0

    lax.fori_loop(0, tiles // 2, tile_step, 0)
    for copy in near_sends:
        copy.wait()
    for m, (got, wmsg) in enumerate(((got0, wmsg0), (got1, wmsg1))):
        through = [pass_own[m]]
        for k in range(2):
            through.append(through[k] * passing_of(got.at[k]))
        window = states[m]
        for k in range(2):
            window += got[k, 0:STATE, :].astype(F32) * (through[k] * source_mask[4 * m + k])
        fill(wmsg, window, through[2])
    far_sends = []
    for k, d in enumerate((1, 4, 7)):
        for m, (wmsg, wgot, step) in enumerate(((wmsg0, wgot0, d), (wmsg1, wgot1, -d))):
            n = 4 + 2 * k + m
            far_sends.append(copy_to(wmsg, wgot.at[k], state_send.at[n], state_recv.at[n], at(step)))
    for copy in reversed(far_sends):
        copy.start()
    ring.down_step(1)
    ring.down_half(0, False)
    lax.fori_loop(tiles // 2, tiles, tile_step, 0)
    for copy in far_sends:
        copy.wait()
    ring.up_step(3)
    ring.up_step(2)
    ring.up_step(4)
    carried = []
    for m, wgot in enumerate((wgot0, wgot1)):
        once = passing_of(wgot.at[0])
        twice = once * passing_of(wgot.at[1])
        state = (wgot[0, 0:STATE, :].astype(F32)
                 + wgot[1, 0:STATE, :].astype(F32) * (once * source_mask[4 * m + 2])
                 + wgot[2, 0:STATE, :].astype(F32) * (twice * source_mask[4 * m + 3]))
        carried.append(state.astype(BF16))

    for t in range(tiles):
        r = pl.ds(128 * t, 128)
        here = rdo[r, :]
        y = local[r, :]
        y += jnp.dot(here, carried[0], preferred_element_type=F32) * lanes_of(cols, r, A0)
        y += jnp.dot(here, carried[1], preferred_element_type=F32) * lanes_of(cols, r, A1)
        z = gate[r, :].astype(F32)
        y = y * (z * jax.nn.sigmoid(z))
        y = y * lax.rsqrt(jnp.mean(y * y, axis=1, keepdims=True) + norm_eps)
        norm_out[r, :] = (y * gain[...].reshape(1, 256)).astype(BF16)

    x, c = tp // 2, lax.rem(tp, 2)
    half_share = share // 2

    def chip(d):
        return lax.rem(x + d + 4, 4)

    def project(k, d):
        for other in (True, False):
            q = 2 * chip(d) + (1 - c if other else c)
            part = jnp.dot(norm_out[pl.ds(pl.multiple_of(q * share, 16), share), :], wout_in[...],
                           preferred_element_type=F32)
            if other:
                mix_sib[k] = part.astype(BF16)
            else:
                mix_own[k] = part
        copy = copy_to(mix_sib.at[k], mix_got.at[k], mx_s.at[k], mx_r.at[k], (sp, 2 * x + 1 - c))
        copy.start()
        return copy

    def mix_push(src, dst, n, d):
        copy = copy_to(src, dst, mx_s.at[n], mx_r.at[n], (sp, 2 * chip(d) + c))
        copy.start()
        sends.append(copy)

    def mix_arrived(dst, n):
        copy_to(dst, dst, mx_s.at[n], mx_r.at[n], (sp, 2 * x + 1 - c)).wait_recv()

    def mix_far_out():
        crossing[0].wait()
        mix_far[...] = (mix_own[0] + mix_got[0].astype(F32)).astype(BF16)
        for e, d in enumerate((1, -1)):
            mix_push(mix_far.at[pl.ds(half_share * e, half_share)], mix_relay.at[e], 4 + e, d)
        return [sends.pop(), sends.pop()]

    def mix_near_rest():
        for copy in far_out:
            copy.wait_send()
        for e, d in enumerate((1, -1)):
            crossing[1 + e].wait()
            rest = pl.ds(half_share * (1 - e), half_share)
            mix_near[e, rest] = (mix_own[1 + e, rest] + mix_got[1 + e, rest].astype(F32)).astype(BF16)
            mix_push(mix_near.at[e, rest], mix_in.at[e, rest], 6 + e, d)
        crossing[3].wait()

    def mix_near_last():
        for e, d in enumerate((1, -1)):
            mix_arrived(mix_relay.at[e], 4 + e)
            half = pl.ds(half_share * e, half_share)
            total = mix_own[1 + e, half] + mix_got[1 + e, half].astype(F32) + mix_relay[e].astype(F32)
            mix_near[e, half] = total.astype(BF16)
            mix_push(mix_near.at[e, half], mix_in.at[e, half], 8 + e, d)

    def mix_finish():
        for e in range(2):
            mix_arrived(mix_in.at[e, pl.ds(half_share * (1 - e), half_share)], 6 + e)
            mix_arrived(mix_in.at[e, pl.ds(half_share * e, half_share)], 8 + e)
        first[...] = (resid_scale * stream_in[...].astype(F32) + mix_own[3] + mix_got[3].astype(F32)
                      + mix_in[0].astype(F32) + mix_in[1].astype(F32))

    crossing = [project(0, 2)]
    crossing.append(project(1, 1))
    far_out = mix_far_out()
    crossing.append(project(2, -1))
    crossing.append(project(3, 0))
    ring.up_step(6)
    ring.down_step(2)
    ring.down_half(1, False)
    mix_near_rest()
    ring.up_step(5)
    mix_near_last()
    ring.down_step(3)
    ring.down_half(2, False)
    ring.turn(0)
    ring.turn(1)
    ring.up_step(7)
    ring.up_step(9)
    exchanged(0, stream_in)
    exchanged(1, gains)
    mix_finish()
    f = first[...]
    mean = jnp.sum(f, axis=1, keepdims=True) * (1.0 / D)
    var = jnp.sum(f * f, axis=1, keepdims=True) * (1.0 / D) - mean * mean
    tok[mine, :] = ((f - mean) * lax.rsqrt(var + norm_eps) * gains[0:1, :]).astype(BF16)
    tg = TpGather(tok, share, tk_s, tk_r, sp, tp)
    tg.begin()
    ring.up_step(8)
    ring.down_step(4)
    ring.up_step(10)
    ring.down_half(3, False)
    ring.turn(2)
    tg.relay()
    ring.up_step(11)
    ring.up_step(12)
    ring.down_half(4, False)
    ring.up_step(13)
    tg.far()
    ring.turn(3)
    ring.up_step(14)
    ring.turn(4)
    for k in (2, 5, 6, 7):
        tg.sibling(k)

    def chunk_rows(k):
        return pl.ds(2 * share * k, 2 * share)

    def hidden(k):
        chunk = tok[chunk_rows(k), :]
        for n in range(4):
            h = jnp.maximum(jnp.dot(chunk, up[:, 256 * n : 256 * n + 256], preferred_element_type=F32), 0.0)
            squares[:, 256 * n : 256 * n + 256] = (h * h).astype(BF16)

    def compute(k):
        sq = squares[...]
        for n, d in enumerate((2, 1, -1, 0)):
            for other in (True, False):
                q = 2 * chip(d) + (1 - c if other else c)
                w = turned[:, pl.ds(pl.multiple_of(q * 256, 256), 256)]
                part = jnp.dot(sq, w, preferred_element_type=F32)
                if other:
                    sib_out[k, n] = part.astype(BF16)
                else:
                    own_part[k % 3, n] = part
        crossing = []
        for n, r in enumerate((pl.ds(0, 1), pl.ds(1, 3))):
            copy = copy_to(sib_out.at[k, r], sib_in.at[k, r], sb_s.at[k, n], sb_r.at[k, n], (sp, 2 * x + 1 - c))
            copy.start()
            crossing.append(copy)
        return crossing

    def push(src, dst, k, e, d):
        copy = copy_to(src, dst, rs_s.at[k, e], rs_r.at[k, e], (sp, 2 * chip(d) + c))
        copy.start()
        sends.append(copy)

    def pass_on(k, crossing):
        crossing[0].wait()
        outgoing[k, 2] = (own_part[k % 3, 0] + sib_in[k, 0].astype(F32)).astype(BF16)
        for e, d in enumerate((1, -1)):
            half = pl.ds(share * e, share)
            push(outgoing.at[k, 2, half], relay.at[k, e], k, 2 + e, d)
        crossing[1].wait()
        for e, d in enumerate((1, -1)):
            rest = pl.ds(share * (1 - e), share)
            outgoing[k, e, rest] = (own_part[k % 3, 1 + e, rest] + sib_in[k, 1 + e, rest].astype(F32)).astype(BF16)
            push(outgoing.at[k, e, rest], parts.at[e, pl.ds(2 * share * k + share * (1 - e), share)], k, 4 + e, d)
        local[chunk_rows(k), :] = own_part[k % 3, 3] + sib_in[k, 3].astype(F32)

    def push_near(k):
        for e, d in enumerate((1, -1)):
            copy_to(relay.at[k, e], relay.at[k, e], rs_s.at[k, 2 + e], rs_r.at[k, 2 + e], (sp, 2 * chip(d) + c)).wait_recv()
            half = pl.ds(share * e, share)
            total = own_part[k % 3, 1 + e, half] + sib_in[k, 1 + e, half].astype(F32)
            outgoing[k, e, half] = (total + relay[k, e].astype(F32)).astype(BF16)
            push(outgoing.at[k, e, half], parts.at[e, pl.ds(2 * share * k + share * e, share)], k, e, d)

    hidden(0)
    copy0 = compute(0)
    hidden(1)
    pass_on(0, copy0)
    copy1 = compute(1)
    hidden(2)
    pass_on(1, copy1)
    push_near(0)
    copy2 = compute(2)
    hidden(3)
    pass_on(2, copy2)
    push_near(1)
    copy3 = compute(3)
    pass_on(3, copy3)

    def parts_arrived(k):
        for e, d in enumerate((1, -1)):
            for n, low in ((4 + e, share * (1 - e)), (e, share * e)):
                r = parts.at[e, pl.ds(2 * share * k + low, share)]
                copy_to(r, r, rs_s.at[k, n], rs_r.at[k, n], (sp, 2 * chip(d) + c)).wait_recv()

    lane_at = lax.broadcasted_iota(jnp.int32, (128, 128), 1)
    group = tiles // 2

    def row_sums(g):
        for t in range(group * g, group * g + group):
            r = pl.ds(128 * t, 128)
            y = local[r, :] + resid_scale * tok[r, my_cols].astype(F32)
            for e in range(2):
                y += parts[e, r, :].astype(F32)
            local[r, :] = y
            one = jnp.sum(y, axis=1, keepdims=True)
            two = jnp.sum(y * y, axis=1, keepdims=True)
            pair = jnp.where(lane_at == 0, one, jnp.where(lane_at == 1, two, 0.0))
            at_lane = 128 * (t - group * g)
            stat_out[g, :, at_lane : at_lane + 128] = jnp.transpose(pair)[0:2, :]
        for d in range(1, n_tp):
            copy = copy_to(stat_out.at[g], stat_in.at[g, d - 1], st_s.at[g, d - 1], st_r.at[g, d - 1], (sp, peer(d)))
            copy.start()
            sends.append(copy)

    def stats_arrived(g):
        for d in range(1, n_tp):
            dst = stat_in.at[g, d - 1]
            copy_to(dst, dst, st_s.at[g, d - 1], st_r.at[g, d - 1], (sp, peer(d))).wait_recv()

    def all_sent(copies):
        for copy in copies:
            copy.wait_send()

    def second_norm(g):
        stats = stat_out[g]
        for d in range(1, n_tp):
            stats += stat_in[g, d - 1]
        mean = stats[0:1] * (1.0 / D)
        scale = lax.rsqrt(stats[1:2] * (1.0 / D) - mean * mean + norm_eps)
        lanes = pl.ds(128 * group * g, 128 * group)
        rowq[0:1, lanes] = mean
        rowq[1:2, lanes] = scale
        for t in range(group * g, group * g + group):
            r = pl.ds(128 * t, 128)
            both = jnp.transpose(rowq[:, 128 * t : 128 * t + 128])
            out[r, :] = ((local[r, :] - both[:, 0:1]) * both[:, 1:2] * last_gain[...].reshape(1, 256)).astype(BF16)

    push_near(2)
    parts_arrived(0)
    parts_arrived(1)
    row_sums(0)
    push_near(3)
    parts_arrived(2)
    parts_arrived(3)
    row_sums(1)
    stats_arrived(0)
    second_norm(0)
    all_sent(sends[: -2 * (n_tp - 1)] + ring.sent + tg.sent)
    stats_arrived(1)
    second_norm(1)
    all_sent(sends[-2 * (n_tp - 1) :])


def per_device(hv, em, rm, gate, step, sudden, document_index, rate, bias, tv, te, tr, gain,
               out_weight, stream, first_gain, last_gain, up_in, down_in):
    rows = hv.shape[0]
    docs = document_index.reshape(-1, 128)
    vmem = pl.BlockSpec(memory_space=pltpu.VMEM)
    dma = pltpu.SemaphoreType.DMA
    share = rows // 8
    return pl.pallas_call(
        layer_kernel,
        out_shape=jax.ShapeDtypeStruct((rows, 256), BF16),
        in_specs=[pl.BlockSpec(memory_space=pl.ANY)] * 8 + [vmem] * 3 + [pl.BlockSpec(memory_space=pltpu.SMEM)] * 2
        + [vmem] * 6,
        out_specs=vmem,
        scratch_shapes=[
            pltpu.VMEM((rows, 256), BF16), pltpu.VMEM((rows, 128), BF16), pltpu.VMEM((rows, 128), BF16),
            pltpu.VMEM((rows, 256), BF16), pltpu.VMEM((rows, 256), BF16), pltpu.VMEM((256, D), BF16),
            pltpu.VMEM((16, 256), BF16), pltpu.VMEM((16, 128), BF16), pltpu.VMEM((16, 128), BF16),
            pltpu.VMEM((16, 256), BF16), pltpu.VMEM((16, 128), BF16), pltpu.VMEM((16, 128), BF16),
            pltpu.VMEM((24, rows), F32), pltpu.VMEM((8, 256), F32),
            pltpu.VMEM((rows + 16, 512), F32),
            pltpu.VMEM((128, rows), F32),
            pltpu.VMEM((rows, 128), F32),
            pltpu.VMEM((rows, 256), BF16), pltpu.VMEM((rows, 128), BF16), pltpu.VMEM((rows, 128), F32),
            pltpu.VMEM((rows, 128), BF16),
            pltpu.VMEM((2, 128, rows), F32),
            pltpu.VMEM((rows, 256), F32),
            pltpu.VMEM((STATE + 16, 256), BF16), pltpu.VMEM((STATE + 16, 256), BF16),
            pltpu.VMEM((2, STATE + 16, 256), BF16), pltpu.VMEM((2, STATE + 16, 256), BF16),
            pltpu.VMEM((STATE + 16, 256), BF16), pltpu.VMEM((STATE + 16, 256), BF16),
            pltpu.VMEM((3, STATE + 16, 256), BF16), pltpu.VMEM((3, STATE + 16, 256), BF16),
            pltpu.VMEM((2, STATE, 256), F32),
            pltpu.VMEM((D, 1024), BF16), pltpu.VMEM((D, 1024), BF16), pltpu.VMEM((1024, D), BF16),
            pltpu.VMEM((rows, 256), BF16), pltpu.VMEM((4, share, D), BF16), pltpu.VMEM((4, share, D), BF16),
            pltpu.VMEM((4, share, D), F32), pltpu.VMEM((share, D), BF16), pltpu.VMEM((2, share, D), BF16),
            pltpu.VMEM((2, share // 2, D), BF16), pltpu.VMEM((2, share, D), BF16), pltpu.VMEM((share, D), BF16),
            pltpu.VMEM((8, D), F32), pltpu.VMEM((share, D), F32), pltpu.VMEM((rows, D), BF16),
            pltpu.VMEM((2 * share, 1024), BF16),
            pltpu.VMEM((4, 4, 2 * share, 256), BF16), pltpu.VMEM((4, 4, 2 * share, 256), BF16),
            pltpu.VMEM((3, 4, 2 * share, 256), F32), pltpu.VMEM((4, 3, 2 * share, 256), BF16),
            pltpu.VMEM((2, rows, 256), BF16), pltpu.VMEM((4, 2, share, 256), BF16), pltpu.VMEM((2, 2, rows // 2), F32),
            pltpu.VMEM((2, 7, 2, rows // 2), F32),
            dma((8,)), dma((6,)), dma((6,)), dma((10,)), dma((10,)),
            dma((2,)), dma((2,)), dma((2,)), dma((2,)), dma((2, 4, 4)), dma((2, 4, 4)),
            dma((2, 2, 4)), dma((2, 2, 4)), dma((2, 8, 2)), dma((2, 8, 2)), dma((2, 8, 2)), dma((2, 8, 2)),
            dma((10,)), dma((10,)), dma((10,)), dma((10,)), dma((2, 7)), dma((2, 7)),
            dma((4, 2)), dma((4, 2)), dma((4, 6)), dma((4, 6)), dma((2, 7)), dma((2, 7)),
        ],
        compiler_params=pltpu.CompilerParams(
            collective_id=0, has_side_effects=True, vmem_limit_bytes=60 * 1024 * 1024),
        cost_estimate=pl.CostEstimate(flops=9_000_000_000, bytes_accessed=8_000_000, transcendentals=0),
        name="layer",
    )(hv, em, rm, gate, stream, out_weight, up_in, down_in, step.T, sudden.T, docs, rate, bias, tv, te, tr, gain,
      first_gain, last_gain)


SPECS = (
    P("sp", "tp"), P("sp", "tp"), P("sp", "tp"), P("sp", "tp"), P("sp", "tp"), P("sp", "tp"), P(),
    P(None, "tp"), P(None, "tp"), P(None, "tp"), P(None, "tp"), P(None, "tp"), P("tp"),
    P("tp", None), P("sp", "tp"), P("tp"), P("tp"), P("sp", "tp"), P("sp", "tp"),
)


def solution(mesh):
    return jax.shard_map(per_device, mesh=mesh, in_specs=SPECS, out_specs=P("sp", "tp"), check_vma=False)
```
